32 devices in a mesh: sp: 4 (over z), fs: 4 (over y, x), tp: 2 (over core).
Axes of the slice: x: 2, y: 2, z: 4, core: 2. Of those that a mesh axis runs over, the one named last changes fastest.
Arguments:
- tokens: bfloat16 [4, 512, 2048], P('fs', ('sp', 'tp')), may hold values from -6 to 6
- input_norm_gain: float32 [2048], replicated, may hold values from 0.1 to 1.9
- pooling_input_weight: bfloat16 [2048, 1024], P('sp', 'tp'), may hold values from -0.125 to 0.125
- query_weight: bfloat16 [2048, 1024], P('sp', 'tp'), may hold values from -0.125 to 0.125
- forget_weight: bfloat16 [2048, 1024], P('sp', 'tp'), may hold values from -0.125 to 0.125
- value_weight: bfloat16 [2048, 1024], P('sp', 'tp'), may hold values from -0.125 to 0.125
- pooling_group_maps: bfloat16 [4, 256, 256], P('tp'), may hold values from -0.375 to 0.375
- pooling_scale: float32 [1024], P('tp'), may hold values from 0.1 to 1.9
- lower_bound_logits: float32 [1024], P('tp')
- decay_spike: float32 [4, 512, 8], P('fs', 'sp', 'tp'), may hold values from -0.75 to 0
- head_norm_gain: float32 [1024], P('tp'), may hold values from 0.1 to 1.9
- pooling_output_weight: bfloat16 [1024, 2048], P('tp', 'sp'), may hold values from -0.125 to 0.125
- recurrent_output_weight: bfloat16 [1024, 2048], P('tp', 'sp'), may hold values from -0.125 to 0.125
Outputs:
- mixed: bfloat16 [4, 512, 2048], P('fs', ('sp', 'tp'))
The draws below stay inside these ranges and needn't reach their ends.
All inputs are finite; a program needn't handle non-finite values.
Results may differ from the reference program's by a relative error of at most 0.013.
Values may be sent and summed in bfloat16 or wider, within the bound.
A program may use at most 64 MiB of HBM per device.

```python
import jax
import jax.numpy as jnp
from jax import lax

D = 2048
POOL_GROUP = 256
POOL_GROUPS = 4
HEAD = 128
RECURRENT_HEADS = 8
BLOCK = 64
TOK_DEV = 128
D_POOL = 1024
D_REC = 1024
LEN = 512
SEQUENCE_COUNT = 4
N_TP = 2


def head_kinds(key):
    ranking = jax.random.permutation(jax.random.fold_in(key, 11), RECURRENT_HEADS)
    return ranking < RECURRENT_HEADS // 2


def draw_lower_bound_logits(key, part):
    lasting = head_kinds(key)
    spread = jax.random.uniform(jax.random.fold_in(key, 12), (RECURRENT_HEADS, HEAD), jnp.float32)
    slow_rate = 0.3 * jnp.exp(jnp.log(4.0) * spread) / LEN
    fast_rate = 0.03 * jnp.exp(jnp.log(10.0 / 3.0) * spread)
    chosen = jnp.where(lasting[:, None], slow_rate, fast_rate)
    return (jnp.log1p(-chosen) - jnp.log(chosen)).reshape(D_REC)


def draw_decay_spike(key, part):
    lasting = head_kinds(key)
    devices = LEN // TOK_DEV
    spread = jax.random.uniform(jax.random.fold_in(key, 21), (SEQUENCE_COUNT, devices, RECURRENT_HEADS), jnp.float32)
    fast_rate = 0.004 * jnp.exp(jnp.log(5.0) * spread)
    slow_rate = 0.1 * jnp.exp(jnp.log(6.0) * spread) / LEN
    local_decay_rate = jnp.repeat(jnp.where(lasting[None, None, :], slow_rate, fast_rate), TOK_DEV, axis=1)
    third_length = LEN // 3
    spike_locations = jax.random.randint(jax.random.fold_in(key, 22), (SEQUENCE_COUNT, 3, RECURRENT_HEADS), 0, third_length)
    spike_locations = spike_locations + third_length * jnp.arange(3, dtype=jnp.int32)[None, :, None]
    kept_fraction = jax.random.uniform(jax.random.fold_in(key, 23), (SEQUENCE_COUNT, 3, RECURRENT_HEADS), jnp.float32, 0.55, 0.8)
    position_index = jnp.arange(LEN, dtype=jnp.int32)
    agreement = (position_index[None, :, None, None] == spike_locations[:, None, :, :]).astype(jnp.float32)
    spikes = jnp.sum(agreement * jnp.log(kept_fraction)[:, None, :, :], axis=2)
    return spikes - local_decay_rate


def shard_levels(own_key, shape, split, smallest, largest):
    level, own = 1.0, jax.random.fold_in(own_key, 6)
    for axis_at, blocks in split:
        steps = jnp.exp(jax.random.uniform(jax.random.fold_in(own, axis_at), (blocks,), jnp.float32, smallest / len(split), largest / len(split)))
        level = level * jnp.repeat(steps, shape[axis_at] // blocks).reshape([-1 if axis == axis_at else 1 for axis in range(len(shape))])
    return level


def scatter_about(rng, dims, scale, bound, shards=(), kind=jnp.bfloat16):
    drawn = jax.random.normal(rng, dims, jnp.float32) * scale
    if len(shards) > 0:
        drawn = shard_levels(rng, dims, shards, -0.22, 0.18) * drawn
    return jnp.clip(drawn, min=-bound, max=bound).astype(kind)


def setup_inputs(seed: int = 0) -> dict:
    seeds = jax.random.split(jax.random.key(seed), 14)
    return {
        "tokens": scatter_about(seeds[0], (SEQUENCE_COUNT, LEN, D), 1.0, 6.0, ((0, 4), (1, 8))),
        "input_norm_gain": jnp.clip(1.0 + 0.18 * jax.random.normal(seeds[1], (D,), jnp.float32), 0.1, 1.9),
        "pooling_input_weight": scatter_about(seeds[2], (D, D_POOL), D ** -0.5, 0.125, ((0, 4), (1, 2))),
        "query_weight": scatter_about(seeds[3], (D, D_REC), D ** -0.5, 0.125, ((0, 4), (1, 2))),
        "forget_weight": scatter_about(seeds[4], (D, D_REC), D ** -0.5, 0.125, ((0, 4), (1, 2))),
        "value_weight": scatter_about(seeds[5], (D, D_REC), D ** -0.5, 0.125, ((0, 4), (1, 2))),
        "pooling_group_maps": scatter_about(seeds[6], (POOL_GROUPS, POOL_GROUP, POOL_GROUP), POOL_GROUP ** -0.5, 0.375, ((0, 2),)),
        "pooling_scale": jnp.clip(1.0 + 0.18 * jax.random.normal(seeds[7], (D_POOL,), jnp.float32), 0.1, 1.9),
        "lower_bound_logits": draw_lower_bound_logits(jax.random.fold_in(seeds[13], 71), 0),
        "decay_spike": draw_decay_spike(jax.random.fold_in(seeds[13], 71), 0),
        "head_norm_gain": jnp.clip(1.0 + 0.18 * jax.random.normal(seeds[10], (D_REC,), jnp.float32), 0.1, 1.9),
        "pooling_output_weight": scatter_about(seeds[11], (D_POOL, D), (D_POOL + D_REC) ** -0.5, 0.125, ((0, 2), (1, 4))),
        "recurrent_output_weight": scatter_about(seeds[12], (D_REC, D), (D_POOL + D_REC) ** -0.5, 0.125, ((0, 2), (1, 4))),
    }


EPSILON = 1e-06
HIGHEST = lax.Precision.HIGHEST

def stored(values):
    return lax.optimization_barrier(values.astype(jnp.bfloat16))

def rms_scale(values, gain):
    return values * lax.rsqrt(lax.optimization_barrier(jnp.mean(values * values, axis=-1, keepdims=True)) + EPSILON) * gain

def pooling(pool_input, pooling_group_maps, pooling_scale):
    length_total = pool_input.shape[0]
    groups = pooling_group_maps.shape[0]
    group_size = pooling_group_maps.shape[1]
    reach_rows = 2 ** groups
    padded = jnp.pad(pool_input.astype(jnp.float32).reshape(length_total, groups, group_size), ((reach_rows, 0), (0, 0), (0, 0)))
    windows = 2 ** (jnp.arange(groups, dtype=jnp.int32) + 1)
    window_sum = jnp.zeros((length_total, groups, group_size), jnp.float32)
    for offset in range(reach_rows):
        inside = (offset < windows).astype(jnp.float32)
        window_sum = window_sum + padded[reach_rows - offset:reach_rows - offset + length_total] * inside[:, None]
    counts = jnp.minimum(jnp.arange(length_total, dtype=jnp.int32)[:, None] + 1, windows[None, :]).astype(jnp.float32)
    pool_diff = stored(window_sum / counts[:, :, None] - padded[reach_rows:])
    mapped = jnp.einsum('tgc,gcd->tgd', pool_diff.astype(jnp.float32), pooling_group_maps.astype(jnp.float32))
    return (mapped.reshape(length_total, groups * group_size) * pooling_scale).astype(jnp.bfloat16)

def linear_recurrence(query_matrix, forget_gate_logit, value_projected, lower_bound_logits, spike_row, head_norm_gain):
    length_total, width = query_matrix.shape
    number_heads = spike_row.shape[1]
    head_width = width // number_heads
    block_layout = (length_total // BLOCK, BLOCK, number_heads, head_width)
    reader = jax.nn.silu(query_matrix.astype(jnp.float32)).reshape(block_layout)
    key_gate_value = jax.nn.sigmoid(-lower_bound_logits) * jax.nn.sigmoid(-forget_gate_logit.astype(jnp.float32))
    decay_logarithm = (jnp.log1p(-key_gate_value).reshape(length_total, number_heads, head_width) + spike_row[:, :, None]).reshape(block_layout)
    key_rows = key_gate_value.reshape(block_layout)
    value_rows = value_projected.astype(jnp.float32).reshape(block_layout)
    causal = (jnp.arange(BLOCK)[:, None] >= jnp.arange(BLOCK)[None, :]).astype(jnp.float32)

    def advance(carried, input_batch):
        block_reader, block_key, block_value, block_log = input_batch
        inner_log = jnp.cumsum(block_log, axis=0)
        read_scaled = block_reader * jnp.exp(inner_log)
        key_scaled = block_key * jnp.exp(-inner_log)
        scores = jnp.einsum('thd,shd->hts', read_scaled, key_scaled, precision=HIGHEST) * causal
        output = jnp.einsum('hts,she->the', scores, block_value, precision=HIGHEST)
        output = output + jnp.einsum('thd,hde->the', read_scaled, carried, precision=HIGHEST)
        closing = inner_log[-1]
        key_tail = block_key * jnp.exp(closing[None] - inner_log)
        carried = jnp.exp(closing)[:, :, None] * carried + jnp.einsum('shd,she->hde', key_tail, block_value, precision=HIGHEST)
        return (carried, output)
    initial = jnp.zeros((number_heads, head_width, head_width), jnp.float32)
    final_state, read_out = lax.scan(advance, initial, (reader, key_rows, value_rows, decay_logarithm))
    read_out = read_out.reshape(length_total, number_heads, head_width)
    return (rms_scale(read_out, 1.0).reshape(length_total, width) * head_norm_gain).astype(jnp.bfloat16)

def reference(tokens, input_norm_gain, pooling_input_weight, query_weight, forget_weight, value_weight, pooling_group_maps, pooling_scale, lower_bound_logits, decay_spike, head_norm_gain, pooling_output_weight, recurrent_output_weight):
    pool_width = pooling_input_weight.shape[1] // N_TP
    rec_width = query_weight.shape[1] // N_TP

    def sequence_tokens(input_batch):
        token_series, spike_row = input_batch
        normed = rms_scale(token_series.astype(jnp.float32), input_norm_gain).astype(jnp.bfloat16)
        pool_input = stored(jnp.dot(normed, pooling_input_weight, preferred_element_type=jnp.float32))
        query_matrix = stored(jnp.dot(normed, query_weight, preferred_element_type=jnp.float32))
        forget_gate_logit = stored(jnp.dot(normed, forget_weight, preferred_element_type=jnp.float32))
        value_projected = stored(jnp.dot(normed, value_weight, preferred_element_type=jnp.float32))
        pool_out = pooling(pool_input, pooling_group_maps, pooling_scale)
        recurrent_output = linear_recurrence(query_matrix, forget_gate_logit, value_projected, lower_bound_logits, spike_row, head_norm_gain)
        mixed_sum = jnp.zeros((token_series.shape[0], pooling_output_weight.shape[1]), jnp.float32)
        for member in range(N_TP):
            pool_lo = member * pool_width
            rec_lo = member * rec_width
            partial_value = jnp.dot(pool_out[:, pool_lo:pool_lo + pool_width], pooling_output_weight[pool_lo:pool_lo + pool_width], preferred_element_type=jnp.float32)
            partial_value = partial_value + jnp.dot(recurrent_output[:, rec_lo:rec_lo + rec_width], recurrent_output_weight[rec_lo:rec_lo + rec_width], preferred_element_type=jnp.float32)
            mixed_sum = mixed_sum + stored(partial_value).astype(jnp.float32)
        return mixed_sum.astype(jnp.bfloat16)
    return lax.map(sequence_tokens, (tokens, decay_spike))
```

```python
import functools

import jax
import jax.numpy as jnp
from jax import lax
from jax.experimental import pallas as pl
from jax.experimental.pallas import tpu as pltpu
from jax.sharding import PartitionSpec as P

BLOCK = 64


EPSILON = 1e-06
HIGHEST = lax.Precision.HIGHEST


def shifted(value, axis, steps):
    count = lax.axis_size(axis)
    first, last = (max(0, -steps), min(count, count - steps))
    return lax.ppermute(value, axis, [(source, source + steps) for source in range(first, last)])


def entering(shard, axis, join, neutral):
    place = lax.axis_index(axis)
    gathered = jax.tree.map(
        lambda a, kind: lax.all_gather(a.astype(kind), axis), shard, (jnp.bfloat16, jnp.bfloat16)
    )
    state = jax.tree.map(lambda a, e: jnp.zeros_like(a) + jnp.asarray(e, a.dtype), shard, neutral)

    def one(step, state):
        return join(
            state,
            jax.tree.map(
                lambda a, own: lax.dynamic_index_in_dim(a, step, 0, False).astype(own.dtype),
                gathered,
                shard,
            ),
        )

    return lax.fori_loop(0, place, one, state)


def rms_scale(values, gain):
    return values * lax.rsqrt(jnp.mean(values * values, axis=-1, keepdims=True) + EPSILON) * gain


def join_state(earlier, later):
    decay_one, state_one = earlier
    decay_two, state_two = later
    return (decay_one * decay_two, decay_two[..., None] * state_one + state_two)


def body(
    tokens,
    input_norm_gain,
    pooling_input_weight,
    query_weight,
    forget_weight,
    value_weight,
    pooling_group_maps,
    pooling_scale,
    lower_bound_logits,
    decay_spike,
    head_norm_gain,
    pooling_output_weight,
    recurrent_output_weight,
):
    gathered = lax.all_gather(tokens, "tp", axis=1, tiled=True)[0]
    length_total = gathered.shape[0]
    normed = rms_scale(gathered.astype(jnp.float32), input_norm_gain).astype(jnp.bfloat16)
    pool_width = pooling_input_weight.shape[1]
    rec_width = query_weight.shape[1]
    stacked = jnp.concatenate(
        [pooling_input_weight, query_weight, forget_weight, value_weight], axis=1
    )
    out_local = jnp.concatenate([pooling_output_weight, recurrent_output_weight], axis=0)
    groups_fs = lax.axis_size("fs")
    member = lax.axis_index("fs")
    slice_width = stacked.shape[1] // groups_fs
    own_slice = lax.dynamic_slice_in_dim(stacked, member * slice_width, slice_width, 1)
    column_part = lax.all_gather(own_slice, "sp", axis=0, tiled=True)
    full_input = lax.all_gather(column_part, "fs", axis=1, tiled=True)
    projected = jnp.dot(normed, full_input, preferred_element_type=jnp.float32)
    slice_height = out_local.shape[0] // groups_fs
    own_rows = lax.dynamic_slice_in_dim(out_local, member * slice_height, slice_height, 0)
    row_part = lax.all_gather(own_rows, "sp", axis=1, tiled=True)
    out_full = lax.all_gather(row_part, "fs", axis=0, tiled=True)
    rounded = lax.optimization_barrier(projected.astype(jnp.bfloat16))
    pool_input = rounded[:, :pool_width]
    query_matrix = rounded[:, pool_width : pool_width + rec_width].astype(jnp.float32)
    forget_gate_logit = rounded[:, pool_width + rec_width : pool_width + 2 * rec_width].astype(
        jnp.float32
    )
    value_projected = rounded[:, pool_width + 2 * rec_width :].astype(jnp.float32)
    groups_local = pooling_group_maps.shape[0]
    group_size = pooling_group_maps.shape[1]
    reach_rows = 2 ** (groups_local * lax.axis_size("tp"))
    previous = shifted(pool_input[length_total - reach_rows :], "sp", 1)
    extended = jnp.concatenate([previous, pool_input], axis=0).astype(jnp.float32)
    extended = extended.reshape(reach_rows + length_total, groups_local, group_size)
    group_ids = lax.axis_index("tp") * groups_local + jnp.arange(groups_local, dtype=jnp.int32)
    windows = jnp.left_shift(jnp.int32(2), group_ids)
    window_sum = jnp.zeros((length_total, groups_local, group_size), jnp.float32)
    for offset in range(reach_rows):
        inside = (offset < windows).astype(jnp.float32)
        window_sum = (
            window_sum
            + extended[reach_rows - offset : reach_rows - offset + length_total] * inside[:, None]
        )
    position_index = lax.axis_index("sp") * length_total + jnp.arange(length_total, dtype=jnp.int32)
    counts = jnp.minimum(position_index[:, None] + 1, windows[None, :]).astype(jnp.float32)
    pool_diff = (window_sum / counts[:, :, None] - extended[reach_rows:]).astype(jnp.bfloat16)
    pool_mapped = jnp.einsum(
        "tgc,gcd->tgd", pool_diff, pooling_group_maps, preferred_element_type=jnp.float32
    )
    pool_out = (pool_mapped.reshape(length_total, pool_width) * pooling_scale).astype(jnp.bfloat16)
    local_heads = decay_spike.shape[2]
    head_width = rec_width // local_heads
    blocks = length_total // BLOCK
    block_layout = (blocks, BLOCK, local_heads, head_width)
    reader = jax.nn.silu(query_matrix).reshape(block_layout)
    key_gate_value = jax.nn.sigmoid(-lower_bound_logits) * jax.nn.sigmoid(-forget_gate_logit)
    decay_logarithm = (
        jnp.log1p(-key_gate_value).reshape(length_total, local_heads, head_width)
        + decay_spike[0][:, :, None]
    ).reshape(block_layout)
    key_rows = key_gate_value.reshape(block_layout)
    value_rows = value_projected.reshape(block_layout)
    inner_log = jnp.cumsum(decay_logarithm, axis=1)
    read_scaled = reader * jnp.exp(inner_log)
    key_scaled = key_rows * jnp.exp(-inner_log)
    causal = (jnp.arange(BLOCK)[:, None] >= jnp.arange(BLOCK)[None, :]).astype(jnp.float32)
    scores = jnp.einsum("nthd,nshd->nhts", read_scaled, key_scaled, precision=HIGHEST) * causal
    within = jnp.einsum("nhts,nshe->nthe", scores, value_rows, precision=HIGHEST)
    closing = inner_log[:, -1]
    key_tail = key_rows * jnp.exp(closing[:, None] - inner_log)
    deltas = jnp.einsum("nshd,nshe->nhde", key_tail, value_rows, precision=HIGHEST)
    block_decay = jnp.exp(closing)

    def advance(carried, input_batch):
        decay_now, delta_now = input_batch
        return (decay_now[..., None] * carried + delta_now, carried)

    initial = jnp.zeros((local_heads, head_width, head_width), jnp.float32)
    device_state, entry_states = lax.scan(advance, initial, (block_decay, deltas))
    device_decay = jnp.exp(jnp.sum(closing, axis=0))
    scanned = entering(
        (device_decay, device_state),
        "sp",
        join_state,
        (jnp.ones_like(device_decay), jnp.zeros_like(device_state)),
    )
    prior_state = scanned[1]
    before = jnp.cumsum(closing, axis=0) - closing
    start_states = entry_states + jnp.exp(before)[..., None] * prior_state[None]
    read_out = within + jnp.einsum("nthd,nhde->nthe", read_scaled, start_states, precision=HIGHEST)
    read_out = read_out.reshape(length_total, local_heads, head_width)
    recurrent_output = (
        rms_scale(read_out, 1.0).reshape(length_total, rec_width) * head_norm_gain
    ).astype(jnp.bfloat16)
    mixed_rows = jnp.concatenate([pool_out, recurrent_output], axis=1)
    summed = lax.psum_scatter(
        jnp.dot(mixed_rows, out_full, preferred_element_type=jnp.float32).astype(jnp.bfloat16),
        "tp",
        scatter_dimension=0,
        tiled=True,
    )
    return summed[None]


F32 = jnp.float32
BF16 = jnp.bfloat16
NT = (((1,), (1,)), ((), ()))
TN = (((0,), (0,)), ((), ()))

CHUNKS = 4


def layer_kernel(
    n_fs, n_tp,
    tok, gain, w_pool, w_query, w_forget, w_value, maps, scale, low, spike, hgain, w_po, w_ro,
    out,
    tbuf, stage, wbuf, nbuf, sbuf, proj, pool_g, rec_g, wo, map_v, pacc, part, dbuf, summed, obuf,
    ld, w_s, w_r, wt_s, wt_r, sp_s, sp_r, tz_s, tz_r, tq_s, td_s, td_r,
    wo_s, wo_r, ot_s, ot_r, pg_s, pg_r, pq_s, rg_s, rg_r, rq_s, d_s, d_r, o_s, o_r,
):
    s = lax.axis_index("sp")
    f = lax.axis_index("fs")
    t = lax.axis_index("tp")
    n_sp = 4
    rows = tok.shape[0]
    depth = w_pool.shape[0]
    width = w_pool.shape[1] // n_sp
    cols = w_po.shape[1]
    piece = depth // n_fs
    half = piece // 2
    strip = n_tp * rows
    length = n_sp * strip
    weights = (w_pool, w_query, w_forget, w_value)

    side = s // 2
    end, mid, omid, oend = 3 * side, 1 + side, 2 - side, 3 - 3 * side
    mate = end + mid - s
    is_end, is_mid = s == end, s == mid
    peers = (mate, omid, oend)

    def z(o):
        return {"sp": o, "fs": f, "tp": t}

    at_x = {"sp": s, "fs": f + 1 - 2 * lax.rem(f, 2), "tp": t}
    at_y = {"sp": s, "fs": f + 2 - 4 * (f // 2), "tp": t}
    other = {"sp": s, "fs": f, "tp": 1 - t}
    f_x, f_y, f_d = at_x["fs"], at_y["fs"], 3 - f

    def ds(start, size):
        return pl.ds(pl.multiple_of(start, size), size)

    def remote(src, dst, ssem, rsem, dev):
        return pltpu.make_async_remote_copy(
            src_ref=src, dst_ref=dst, send_sem=ssem, recv_sem=rsem,
            device_id=dev, device_id_type=pl.DeviceIdType.MESH,
        )

    drains = []

    def send(copy, cond=None, drain_cond=None):
        if cond is None:
            copy.start()
        else:
            pl.when(cond)(copy.start)
        drains.append((drain_cond if cond is None else cond, copy))

    def load(src, dst, i):
        copy = pltpu.make_async_copy(src, dst, ld.at[i])
        copy.start()
        return copy

    tok_load = load(tok, tbuf, 0)
    stage_loads = [
        [
            load(
                weights[m].at[ds(f * piece, piece), ds(dest * width, width)],
                stage.at[j, :, pl.ds(m * width, width)],
                1 + 4 * j + m,
            )
            for m in range(4)
        ]
        for j, dest in enumerate(peers)
    ]
    own_loads = [
        load(
            weights[m].at[:, ds(s * width, width)],
            wbuf.at[ds(s * depth, depth), pl.ds(m * width, width)],
            13 + m,
        )
        for m in range(4)
    ]
    late_loads = [
        load(maps, map_v, 17),
        load(w_po, wo.at[0, :, ds(lax.rem(s, 2) * cols, cols)], 18),
        load(w_ro, wo.at[1, :, ds(lax.rem(s, 2) * cols, cols)], 19),
    ]

    barrier = pltpu.get_barrier_semaphore()
    partners = [z(o) for o in peers] + [at_x, at_y, other]
    for dev in partners:
        pl.semaphore_signal(barrier, inc=1, device_id=dev, device_id_type=pl.DeviceIdType.MESH)
    pl.semaphore_wait(barrier, len(partners))

    def w_view(o, giver, h=None):
        if h is None:
            return wbuf.at[ds(o * depth + giver * piece, piece), :]
        return wbuf.at[ds(o * depth + giver * piece + h * half, half), :]

    def wo_view(k, giver, h=None):
        place = ds(lax.rem(end, 2) * cols, cols)
        if h is None:
            return wo.at[k, ds(giver * piece, piece), place]
        return wo.at[k, ds(giver * piece + h * half, half), place]

    def tree(view, ssem, rsem):
        def first(i, o):
            mine = view(o, f)
            send(remote(mine, mine, ssem.at[0, i], rsem.at[0, i], at_x))
            send(remote(mine, mine, ssem.at[1, i], rsem.at[1, i], at_y))

        def second(i, o):
            got = view(o, f_x)
            remote(got, got, ssem.at[0, i], rsem.at[0, i], at_x).wait_recv()
            on = view(o, f_x, 0)
            send(remote(on, on, ssem.at[2, i], rsem.at[2, i], at_y))
            got = view(o, f_y)
            remote(got, got, ssem.at[1, i], rsem.at[1, i], at_y).wait_recv()
            on = view(o, f_y, 1)
            send(remote(on, on, ssem.at[3, i], rsem.at[3, i], at_x))

        def last(i, o):
            got = view(o, f_d, 0)
            remote(got, got, ssem.at[2, i], rsem.at[2, i], at_y).wait_recv()
            got = view(o, f_d, 1)
            remote(got, got, ssem.at[3, i], rsem.at[3, i], at_x).wait_recv()

        return first, second, last

    for j, dest in enumerate(peers):
        for copy in stage_loads[j]:
            copy.wait()
        send(remote(stage.at[j], w_view(s, f), w_s.at[j], w_r.at[s], z(dest)))
    for j, dest in enumerate(peers):
        send(remote(spike, sbuf.at[s], sp_s.at[j], sp_r.at[s], z(dest)))

    chunk = rows // CHUNKS

    def tok_view(o, core, c):
        return nbuf.at[o, core, pl.ds(c * chunk, chunk), :]

    def core_pass(o, c):
        view = tok_view(o, t, c)
        send(remote(view, view, td_s.at[o, c], td_r.at[o, c], other))

    def core_arrival(o):
        for c in range(CHUNKS):
            view = tok_view(o, 1 - t, c)
            remote(view, view, td_s.at[o, c], td_r.at[o, c], other).wait_recv()

    def tok_arrival(o, c):
        view = tok_view(o, t, c)
        remote(view, view, tz_s.at[0, c], tz_r.at[o, c], z(o)).wait_recv()

    tok_load.wait()
    gain_row = gain[...]
    x = tbuf[...].astype(F32)
    y = x * lax.rsqrt(jnp.mean(x * x, axis=-1, keepdims=True) + EPSILON) * gain_row
    nbuf[s, t] = y.astype(BF16)
    for j, dest in enumerate((omid, mate)):
        for c in range(CHUNKS):
            view = tok_view(s, t, c)
            send(remote(view, view, tz_s.at[j, c], tz_r.at[s, c], z(dest)))
    for c in range(CHUNKS):
        core_pass(s, c)
    for k, w_out in enumerate((w_po, w_ro)):
        dst = wo.at[k, ds(f * piece, piece), ds(lax.rem(s, 2) * cols, cols)]
        send(remote(w_out.at[ds(f * piece, piece), :], dst, wo_s.at[k], wo_r.at[k], z(mid)), is_end)
    sbuf[s] = spike[...]

    first, second, last = tree(w_view, wt_s, wt_r)

    def w_arrival(j):
        view = w_view(peers[j], f)
        remote(view, view, w_s.at[j], w_r.at[peers[j]], z(peers[j])).wait_recv()

    w_arrival(0)
    first(0, peers[0])
    w_arrival(1)
    first(1, peers[1])
    second(0, peers[0])
    w_arrival(2)
    first(2, peers[2])
    second(1, peers[1])
    second(2, peers[2])

    far = (omid, oend)
    relays = [
        [remote(tok_view(o, t, c), tok_view(o, t, c), tq_s.at[k, c], tz_r.at[o, c], z(end)) for c in range(CHUNKS)]
        for k, o in enumerate(far)
    ]
    passes = [
        [remote(tok_view(o, t, c), tok_view(o, t, c), td_s.at[o, c], td_r.at[o, c], other) for c in range(CHUNKS)]
        for o in far
    ]

    @pl.when(is_mid)
    def _():
        for c in range(CHUNKS):
            for k, o in enumerate(far):
                tok_arrival(o, c)
                relays[k][c].start()
                passes[k][c].start()

    for c in range(CHUNKS):
        tok_arrival(mate, c)
        core_pass(mate, c)
    for j in range(3):
        last(j, peers[j])
    for copy in own_loads:
        copy.wait()
    core_arrival(s)
    core_arrival(mate)

    def project(base):
        x = nbuf[pl.ds(base, 2)].reshape(2 * strip, nbuf.shape[3])
        y = jnp.dot(x, wbuf[...], preferred_element_type=F32)
        proj[pl.ds(base, 2)] = y.astype(BF16).reshape(2, strip, 4 * width)

    project(2 * side)

    @pl.when(is_end)
    def _():
        for c in range(CHUNKS):
            for k, o in enumerate(far):
                tok_arrival(o, c)
                passes[k][c].start()

    core_arrival(omid)
    core_arrival(oend)
    project(2 - 2 * side)
    for k in range(2):
        for c in range(CHUNKS):
            drains.append((is_mid, relays[k][c]))
            drains.append((None, passes[k][c]))

    target = 1 + lax.rem(s, 2)
    projected = proj[...].reshape(length, 4 * width)
    x = projected[:, :width].astype(F32)
    group_size = maps.shape[1]
    groups = maps.shape[0]
    share = group_size // width
    group = t * groups + s // share
    position = lax.broadcasted_iota(jnp.int32, (length, width), 0)
    total = x
    window_sum = x
    window = jnp.int32(2)
    for g in range(n_tp * groups):
        reach = 2 ** g
        total = total + jnp.concatenate([jnp.zeros((reach, width), F32), total[: length - reach]], axis=0)
        window_sum = total if g == 0 else jnp.where(group == g, total, window_sum)
    for g in range(1, n_tp * groups):
        window = jnp.where(group == g, 2 ** (g + 1), window)
    counts = jnp.minimum(position + 1, window).astype(F32)
    pool_g[s] = (window_sum / counts - x).astype(BF16)
    send(remote(pool_g.at[s], pool_g.at[s], pg_s.at[0], pg_r.at[s], z(target)))

    wo_first, wo_second, wo_last = tree(wo_view, ot_s, ot_r)
    tree_from = len(drains)

    @pl.when(is_mid)
    def _():
        for copy in late_loads[1:]:
            copy.wait()
        for k in range(2):
            view = wo_view(k, f)
            remote(view, view, wo_s.at[k], wo_r.at[k], z(end)).wait_recv()
            mine = wo_view(k, f)
            remote(mine, mine, ot_s.at[0, k], ot_r.at[0, k], at_x).start()
            remote(mine, mine, ot_s.at[1, k], ot_r.at[1, k], at_y).start()

    for d in range(1, n_sp):
        o = lax.rem(s + d, n_sp)
        remote(spike, sbuf.at[o], sp_s.at[d - 1], sp_r.at[o], z(o)).wait_recv()
    lows = low[s]
    tri_r = lax.broadcasted_iota(jnp.int32, (BLOCK, BLOCK), 0)
    tri_c = lax.broadcasted_iota(jnp.int32, (BLOCK, BLOCK), 1)
    causal = tri_r >= tri_c
    tri = causal.astype(F32)
    gate_low = jax.nn.sigmoid(-lows)
    state = jnp.zeros((width, width), F32)
    columns = [jnp.transpose(jnp.broadcast_to(sbuf[o, pl.ds(s, 1)], (8, strip)))[:, :1] for o in range(n_sp)]
    for b in range(length // BLOCK):
        lo = b * BLOCK
        here = slice(lo, lo + BLOCK)
        q = projected[here, width:2 * width].astype(F32)
        logit = projected[here, 2 * width:3 * width].astype(F32)
        v = projected[here, 3 * width:]
        reader = q * jax.nn.sigmoid(q)
        key = gate_low * jax.nn.sigmoid(-logit)
        off = lo % strip
        logs = jnp.log1p(-key) + columns[lo // strip][off:off + BLOCK]
        inner = jnp.dot(tri, logs, preferred_element_type=F32, precision=HIGHEST)
        read_scaled = (reader * jnp.exp(inner)).astype(BF16)
        key_scaled = (key * jnp.exp(-inner)).astype(BF16)
        scores = lax.dot_general(read_scaled, key_scaled, NT, preferred_element_type=F32)
        scores = jnp.where(causal, scores, 0.0).astype(BF16)
        read = jnp.dot(scores, v, preferred_element_type=F32)
        read = read + lax.dot_general(read_scaled, state.astype(BF16), NT, preferred_element_type=F32)
        closing = inner[BLOCK - 1:]
        key_tail = (key * jnp.exp(closing - inner)).astype(BF16)
        state = jnp.exp(closing) * state + lax.dot_general(v, key_tail, TN, preferred_element_type=F32)
        rec = read * lax.rsqrt(jnp.mean(read * read, axis=-1, keepdims=True) + EPSILON) * hgain[s]
        rec_g[s, lo:lo + BLOCK] = rec.astype(BF16)

    def rec_view(o, p):
        return rec_g.at[o, ds(p * strip, strip), :]

    order = (oend, end, omid, mid)
    for p in order:
        view = rec_view(s, p)
        send(remote(view, view, rg_s.at[p], rg_r.at[s, p], z(target)))

    def pool_arrival(o):
        view = pool_g.at[o]
        remote(view, view, pg_s.at[0], pg_r.at[o], z(o)).wait_recv()

    def rec_arrival(o, p):
        view = rec_view(o, p)
        remote(view, view, rg_s.at[p], rg_r.at[o, p], z(o)).wait_recv()

    pool_relay = remote(pool_g.at[end], pool_g.at[end], pq_s.at[0], pg_r.at[end], z(omid))
    rec_relays = [
        remote(rec_view(end, p), rec_view(end, p), rq_s.at[p], rg_r.at[end, p], z(omid)) for p in order
    ]
    blocks = (oend, omid, end, mid)

    def across(i):
        return remote(part.at[i, 1 - t], dbuf.at[i], d_s.at[i], d_r.at[i], other)

    def deliver(i):
        return remote(summed.at[i], obuf.at[side], o_s.at[i], o_r.at[side], z(blocks[i]))

    @pl.when(is_mid)
    def _():
        pool_arrival(end)
        pool_relay.start()
        for k in range(2):
            mark = len(drains)
            wo_second(k, k)
            del drains[mark:]
        for i, p in enumerate(order):
            rec_arrival(end, p)
            rec_relays[i].start()
        late_loads[0].wait()
        for k in range(2):
            wo_last(k, k)
        pool_arrival(omid)
        pool_arrival(oend)
        mixed = []
        for g in range(groups):
            diff = jnp.concatenate([pool_g[g * share + c] for c in range(share)], axis=1)
            mapped = jnp.dot(diff, map_v[g], preferred_element_type=F32)
            mixed.append((mapped * scale[:, g * group_size:(g + 1) * group_size]).astype(BF16))
        pacc[...] = jnp.dot(jnp.concatenate(mixed, axis=1), wo[0], preferred_element_type=F32)

        def settle(i):
            across(i).wait_recv()
            both = (part[i, t].astype(F32) + dbuf[i].astype(F32)).astype(BF16)
            if i < 3:
                summed[i] = both
                deliver(i).start()
            else:
                obuf[side] = both

        for i, p in enumerate(blocks):
            rec_arrival(omid, p)
            rec_arrival(oend, p)
            recs = jnp.concatenate([rec_g[c, ds(p * strip, strip), :] for c in range(n_sp)], axis=1)
            acc = pacc[ds(p * strip, strip), :] + jnp.dot(recs, wo[1], preferred_element_type=F32)
            acc = acc.astype(BF16)
            for core in range(n_tp):
                part[i, core] = acc[core * rows:(core + 1) * rows]
            across(i).start()
            if i > 0:
                settle(i - 1)
        settle(3)

    @pl.when(is_end)
    def _():
        for copy in late_loads:
            copy.wait()
        view = obuf.at[side]
        remote(view, view, o_s.at[0], o_r.at[side], z(mid)).wait_recv()

    view = obuf.at[1 - side]
    remote(view, view, o_s.at[0], o_r.at[1 - side], z(omid)).wait_recv()
    for h in range(2):
        out[:, 2 * h * cols:2 * (h + 1) * cols] = obuf[h]

    for cond, copy in drains:
        if cond is None:
            copy.wait_send()
        else:
            pl.when(cond)(copy.wait_send)

    @pl.when(is_mid)
    def _():
        pool_relay.wait_send()
        for copy in rec_relays:
            copy.wait_send()
        for i in range(4):
            across(i).wait_send()
        for i in range(3):
            deliver(i).wait_send()
        for k in range(2):
            mine = wo_view(k, f)
            remote(mine, mine, ot_s.at[0, k], ot_r.at[0, k], at_x).wait_send()
            remote(mine, mine, ot_s.at[1, k], ot_r.at[1, k], at_y).wait_send()
            on = wo_view(k, f_x, 0)
            remote(on, on, ot_s.at[2, k], ot_r.at[2, k], at_y).wait_send()
            on = wo_view(k, f_y, 1)
            remote(on, on, ot_s.at[3, k], ot_r.at[3, k], at_x).wait_send()


def head_body(sizes, *args):
    (tokens, gain, w_pool, w_query, w_forget, w_value, maps, scale, low, spike, hgain, w_po, w_ro) = args
    n_sp, n_fs, n_tp = sizes
    tok = tokens[0]
    rows, features = tok.shape
    depth = w_pool.shape[0]
    width = w_pool.shape[1] // n_sp
    length = n_sp * n_tp * rows
    cols = w_po.shape[1]
    dma = pltpu.SemaphoreType.DMA
    whole = pl.BlockSpec(memory_space=pltpu.VMEM)
    here = pl.BlockSpec(memory_space=pl.ANY)
    result = pl.pallas_call(
        functools.partial(layer_kernel, n_fs, n_tp),
        out_shape=jax.ShapeDtypeStruct((rows, n_sp * cols), BF16),
        in_specs=[here, whole, here, here, here, here, here, whole, whole, whole, whole, here, here],
        out_specs=whole,
        scratch_shapes=[
            pltpu.VMEM((rows, features), BF16),
            pltpu.VMEM((3, depth // n_fs, 4 * width), BF16),
            pltpu.VMEM((features, 4 * width), BF16),
            pltpu.VMEM((n_sp, n_tp, rows, features), BF16),
            pltpu.VMEM((n_sp,) + (spike.shape[2], spike.shape[1]), F32),
            pltpu.VMEM((n_sp, n_tp * rows, 4 * width), BF16),
            pltpu.VMEM((n_sp, length, width), BF16),
            pltpu.VMEM((n_sp, length, width), BF16),
            pltpu.VMEM((2, w_po.shape[0], 2 * cols), BF16),
            pltpu.VMEM(maps.shape, BF16),
            pltpu.VMEM((length, 2 * cols), F32),
            pltpu.VMEM((n_sp, n_tp, rows, 2 * cols), BF16),
            pltpu.VMEM((n_sp, rows, 2 * cols), BF16),
            pltpu.VMEM((n_sp, rows, 2 * cols), BF16),
            pltpu.VMEM((2, rows, 2 * cols), BF16),
            dma((20,)),
            dma((3,)), dma((n_sp,)),
            dma((4, 3)), dma((4, 3)),
            dma((3,)), dma((n_sp,)),
            dma((2, CHUNKS)), dma((n_sp, CHUNKS)), dma((2, CHUNKS)),
            dma((n_sp, CHUNKS)), dma((n_sp, CHUNKS)),
            dma((2,)), dma((2,)),
            dma((4, 2)), dma((4, 2)),
            dma((1,)), dma((n_sp,)), dma((1,)),
            dma((n_sp,)), dma((n_sp, n_sp)), dma((n_sp,)),
            dma((n_sp,)), dma((n_sp,)),
            dma((n_sp,)), dma((2,)),
        ],
        compiler_params=pltpu.CompilerParams(
            collective_id=0, has_side_effects=True, vmem_limit_bytes=56 * 1024 * 1024
        ),
        name="layer",
    )(
        tok, gain[None], w_pool, w_query, w_forget, w_value, maps, scale[None],
        low.reshape(n_sp, 1, width), spike[0].T, hgain.reshape(n_sp, 1, width), w_po, w_ro,
    )
    return result[None]


def solution(mesh):
    placed = (
        P("fs", ("sp", "tp"), None),
        P(),
        P("sp", "tp"),
        P("sp", "tp"),
        P("sp", "tp"),
        P("sp", "tp"),
        P("tp", None, None),
        P("tp"),
        P("tp"),
        P("fs", "sp", "tp"),
        P("tp"),
        P("tp", "sp"),
        P("tp", "sp"),
    )
    sizes = (mesh.shape["sp"], mesh.shape["fs"], mesh.shape["tp"])

    def one(*args):
        maps, spike = args[6], args[9]
        width = args[2].shape[1] // sizes[0]
        fits = spike.shape[2] == sizes[0] and sizes == (4, 4, 2) and width % 128 == 0
        fits = fits and args[3].shape[1] == args[2].shape[1] and maps.shape[1] % width == 0
        return head_body(sizes, *args) if fits else body(*args)

    return jax.shard_map(
        one, mesh=mesh, in_specs=placed, out_specs=P("fs", ("sp", "tp"), None), check_vma=False
    )
```

```python
import functools

import jax
import jax.numpy as jnp
from jax import lax
from jax.experimental import pallas as pl
from jax.experimental.pallas import tpu as pltpu
from jax.sharding import PartitionSpec as P

BLOCK = 64


EPSILON = 1e-06
HIGHEST = lax.Precision.HIGHEST


def shifted(value, axis, steps):
    count = lax.axis_size(axis)
    first, last = (max(0, -steps), min(count, count - steps))
    return lax.ppermute(value, axis, [(source, source + steps) for source in range(first, last)])


def entering(shard, axis, join, neutral):
    place = lax.axis_index(axis)
    gathered = jax.tree.map(
        lambda a, kind: lax.all_gather(a.astype(kind), axis), shard, (jnp.bfloat16, jnp.bfloat16)
    )
    state = jax.tree.map(lambda a, e: jnp.zeros_like(a) + jnp.asarray(e, a.dtype), shard, neutral)

    def one(step, state):
        return join(
            state,
            jax.tree.map(
                lambda a, own: lax.dynamic_index_in_dim(a, step, 0, False).astype(own.dtype),
                gathered,
                shard,
            ),
        )

    return lax.fori_loop(0, place, one, state)


def rms_scale(values, gain):
    return values * lax.rsqrt(jnp.mean(values * values, axis=-1, keepdims=True) + EPSILON) * gain


def join_state(earlier, later):
    decay_one, state_one = earlier
    decay_two, state_two = later
    return (decay_one * decay_two, decay_two[..., None] * state_one + state_two)


def body(
    tokens,
    input_norm_gain,
    pooling_input_weight,
    query_weight,
    forget_weight,
    value_weight,
    pooling_group_maps,
    pooling_scale,
    lower_bound_logits,
    decay_spike,
    head_norm_gain,
    pooling_output_weight,
    recurrent_output_weight,
):
    gathered = lax.all_gather(tokens, "tp", axis=1, tiled=True)[0]
    length_total = gathered.shape[0]
    normed = rms_scale(gathered.astype(jnp.float32), input_norm_gain).astype(jnp.bfloat16)
    pool_width = pooling_input_weight.shape[1]
    rec_width = query_weight.shape[1]
    stacked = jnp.concatenate(
        [pooling_input_weight, query_weight, forget_weight, value_weight], axis=1
    )
    out_local = jnp.concatenate([pooling_output_weight, recurrent_output_weight], axis=0)
    groups_fs = lax.axis_size("fs")
    member = lax.axis_index("fs")
    slice_width = stacked.shape[1] // groups_fs
    own_slice = lax.dynamic_slice_in_dim(stacked, member * slice_width, slice_width, 1)
    column_part = lax.all_gather(own_slice, "sp", axis=0, tiled=True)
    full_input = lax.all_gather(column_part, "fs", axis=1, tiled=True)
    projected = jnp.dot(normed, full_input, preferred_element_type=jnp.float32)
    slice_height = out_local.shape[0] // groups_fs
    own_rows = lax.dynamic_slice_in_dim(out_local, member * slice_height, slice_height, 0)
    row_part = lax.all_gather(own_rows, "sp", axis=1, tiled=True)
    out_full = lax.all_gather(row_part, "fs", axis=0, tiled=True)
    rounded = lax.optimization_barrier(projected.astype(jnp.bfloat16))
    pool_input = rounded[:, :pool_width]
    query_matrix = rounded[:, pool_width : pool_width + rec_width].astype(jnp.float32)
    forget_gate_logit = rounded[:, pool_width + rec_width : pool_width + 2 * rec_width].astype(
        jnp.float32
    )
    value_projected = rounded[:, pool_width + 2 * rec_width :].astype(jnp.float32)
    groups_local = pooling_group_maps.shape[0]
    group_size = pooling_group_maps.shape[1]
    reach_rows = 2 ** (groups_local * lax.axis_size("tp"))
    previous = shifted(pool_input[length_total - reach_rows :], "sp", 1)
    extended = jnp.concatenate([previous, pool_input], axis=0).astype(jnp.float32)
    extended = extended.reshape(reach_rows + length_total, groups_local, group_size)
    group_ids = lax.axis_index("tp") * groups_local + jnp.arange(groups_local, dtype=jnp.int32)
    windows = jnp.left_shift(jnp.int32(2), group_ids)
    window_sum = jnp.zeros((length_total, groups_local, group_size), jnp.float32)
    for offset in range(reach_rows):
        inside = (offset < windows).astype(jnp.float32)
        window_sum = (
            window_sum
            + extended[reach_rows - offset : reach_rows - offset + length_total] * inside[:, None]
        )
    position_index = lax.axis_index("sp") * length_total + jnp.arange(length_total, dtype=jnp.int32)
    counts = jnp.minimum(position_index[:, None] + 1, windows[None, :]).astype(jnp.float32)
    pool_diff = (window_sum / counts[:, :, None] - extended[reach_rows:]).astype(jnp.bfloat16)
    pool_mapped = jnp.einsum(
        "tgc,gcd->tgd", pool_diff, pooling_group_maps, preferred_element_type=jnp.float32
    )
    pool_out = (pool_mapped.reshape(length_total, pool_width) * pooling_scale).astype(jnp.bfloat16)
    local_heads = decay_spike.shape[2]
    head_width = rec_width // local_heads
    blocks = length_total // BLOCK
    block_layout = (blocks, BLOCK, local_heads, head_width)
    reader = jax.nn.silu(query_matrix).reshape(block_layout)
    key_gate_value = jax.nn.sigmoid(-lower_bound_logits) * jax.nn.sigmoid(-forget_gate_logit)
    decay_logarithm = (
        jnp.log1p(-key_gate_value).reshape(length_total, local_heads, head_width)
        + decay_spike[0][:, :, None]
    ).reshape(block_layout)
    key_rows = key_gate_value.reshape(block_layout)
    value_rows = value_projected.reshape(block_layout)
    inner_log = jnp.cumsum(decay_logarithm, axis=1)
    read_scaled = reader * jnp.exp(inner_log)
    key_scaled = key_rows * jnp.exp(-inner_log)
    causal = (jnp.arange(BLOCK)[:, None] >= jnp.arange(BLOCK)[None, :]).astype(jnp.float32)
    scores = jnp.einsum("nthd,nshd->nhts", read_scaled, key_scaled, precision=HIGHEST) * causal
    within = jnp.einsum("nhts,nshe->nthe", scores, value_rows, precision=HIGHEST)
    closing = inner_log[:, -1]
    key_tail = key_rows * jnp.exp(closing[:, None] - inner_log)
    deltas = jnp.einsum("nshd,nshe->nhde", key_tail, value_rows, precision=HIGHEST)
    block_decay = jnp.exp(closing)

    def advance(carried, input_batch):
        decay_now, delta_now = input_batch
        return (decay_now[..., None] * carried + delta_now, carried)

    initial = jnp.zeros((local_heads, head_width, head_width), jnp.float32)
    device_state, entry_states = lax.scan(advance, initial, (block_decay, deltas))
    device_decay = jnp.exp(jnp.sum(closing, axis=0))
    scanned = entering(
        (device_decay, device_state),
        "sp",
        join_state,
        (jnp.ones_like(device_decay), jnp.zeros_like(device_state)),
    )
    prior_state = scanned[1]
    before = jnp.cumsum(closing, axis=0) - closing
    start_states = entry_states + jnp.exp(before)[..., None] * prior_state[None]
    read_out = within + jnp.einsum("nthd,nhde->nthe", read_scaled, start_states, precision=HIGHEST)
    read_out = read_out.reshape(length_total, local_heads, head_width)
    recurrent_output = (
        rms_scale(read_out, 1.0).reshape(length_total, rec_width) * head_norm_gain
    ).astype(jnp.bfloat16)
    mixed_rows = jnp.concatenate([pool_out, recurrent_output], axis=1)
    summed = lax.psum_scatter(
        jnp.dot(mixed_rows, out_full, preferred_element_type=jnp.float32).astype(jnp.bfloat16),
        "tp",
        scatter_dimension=0,
        tiled=True,
    )
    return summed[None]


F32 = jnp.float32
BF16 = jnp.bfloat16
NT = (((1,), (1,)), ((), ()))
TN = (((0,), (0,)), ((), ()))

CHUNKS = 4


def layer_kernel(
    n_fs, n_tp,
    tok, gain, w_pool, w_query, w_forget, w_value, maps, scale, low, spike, hgain, w_po, w_ro,
    out,
    tbuf, stage, wbuf, nbuf, sbuf, proj, pool_g, rec_g, wo, map_v, pacc, part, dbuf, summed, obuf,
    ld, w_s, w_r, wt_s, wt_r, sp_s, sp_r, tz_s, tz_r, tq_s, td_s, td_r,
    wo_s, wo_r, ot_s, ot_r, pg_s, pg_r, pq_s, rg_s, rg_r, rq_s, d_s, d_r, o_s, o_r,
):
    s = lax.axis_index("sp")
    f = lax.axis_index("fs")
    t = lax.axis_index("tp")
    n_sp = 4
    rows = tok.shape[0]
    depth = w_pool.shape[0]
    width = w_pool.shape[1] // n_sp
    cols = w_po.shape[1]
    piece = depth // n_fs
    half = piece // 2
    strip = n_tp * rows
    length = n_sp * strip
    weights = (w_pool, w_query, w_forget, w_value)

    side = s // 2
    end, mid, omid, oend = 3 * side, 1 + side, 2 - side, 3 - 3 * side
    mate = end + mid - s
    is_end, is_mid = s == end, s == mid
    peers = (mate, omid, oend)

    def z(o):
        return {"sp": o, "fs": f, "tp": t}

    at_x = {"sp": s, "fs": f + 1 - 2 * lax.rem(f, 2), "tp": t}
    at_y = {"sp": s, "fs": f + 2 - 4 * (f // 2), "tp": t}
    other = {"sp": s, "fs": f, "tp": 1 - t}
    f_x, f_y, f_d = at_x["fs"], at_y["fs"], 3 - f

    def ds(start, size):
        return pl.ds(pl.multiple_of(start, size), size)

    def remote(src, dst, ssem, rsem, dev):
        return pltpu.make_async_remote_copy(
            src_ref=src, dst_ref=dst, send_sem=ssem, recv_sem=rsem,
            device_id=dev, device_id_type=pl.DeviceIdType.MESH,
        )

    drains = []

    def send(copy, cond=None, drain_cond=None):
        if cond is None:
            copy.start()
        else:
            pl.when(cond)(copy.start)
        drains.append((drain_cond if cond is None else cond, copy))

    def load(src, dst, i):
        copy = pltpu.make_async_copy(src, dst, ld.at[i])
        copy.start()
        return copy

    tok_load = load(tok, tbuf, 0)
    stage_loads = [
        [
            load(
                weights[m].at[ds(f * piece, piece), ds(dest * width, width)],
                stage.at[j, :, pl.ds(m * width, width)],
                1 + 4 * j + m,
            )
            for m in range(4)
        ]
        for j, dest in enumerate(peers)
    ]
    own_loads = [
        load(
            weights[m].at[:, ds(s * width, width)],
            wbuf.at[ds(s * depth, depth), pl.ds(m * width, width)],
            13 + m,
        )
        for m in range(4)
    ]
    late_loads = [
        load(maps, map_v, 17),
        load(w_po, wo.at[0, :, ds(lax.rem(s, 2) * cols, cols)], 18),
        load(w_ro, wo.at[1, :, ds(lax.rem(s, 2) * cols, cols)], 19),
    ]

    barrier = pltpu.get_barrier_semaphore()
    partners = [z(o) for o in peers] + [at_x, at_y, other]
    for dev in partners:
        pl.semaphore_signal(barrier, inc=1, device_id=dev, device_id_type=pl.DeviceIdType.MESH)
    pl.semaphore_wait(barrier, len(partners))

    def w_view(o, giver, h=None):
        if h is None:
            return wbuf.at[ds(o * depth + giver * piece, piece), :]
        return wbuf.at[ds(o * depth + giver * piece + h * half, half), :]

    def wo_view(k, giver, h=None):
        place = ds(lax.rem(end, 2) * cols, cols)
        if h is None:
            return wo.at[k, ds(giver * piece, piece), place]
        return wo.at[k, ds(giver * piece + h * half, half), place]

    def tree(view, ssem, rsem):
        def first(i, o):
            mine = view(o, f)
            send(remote(mine, mine, ssem.at[0, i], rsem.at[0, i], at_x))
            send(remote(mine, mine, ssem.at[1, i], rsem.at[1, i], at_y))

        def second(i, o):
            got = view(o, f_x)
            remote(got, got, ssem.at[0, i], rsem.at[0, i], at_x).wait_recv()
            on = view(o, f_x, 0)
            send(remote(on, on, ssem.at[2, i], rsem.at[2, i], at_y))
            got = view(o, f_y)
            remote(got, got, ssem.at[1, i], rsem.at[1, i], at_y).wait_recv()
            on = view(o, f_y, 1)
            send(remote(on, on, ssem.at[3, i], rsem.at[3, i], at_x))

        def last(i, o):
            got = view(o, f_d, 0)
            remote(got, got, ssem.at[2, i], rsem.at[2, i], at_y).wait_recv()
            got = view(o, f_d, 1)
            remote(got, got, ssem.at[3, i], rsem.at[3, i], at_x).wait_recv()

        return first, second, last

    w_sends = []
    for j in (0, 2, 1):
        for copy in stage_loads[j]:
            copy.wait()
        w_sends.append(remote(stage.at[j], w_view(s, f), w_s.at[j], w_r.at[s], z(peers[j])))
        w_sends[-1].start()
    for j, dest in enumerate(peers):
        send(remote(spike, sbuf.at[s], sp_s.at[j], sp_r.at[s], z(dest)))

    chunk = rows // CHUNKS

    def tok_view(o, core, c):
        return nbuf.at[o, core, pl.ds(c * chunk, chunk), :]

    def core_pass(o, c):
        view = tok_view(o, t, c)
        send(remote(view, view, td_s.at[o, c], td_r.at[o, c], other))

    def core_arrival(o):
        for c in range(CHUNKS):
            view = tok_view(o, 1 - t, c)
            remote(view, view, td_s.at[o, c], td_r.at[o, c], other).wait_recv()

    def tok_arrival(o, c):
        view = tok_view(o, t, c)
        remote(view, view, tz_s.at[0, c], tz_r.at[o, c], z(o)).wait_recv()

    tok_load.wait()
    gain_row = gain[...]
    x = tbuf[...].astype(F32)
    y = x * lax.rsqrt(jnp.mean(x * x, axis=-1, keepdims=True) + EPSILON) * gain_row
    nbuf[s, t] = y.astype(BF16)
    to_mate = [
        remote(tok_view(s, t, c), tok_view(s, t, c), tz_s.at[1, c], tz_r.at[s, c], z(mate)) for c in range(CHUNKS)
    ]

    @pl.when(is_mid)
    def _():
        for copy in to_mate:
            copy.start()

    for c in range(CHUNKS):
        core_pass(s, c)
    sbuf[s] = spike[...]

    first, second, last = tree(w_view, wt_s, wt_r)

    def w_arrival(j):
        view = w_view(peers[j], f)
        remote(view, view, w_s.at[j], w_r.at[peers[j]], z(peers[j])).wait_recv()

    to_far = [
        remote(tok_view(s, t, c), tok_view(s, t, c), tz_s.at[0, c], tz_r.at[s, c], z(omid)) for c in range(CHUNKS)
    ]
    w_arrival(0)
    first(0, peers[0])
    for k, w_out in enumerate((w_po, w_ro)):
        dst = wo.at[k, ds(f * piece, piece), ds(lax.rem(s, 2) * cols, cols)]
        send(remote(w_out.at[ds(f * piece, piece), :], dst, wo_s.at[k], wo_r.at[k], z(mid)), is_end)
    w_arrival(1)
    first(1, peers[1])

    @pl.when(is_end)
    def _():
        for copy in to_far:
            copy.start()
        for copy in to_mate:
            copy.start()

    second(0, peers[0])

    @pl.when(is_mid)
    def _():
        for copy in to_far:
            copy.start()

    for copy in to_mate + to_far + w_sends:
        drains.append((None, copy))
    far = (omid, oend)
    relays = [
        [remote(tok_view(o, t, c), tok_view(o, t, c), tq_s.at[k, c], tz_r.at[o, c], z(end)) for c in range(CHUNKS)]
        for k, o in enumerate(far)
    ]
    passes = [
        [remote(tok_view(o, t, c), tok_view(o, t, c), td_s.at[o, c], td_r.at[o, c], other) for c in range(CHUNKS)]
        for o in far
    ]

    def relay(c):
        for k, o in enumerate(far):
            tok_arrival(o, c)
            relays[k][c].start()
            passes[k][c].start()

    w_arrival(2)
    first(2, peers[2])
    pl.when(is_mid)(functools.partial(relay, 0))
    second(1, peers[1])
    pl.when(is_mid)(functools.partial(relay, 1))
    second(2, peers[2])

    @pl.when(is_mid)
    def _():
        for c in range(2, CHUNKS):
            relay(c)

    wo_first, wo_second, wo_last = tree(wo_view, ot_s, ot_r)
    tree_from = len(drains)

    @pl.when(is_mid)
    def _():
        for copy in late_loads[1:]:
            copy.wait()
        for k in range(2):
            view = wo_view(k, f)
            remote(view, view, wo_s.at[k], wo_r.at[k], z(end)).wait_recv()
            mine = wo_view(k, f)
            remote(mine, mine, ot_s.at[0, k], ot_r.at[0, k], at_x).start()
            remote(mine, mine, ot_s.at[1, k], ot_r.at[1, k], at_y).start()

    for c in range(CHUNKS):
        tok_arrival(mate, c)
        core_pass(mate, c)
    for j in range(3):
        last(j, peers[j])
    for copy in own_loads:
        copy.wait()
    core_arrival(s)
    core_arrival(mate)

    def project(base):
        x = nbuf[pl.ds(base, 2)].reshape(2 * strip, nbuf.shape[3])
        y = jnp.dot(x, wbuf[...], preferred_element_type=F32)
        proj[pl.ds(base, 2)] = y.astype(BF16).reshape(2, strip, 4 * width)

    project(2 * side)

    @pl.when(is_end)
    def _():
        for c in range(CHUNKS):
            for k, o in enumerate(far):
                tok_arrival(o, c)
                passes[k][c].start()

    core_arrival(omid)
    core_arrival(oend)
    project(2 - 2 * side)
    for k in range(2):
        for c in range(CHUNKS):
            drains.append((is_mid, relays[k][c]))
            drains.append((None, passes[k][c]))

    target = 1 + lax.rem(s, 2)
    projected = proj[...].reshape(length, 4 * width)
    x = projected[:, :width].astype(F32)
    group_size = maps.shape[1]
    groups = maps.shape[0]
    share = group_size // width
    group = t * groups + s // share
    position = lax.broadcasted_iota(jnp.int32, (length, width), 0)
    total = x
    window_sum = x
    window = jnp.int32(2)
    for g in range(n_tp * groups):
        reach = 2 ** g
        total = total + jnp.concatenate([jnp.zeros((reach, width), F32), total[: length - reach]], axis=0)
        window_sum = total if g == 0 else jnp.where(group == g, total, window_sum)
    for g in range(1, n_tp * groups):
        window = jnp.where(group == g, 2 ** (g + 1), window)
    counts = jnp.minimum(position + 1, window).astype(F32)
    pool_g[s] = (window_sum / counts - x).astype(BF16)
    send(remote(pool_g.at[s], pool_g.at[s], pg_s.at[0], pg_r.at[s], z(target)))

    for d in range(1, n_sp):
        o = lax.rem(s + d, n_sp)
        remote(spike, sbuf.at[o], sp_s.at[d - 1], sp_r.at[o], z(o)).wait_recv()
    lows = low[s]
    tri_r = lax.broadcasted_iota(jnp.int32, (BLOCK, BLOCK), 0)
    tri_c = lax.broadcasted_iota(jnp.int32, (BLOCK, BLOCK), 1)
    causal = tri_r >= tri_c
    tri = causal.astype(F32)
    gate_low = jax.nn.sigmoid(-lows)
    state = jnp.zeros((width, width), F32)
    columns = [jnp.transpose(jnp.broadcast_to(sbuf[o, pl.ds(s, 1)], (8, strip)))[:, :1] for o in range(n_sp)]
    for b in range(length // BLOCK):
        lo = b * BLOCK
        here = slice(lo, lo + BLOCK)
        q = projected[here, width:2 * width].astype(F32)
        logit = projected[here, 2 * width:3 * width].astype(F32)
        v = projected[here, 3 * width:]
        reader = q * jax.nn.sigmoid(q)
        key = gate_low * jax.nn.sigmoid(-logit)
        off = lo % strip
        logs = jnp.log1p(-key) + columns[lo // strip][off:off + BLOCK]
        inner = jnp.dot(tri, logs, preferred_element_type=F32, precision=HIGHEST)
        read_scaled = (reader * jnp.exp(inner)).astype(BF16)
        key_scaled = (key * jnp.exp(-inner)).astype(BF16)
        scores = lax.dot_general(read_scaled, key_scaled, NT, preferred_element_type=F32)
        scores = jnp.where(causal, scores, 0.0).astype(BF16)
        read = jnp.dot(scores, v, preferred_element_type=F32)
        read = read + lax.dot_general(read_scaled, state.astype(BF16), NT, preferred_element_type=F32)
        closing = inner[BLOCK - 1:]
        key_tail = (key * jnp.exp(closing - inner)).astype(BF16)
        state = jnp.exp(closing) * state + lax.dot_general(v, key_tail, TN, preferred_element_type=F32)
        rec = read * lax.rsqrt(jnp.mean(read * read, axis=-1, keepdims=True) + EPSILON) * hgain[s]
        rec_g[s, lo:lo + BLOCK] = rec.astype(BF16)

    def rec_view(o, p):
        return rec_g.at[o, ds(p * strip, strip), :]

    order = (oend, end, omid, mid)
    for p in order:
        view = rec_view(s, p)
        send(remote(view, view, rg_s.at[p], rg_r.at[s, p], z(target)))

    def pool_arrival(o):
        view = pool_g.at[o]
        remote(view, view, pg_s.at[0], pg_r.at[o], z(o)).wait_recv()

    def rec_arrival(o, p):
        view = rec_view(o, p)
        remote(view, view, rg_s.at[p], rg_r.at[o, p], z(o)).wait_recv()

    pool_relay = remote(pool_g.at[end], pool_g.at[end], pq_s.at[0], pg_r.at[end], z(omid))
    rec_relays = [
        remote(rec_view(end, p), rec_view(end, p), rq_s.at[p], rg_r.at[end, p], z(omid)) for p in order
    ]
    blocks = (oend, omid, end, mid)

    def across(i):
        return remote(part.at[i, 1 - t], dbuf.at[i], d_s.at[i], d_r.at[i], other)

    def deliver(i):
        return remote(summed.at[i], obuf.at[side], o_s.at[i], o_r.at[side], z(blocks[i]))

    @pl.when(is_mid)
    def _():
        for k in range(2):
            mark = len(drains)
            wo_second(k, k)
            del drains[mark:]
        pool_arrival(end)
        pool_relay.start()
        for i, p in enumerate(order):
            rec_arrival(end, p)
            rec_relays[i].start()
        late_loads[0].wait()
        for k in range(2):
            wo_last(k, k)
        pool_arrival(omid)
        pool_arrival(oend)
        mixed = []
        for g in range(groups):
            diff = jnp.concatenate([pool_g[g * share + c] for c in range(share)], axis=1)
            mapped = jnp.dot(diff, map_v[g], preferred_element_type=F32)
            mixed.append((mapped * scale[:, g * group_size:(g + 1) * group_size]).astype(BF16))
        pacc[...] = jnp.dot(jnp.concatenate(mixed, axis=1), wo[0], preferred_element_type=F32)

        def settle(i):
            across(i).wait_recv()
            both = (part[i, t].astype(F32) + dbuf[i].astype(F32)).astype(BF16)
            if i < 3:
                summed[i] = both
                deliver(i).start()
            else:
                obuf[side] = both

        for i, p in enumerate(blocks):
            rec_arrival(omid, p)
            rec_arrival(oend, p)
            recs = jnp.concatenate([rec_g[c, ds(p * strip, strip), :] for c in range(n_sp)], axis=1)
            acc = pacc[ds(p * strip, strip), :] + jnp.dot(recs, wo[1], preferred_element_type=F32)
            acc = acc.astype(BF16)
            for core in range(n_tp):
                part[i, core] = acc[core * rows:(core + 1) * rows]
            across(i).start()
            if i > 0:
                settle(i - 1)
        settle(3)

    @pl.when(is_end)
    def _():
        for copy in late_loads:
            copy.wait()
        view = obuf.at[side]
        remote(view, view, o_s.at[0], o_r.at[side], z(mid)).wait_recv()

    def store(h):
        return pltpu.make_async_copy(obuf.at[h], out.at[:, ds(2 * h * cols, 2 * cols)], ld.at[20 + h])

    store(side).start()
    view = obuf.at[1 - side]
    remote(view, view, o_s.at[0], o_r.at[1 - side], z(omid)).wait_recv()
    store(1 - side).start()

    for cond, copy in drains:
        if cond is None:
            copy.wait_send()
        else:
            pl.when(cond)(copy.wait_send)

    @pl.when(is_mid)
    def _():
        pool_relay.wait_send()
        for copy in rec_relays:
            copy.wait_send()
        for i in range(4):
            across(i).wait_send()
        for i in range(3):
            deliver(i).wait_send()
        for k in range(2):
            mine = wo_view(k, f)
            remote(mine, mine, ot_s.at[0, k], ot_r.at[0, k], at_x).wait_send()
            remote(mine, mine, ot_s.at[1, k], ot_r.at[1, k], at_y).wait_send()
            on = wo_view(k, f_x, 0)
            remote(on, on, ot_s.at[2, k], ot_r.at[2, k], at_y).wait_send()
            on = wo_view(k, f_y, 1)
            remote(on, on, ot_s.at[3, k], ot_r.at[3, k], at_x).wait_send()

    for h in range(2):
        store(h).wait()


def head_body(sizes, *args):
    (tokens, gain, w_pool, w_query, w_forget, w_value, maps, scale, low, spike, hgain, w_po, w_ro) = args
    n_sp, n_fs, n_tp = sizes
    tok = tokens[0]
    rows, features = tok.shape
    depth = w_pool.shape[0]
    width = w_pool.shape[1] // n_sp
    length = n_sp * n_tp * rows
    cols = w_po.shape[1]
    dma = pltpu.SemaphoreType.DMA
    whole = pl.BlockSpec(memory_space=pltpu.VMEM)
    here = pl.BlockSpec(memory_space=pl.ANY)
    result = pl.pallas_call(
        functools.partial(layer_kernel, n_fs, n_tp),
        out_shape=pltpu.VMEM((rows, n_sp * cols), BF16),
        in_specs=[here, whole, here, here, here, here, here, whole, whole, whole, whole, here, here],
        out_specs=whole,
        scratch_shapes=[
            pltpu.VMEM((rows, features), BF16),
            pltpu.VMEM((3, depth // n_fs, 4 * width), BF16),
            pltpu.VMEM((features, 4 * width), BF16),
            pltpu.VMEM((n_sp, n_tp, rows, features), BF16),
            pltpu.VMEM((n_sp,) + (spike.shape[2], spike.shape[1]), F32),
            pltpu.VMEM((n_sp, n_tp * rows, 4 * width), BF16),
            pltpu.VMEM((n_sp, length, width), BF16),
            pltpu.VMEM((n_sp, length, width), BF16),
            pltpu.VMEM((2, w_po.shape[0], 2 * cols), BF16),
            pltpu.VMEM(maps.shape, BF16),
            pltpu.VMEM((length, 2 * cols), F32),
            pltpu.VMEM((n_sp, n_tp, rows, 2 * cols), BF16),
            pltpu.VMEM((n_sp, rows, 2 * cols), BF16),
            pltpu.VMEM((n_sp, rows, 2 * cols), BF16),
            pltpu.VMEM((2, rows, 2 * cols), BF16),
            dma((22,)),
            dma((3,)), dma((n_sp,)),
            dma((4, 3)), dma((4, 3)),
            dma((3,)), dma((n_sp,)),
            dma((2, CHUNKS)), dma((n_sp, CHUNKS)), dma((2, CHUNKS)),
            dma((n_sp, CHUNKS)), dma((n_sp, CHUNKS)),
            dma((2,)), dma((2,)),
            dma((4, 2)), dma((4, 2)),
            dma((1,)), dma((n_sp,)), dma((1,)),
            dma((n_sp,)), dma((n_sp, n_sp)), dma((n_sp,)),
            dma((n_sp,)), dma((n_sp,)),
            dma((n_sp,)), dma((2,)),
        ],
        compiler_params=pltpu.CompilerParams(
            collective_id=0, has_side_effects=True, vmem_limit_bytes=56 * 1024 * 1024
        ),
        name="layer",
    )(
        tok, gain[None], w_pool, w_query, w_forget, w_value, maps, scale[None],
        low.reshape(n_sp, 1, width), spike[0].T, hgain.reshape(n_sp, 1, width), w_po, w_ro,
    )
    return result[None]


def solution(mesh):
    placed = (
        P("fs", ("sp", "tp"), None),
        P(),
        P("sp", "tp"),
        P("sp", "tp"),
        P("sp", "tp"),
        P("sp", "tp"),
        P("tp", None, None),
        P("tp"),
        P("tp"),
        P("fs", "sp", "tp"),
        P("tp"),
        P("tp", "sp"),
        P("tp", "sp"),
    )
    sizes = (mesh.shape["sp"], mesh.shape["fs"], mesh.shape["tp"])

    def one(*args):
        maps, spike = args[6], args[9]
        width = args[2].shape[1] // sizes[0]
        fits = spike.shape[2] == sizes[0] and sizes == (4, 4, 2) and width % 128 == 0
        fits = fits and args[3].shape[1] == args[2].shape[1] and maps.shape[1] % width == 0
        return head_body(sizes, *args) if fits else body(*args)

    return jax.shard_map(
        one, mesh=mesh, in_specs=placed, out_specs=P("fs", ("sp", "tp"), None), check_vma=False
    )
```

```python
import functools

import jax
import jax.numpy as jnp
from jax import lax
from jax.experimental import pallas as pl
from jax.experimental.pallas import tpu as pltpu
from jax.sharding import PartitionSpec as P

BLOCK = 64


EPSILON = 1e-06
HIGHEST = lax.Precision.HIGHEST


def shifted(value, axis, steps):
    count = lax.axis_size(axis)
    first, last = (max(0, -steps), min(count, count - steps))
    return lax.ppermute(value, axis, [(source, source + steps) for source in range(first, last)])


def entering(shard, axis, join, neutral):
    place = lax.axis_index(axis)
    gathered = jax.tree.map(
        lambda a, kind: lax.all_gather(a.astype(kind), axis), shard, (jnp.bfloat16, jnp.bfloat16)
    )
    state = jax.tree.map(lambda a, e: jnp.zeros_like(a) + jnp.asarray(e, a.dtype), shard, neutral)

    def one(step, state):
        return join(
            state,
            jax.tree.map(
                lambda a, own: lax.dynamic_index_in_dim(a, step, 0, False).astype(own.dtype),
                gathered,
                shard,
            ),
        )

    return lax.fori_loop(0, place, one, state)


def rms_scale(values, gain):
    return values * lax.rsqrt(jnp.mean(values * values, axis=-1, keepdims=True) + EPSILON) * gain


def join_state(earlier, later):
    decay_one, state_one = earlier
    decay_two, state_two = later
    return (decay_one * decay_two, decay_two[..., None] * state_one + state_two)


def body(
    tokens,
    input_norm_gain,
    pooling_input_weight,
    query_weight,
    forget_weight,
    value_weight,
    pooling_group_maps,
    pooling_scale,
    lower_bound_logits,
    decay_spike,
    head_norm_gain,
    pooling_output_weight,
    recurrent_output_weight,
):
    gathered = lax.all_gather(tokens, "tp", axis=1, tiled=True)[0]
    length_total = gathered.shape[0]
    normed = rms_scale(gathered.astype(jnp.float32), input_norm_gain).astype(jnp.bfloat16)
    pool_width = pooling_input_weight.shape[1]
    rec_width = query_weight.shape[1]
    stacked = jnp.concatenate(
        [pooling_input_weight, query_weight, forget_weight, value_weight], axis=1
    )
    out_local = jnp.concatenate([pooling_output_weight, recurrent_output_weight], axis=0)
    groups_fs = lax.axis_size("fs")
    member = lax.axis_index("fs")
    slice_width = stacked.shape[1] // groups_fs
    own_slice = lax.dynamic_slice_in_dim(stacked, member * slice_width, slice_width, 1)
    column_part = lax.all_gather(own_slice, "sp", axis=0, tiled=True)
    full_input = lax.all_gather(column_part, "fs", axis=1, tiled=True)
    projected = jnp.dot(normed, full_input, preferred_element_type=jnp.float32)
    slice_height = out_local.shape[0] // groups_fs
    own_rows = lax.dynamic_slice_in_dim(out_local, member * slice_height, slice_height, 0)
    row_part = lax.all_gather(own_rows, "sp", axis=1, tiled=True)
    out_full = lax.all_gather(row_part, "fs", axis=0, tiled=True)
    rounded = lax.optimization_barrier(projected.astype(jnp.bfloat16))
    pool_input = rounded[:, :pool_width]
    query_matrix = rounded[:, pool_width : pool_width + rec_width].astype(jnp.float32)
    forget_gate_logit = rounded[:, pool_width + rec_width : pool_width + 2 * rec_width].astype(
        jnp.float32
    )
    value_projected = rounded[:, pool_width + 2 * rec_width :].astype(jnp.float32)
    groups_local = pooling_group_maps.shape[0]
    group_size = pooling_group_maps.shape[1]
    reach_rows = 2 ** (groups_local * lax.axis_size("tp"))
    previous = shifted(pool_input[length_total - reach_rows :], "sp", 1)
    extended = jnp.concatenate([previous, pool_input], axis=0).astype(jnp.float32)
    extended = extended.reshape(reach_rows + length_total, groups_local, group_size)
    group_ids = lax.axis_index("tp") * groups_local + jnp.arange(groups_local, dtype=jnp.int32)
    windows = jnp.left_shift(jnp.int32(2), group_ids)
    window_sum = jnp.zeros((length_total, groups_local, group_size), jnp.float32)
    for offset in range(reach_rows):
        inside = (offset < windows).astype(jnp.float32)
        window_sum = (
            window_sum
            + extended[reach_rows - offset : reach_rows - offset + length_total] * inside[:, None]
        )
    position_index = lax.axis_index("sp") * length_total + jnp.arange(length_total, dtype=jnp.int32)
    counts = jnp.minimum(position_index[:, None] + 1, windows[None, :]).astype(jnp.float32)
    pool_diff = (window_sum / counts[:, :, None] - extended[reach_rows:]).astype(jnp.bfloat16)
    pool_mapped = jnp.einsum(
        "tgc,gcd->tgd", pool_diff, pooling_group_maps, preferred_element_type=jnp.float32
    )
    pool_out = (pool_mapped.reshape(length_total, pool_width) * pooling_scale).astype(jnp.bfloat16)
    local_heads = decay_spike.shape[2]
    head_width = rec_width // local_heads
    blocks = length_total // BLOCK
    block_layout = (blocks, BLOCK, local_heads, head_width)
    reader = jax.nn.silu(query_matrix).reshape(block_layout)
    key_gate_value = jax.nn.sigmoid(-lower_bound_logits) * jax.nn.sigmoid(-forget_gate_logit)
    decay_logarithm = (
        jnp.log1p(-key_gate_value).reshape(length_total, local_heads, head_width)
        + decay_spike[0][:, :, None]
    ).reshape(block_layout)
    key_rows = key_gate_value.reshape(block_layout)
    value_rows = value_projected.reshape(block_layout)
    inner_log = jnp.cumsum(decay_logarithm, axis=1)
    read_scaled = reader * jnp.exp(inner_log)
    key_scaled = key_rows * jnp.exp(-inner_log)
    causal = (jnp.arange(BLOCK)[:, None] >= jnp.arange(BLOCK)[None, :]).astype(jnp.float32)
    scores = jnp.einsum("nthd,nshd->nhts", read_scaled, key_scaled, precision=HIGHEST) * causal
    within = jnp.einsum("nhts,nshe->nthe", scores, value_rows, precision=HIGHEST)
    closing = inner_log[:, -1]
    key_tail = key_rows * jnp.exp(closing[:, None] - inner_log)
    deltas = jnp.einsum("nshd,nshe->nhde", key_tail, value_rows, precision=HIGHEST)
    block_decay = jnp.exp(closing)

    def advance(carried, input_batch):
        decay_now, delta_now = input_batch
        return (decay_now[..., None] * carried + delta_now, carried)

    initial = jnp.zeros((local_heads, head_width, head_width), jnp.float32)
    device_state, entry_states = lax.scan(advance, initial, (block_decay, deltas))
    device_decay = jnp.exp(jnp.sum(closing, axis=0))
    scanned = entering(
        (device_decay, device_state),
        "sp",
        join_state,
        (jnp.ones_like(device_decay), jnp.zeros_like(device_state)),
    )
    prior_state = scanned[1]
    before = jnp.cumsum(closing, axis=0) - closing
    start_states = entry_states + jnp.exp(before)[..., None] * prior_state[None]
    read_out = within + jnp.einsum("nthd,nhde->nthe", read_scaled, start_states, precision=HIGHEST)
    read_out = read_out.reshape(length_total, local_heads, head_width)
    recurrent_output = (
        rms_scale(read_out, 1.0).reshape(length_total, rec_width) * head_norm_gain
    ).astype(jnp.bfloat16)
    mixed_rows = jnp.concatenate([pool_out, recurrent_output], axis=1)
    summed = lax.psum_scatter(
        jnp.dot(mixed_rows, out_full, preferred_element_type=jnp.float32).astype(jnp.bfloat16),
        "tp",
        scatter_dimension=0,
        tiled=True,
    )
    return summed[None]


F32 = jnp.float32
BF16 = jnp.bfloat16
NT = (((1,), (1,)), ((), ()))
TN = (((0,), (0,)), ((), ()))

CHUNKS = 4


def layer_kernel(
    n_fs, n_tp,
    tok, gain, w_pool, w_query, w_forget, w_value, maps, scale, low, spike, hgain, w_po, w_ro,
    out,
    tbuf, stage, wbuf, nbuf, sbuf, proj, pool_g, rec_g, halo, wo, map_v, part, dbuf, summed, obuf,
    ld, w_s, w_r, wt_s, wt_r, sp_s, sp_r, tf_s, tm_s, tz_r, td_s, td_r,
    wo_s, wo_r, ot_s, ot_r, pg_s, pg_r, pq_s, h_s, h_r, rg_s, rg_r, d_s, d_r, o_s, o_r, gate,
):
    s = lax.axis_index("sp")
    f = lax.axis_index("fs")
    t = lax.axis_index("tp")
    n_sp = 4
    rows = tok.shape[0]
    depth = w_pool.shape[0]
    width = w_pool.shape[1] // n_sp
    cols = w_po.shape[1]
    piece = depth // n_fs
    half = piece // 2
    strip = n_tp * rows
    pair = 2 * width
    reach_rows = halo.shape[1]

    side = s // 2
    end, mid, omid, oend = 3 * side, 1 + side, 2 - side, 3 - 3 * side
    mate = end + mid - s
    is_end, is_mid = s == end, s == mid
    peers = (mate, omid, oend)
    positions = range(n_sp)
    far_side, own_side = 2 - 2 * side, 2 * side

    def z(o):
        return {"sp": o, "fs": f, "tp": t}

    at_x = {"sp": s, "fs": f + 1 - 2 * lax.rem(f, 2), "tp": t}
    at_y = {"sp": s, "fs": f + 2 - 4 * (f // 2), "tp": t}
    other = {"sp": s, "fs": f, "tp": 1 - t}
    f_x, f_y, f_d = at_x["fs"], at_y["fs"], 3 - f

    def ds(start, size):
        return pl.ds(pl.multiple_of(start, size), size)

    def remote(src, dst, ssem, rsem, dev):
        return pltpu.make_async_remote_copy(
            src_ref=src, dst_ref=dst, send_sem=ssem, recv_sem=rsem,
            device_id=dev, device_id_type=pl.DeviceIdType.MESH,
        )

    def moved(view, ssem, rsem, dev):
        return remote(view, view, ssem, rsem, dev)

    def when(cond, action):
        if cond is None:
            action()
        else:
            pl.when(cond)(action)

    def load(src, dst, i, cond=None):
        copy = pltpu.make_async_copy(src, dst, ld.at[i])
        when(cond, copy.start)
        return copy, cond

    def finish(loaded):
        when(loaded[1], loaded[0].wait)

    tok_load = load(tok, tbuf, 0)
    gates = (w_query, w_forget, w_value)
    stage_loads = []
    for j, dest in enumerate(peers):
        group_loads = []
        if j < 2:
            for m, w in enumerate(gates):
                group_loads.append(load(
                    w.at[ds(f * piece, piece), ds((dest // 2) * pair, pair)],
                    stage.at[j, :, pl.ds(m * pair, pair)], 1 + 4 * j + m, is_end if j == 0 else None,
                ))
        if j != 1:
            group_loads.append(load(
                w_pool.at[ds(f * piece, piece), :], stage.at[j, :, pl.ds(0, 2 * pair)],
                4 + 4 * j, is_mid if j == 0 else None,
            ))
        stage_loads.append(group_loads)
    own_rows = ds(s * depth, depth)
    own_loads = [
        load(w.at[:, ds(side * pair, pair)], wbuf.at[own_rows, pl.ds(m * pair, pair)], 13 + m, is_mid)
        for m, w in enumerate(gates)
    ]
    own_loads.append(load(w_pool, wbuf.at[own_rows, pl.ds(0, 2 * pair)], 16, is_end))
    map_load = load(maps, map_v, 17, is_end)
    wo_place = ds(lax.rem(s, 2) * cols, cols)
    wo_loads = [load(w, wo.at[k, :, wo_place], 18 + k, is_mid) for k, w in enumerate((w_po, w_ro))]

    barrier = pltpu.get_barrier_semaphore()
    partners = [z(o) for o in peers] + [at_x, at_y, other]
    for dev in partners:
        pl.semaphore_signal(barrier, inc=1, device_id=dev, device_id_type=pl.DeviceIdType.MESH)
    pl.semaphore_wait(barrier, len(partners))

    def w_send(j, span):
        dst = wbuf.at[ds(s * depth + f * piece, piece), pl.ds(0, span)]
        return remote(stage.at[j, :, pl.ds(0, span)], dst, w_s.at[j], w_r.at[s], z(peers[j]))

    to_mid_mate, to_end_mate = w_send(0, 3 * pair), w_send(0, 2 * pair)
    to_omid, to_oend = w_send(1, 3 * pair), w_send(2, 2 * pair)
    for j in (1, 0):
        for loaded in stage_loads[j]:
            finish(loaded)
    pl.when(is_mid)(to_omid.start)
    pl.when(is_mid)(to_end_mate.start)
    pl.when(is_end)(to_mid_mate.start)
    spike_sends = [remote(spike, sbuf.at[s], sp_s.at[j], sp_r.at[s], z(dest)) for j, dest in enumerate(peers)]
    for copy in spike_sends:
        copy.start()

    chunk = rows // CHUNKS

    def tok_view(o, core, c):
        return nbuf.at[o, core, pl.ds(c * chunk, chunk), :]

    def core_pass(o, c):
        return moved(tok_view(o, t, c), td_s.at[o, c], td_r.at[o, c], other)

    def core_arrival(o):
        for c in range(CHUNKS):
            moved(tok_view(o, 1 - t, c), td_s.at[o, c], td_r.at[o, c], other).wait_recv()

    finish(tok_load)
    x = tbuf[...].astype(F32)
    y = x * lax.rsqrt(jnp.mean(x * x, axis=-1, keepdims=True) + EPSILON) * gain[...]
    nbuf[s, t] = y.astype(BF16)
    to_mate = [moved(tok_view(s, t, c), tm_s.at[c], tz_r.at[s, c], z(mate)) for c in range(CHUNKS)]
    own_pass = [core_pass(s, c) for c in range(CHUNKS)]
    for copy in own_pass:
        copy.start()
    sbuf[s] = spike[...]
    finish(stage_loads[2][0])

    def tree(view, ssem, rsem, log):
        def start(copy):
            copy.start()
            log.append(copy)

        def first(i, o):
            start(moved(view(o, f), ssem.at[0, i], rsem.at[0, i], at_x))
            start(moved(view(o, f), ssem.at[1, i], rsem.at[1, i], at_y))

        def second(i, o):
            moved(view(o, f_x), ssem.at[0, i], rsem.at[0, i], at_x).wait_recv()
            start(moved(view(o, f_x, 0), ssem.at[2, i], rsem.at[2, i], at_y))
            moved(view(o, f_y), ssem.at[1, i], rsem.at[1, i], at_y).wait_recv()
            start(moved(view(o, f_y, 1), ssem.at[3, i], rsem.at[3, i], at_x))

        def last(i, o):
            moved(view(o, f_d, 0), ssem.at[2, i], rsem.at[2, i], at_y).wait_recv()
            moved(view(o, f_d, 1), ssem.at[3, i], rsem.at[3, i], at_x).wait_recv()

        return first, second, last

    def w_tree(span, log):
        def view(o, giver, h=None):
            start, size = o * depth + giver * piece, piece
            if h is not None:
                start, size = start + h * half, half
            return wbuf.at[ds(start, size), pl.ds(0, span)]

        def arrival(j):
            moved(view(peers[j], f), w_s.at[j], w_r.at[peers[j]], z(peers[j])).wait_recv()

        first, second, last = tree(view, wt_s, wt_r, log)
        return (
            arrival,
            lambda j: first(j, peers[j]),
            lambda j: second(j, peers[j]),
            lambda j: last(j, peers[j]),
        )

    def project(base, span):
        x = nbuf[pl.ds(base, 2)].reshape(2 * strip, nbuf.shape[3])
        y = jnp.dot(x, wbuf[:, :span], preferred_element_type=F32)
        proj[pl.ds(base, 2), :, :span] = y.astype(BF16).reshape(2, strip, span)

    def pool_view(p):
        return pool_g.at[ds(p * strip, strip), :]

    own_blocks = (own_side, own_side + 1)
    pool_sends = [moved(pool_view(p), pg_s.at[i], pg_r.at[p], z(mid)) for i, p in enumerate(own_blocks)]
    tok_arrivals = {
        o: [moved(tok_view(p, t, c), tm_s.at[c], tz_r.at[p, c], z(p)) for c in range(CHUNKS)]
        for o, p in (("mate", mate), ("omid", omid), ("oend", oend))
    }

    def store():
        for h in range(2):
            out[:, 2 * h * cols:2 * (h + 1) * cols] = obuf[h]

    def common_drains():
        for copy in spike_sends + own_pass:
            copy.wait_send()

    @pl.when(is_end)
    def _():
        log = []
        arrival, first, second, last = w_tree(2 * pair, log)
        to_mid_mate.wait_send()
        to_omid.start()
        arrival(0)
        first(0)
        to_omid.wait_send()
        to_oend.start()
        second(0)
        to_oend.wait_send()

        @pl.when(t == 0)
        def _():
            pl.semaphore_signal(gate, inc=1, device_id=other, device_id_type=pl.DeviceIdType.MESH)

        @pl.when(t == 1)
        def _():
            pl.semaphore_wait(gate, 1)

        for copy in to_mate:
            copy.start()
        arrival(1)
        first(1)
        arrival(2)
        first(2)
        for copy in to_mate:
            copy.wait_send()
        wo_sends = [
            remote(
                w.at[ds(f * piece, piece), :], wo.at[k, ds(f * piece, piece), wo_place], wo_s.at[k], wo_r.at[k], z(mid)
            )
            for k, w in enumerate((w_po, w_ro))
        ]
        for copy in wo_sends:
            copy.start()
        second(1)
        second(2)
        passes = [core_pass(mate, c) for c in range(CHUNKS)]
        for c in range(CHUNKS):
            tok_arrivals["mate"][c].wait_recv()
            passes[c].start()
        for j in range(3):
            last(j)
        finish(own_loads[3])
        core_arrival(s)
        core_arrival(mate)
        project(own_side, 2 * pair)
        halo_copy = remote(halo.at[0], halo.at[1], h_s.at[0], h_r.at[0], z(oend))

        @pl.when(side == 0)
        def _():
            halo[0] = proj[1, strip - reach_rows:, :2 * pair]
            halo_copy.start()
            halo[1] = jnp.zeros((reach_rows, 2 * pair), BF16)

        finish(map_load)
        groups = maps.shape[0]
        group = t * groups + lax.broadcasted_iota(jnp.int32, (strip, 2 * pair), 1) // pair
        position = lax.broadcasted_iota(jnp.int32, (strip, 2 * pair), 0)
        scale_row = scale[...]

        def pool(i, before):
            x = jnp.concatenate([before, proj[own_side + i, :, :2 * pair]], axis=0).astype(F32)
            total = x
            for g in range(n_tp * groups):
                reach = 2 ** g
                total = total + jnp.concatenate([jnp.zeros((reach, 2 * pair), F32), total[:-reach]], axis=0)
                if g == 0:
                    window_sum = total[reach_rows:]
                    window = jnp.full((strip, 2 * pair), 2, jnp.int32)
                else:
                    window_sum = jnp.where(group == g, total[reach_rows:], window_sum)
                    window = jnp.where(group == g, 2 ** (g + 1), window)
            counts = jnp.minimum((own_side + i) * strip + position + 1, window).astype(F32)
            diff = (window_sum / counts - x[reach_rows:]).astype(BF16)
            mapped = jnp.concatenate(
                [
                    jnp.dot(diff[:, g * pair:(g + 1) * pair], map_v[g], preferred_element_type=F32)
                    for g in range(groups)
                ],
                axis=1,
            )
            pool_g[ds((own_side + i) * strip, strip), :] = (mapped * scale_row).astype(BF16)

        pool(1, proj[own_side, strip - reach_rows:, :2 * pair])

        @pl.when(side == 1)
        def _():
            pool_sends[1].start()
            halo_copy.wait_recv()

        pool(0, halo[1])
        pool_sends[0].start()
        pl.when(side == 0)(pool_sends[1].start)
        for o in range(1, n_sp):
            origin = lax.rem(s + o, n_sp)
            remote(spike, sbuf.at[origin], sp_s.at[o - 1], sp_r.at[origin], z(origin)).wait_recv()
        common_drains()
        for copy in log + passes + wo_sends + pool_sends:
            copy.wait_send()
        pl.when(side == 0)(halo_copy.wait_send)
        moved(obuf.at[1 - side], o_s.at[0], o_r.at[1 - side], z(omid)).wait_recv()
        moved(obuf.at[side], o_s.at[0], o_r.at[side], z(mid)).wait_recv()
        store()

    @pl.when(is_mid)
    def _():
        log = []
        arrival, first, second, last = w_tree(3 * pair, log)
        to_far = [moved(tok_view(s, t, c), tf_s.at[0, c], tz_r.at[s, c], z(omid)) for c in range(CHUNKS)]
        relays = [moved(tok_view(mate, t, c), tf_s.at[1, c], tz_r.at[mate, c], z(omid)) for c in range(CHUNKS)]
        passes = {
            "mate": [core_pass(mate, c) for c in range(CHUNKS)],
            "omid": [core_pass(omid, c) for c in range(CHUNKS)],
            "oend": [core_pass(oend, c) for c in range(CHUNKS)],
        }

        def relay(c):
            tok_arrivals["mate"][c].wait_recv()
            relays[c].start()
            passes["mate"][c].start()

        def receive(o, c):
            tok_arrivals[o][c].wait_recv()
            passes[o][c].start()

        for copy in to_mate:
            copy.start()
        arrival(0)
        first(0)
        to_omid.wait_send()
        to_oend.start()
        arrival(1)
        first(1)
        second(0)
        arrival(2)
        first(2)
        to_oend.wait_send()

        @pl.when(t == 0)
        def _():
            pl.semaphore_signal(gate, inc=1, device_id=other, device_id_type=pl.DeviceIdType.MESH)

        @pl.when(t == 1)
        def _():
            pl.semaphore_wait(gate, 1)

        for copy in to_far:
            copy.start()
        second(1)
        relay(0)
        relay(1)
        relay(2)
        relay(3)
        second(2)
        for c in range(CHUNKS):
            receive("omid", c)
        def wo_view(k, giver, h=None):
            start, size = giver * piece, piece
            if h is not None:
                start, size = start + h * half, half
            return wo.at[k, ds(start, size), ds(lax.rem(end, 2) * cols, cols)]

        wo_first, wo_second, wo_last = tree(wo_view, ot_s, ot_r, log)
        for k in range(2):
            moved(wo_view(k, f), wo_s.at[k], wo_r.at[k], z(end)).wait_recv()
            wo_first(k, k)
        for c in range(CHUNKS):
            receive("oend", c)
        for j in range(3):
            last(j)
        for loaded in own_loads[:3]:
            finish(loaded)
        core_arrival(s)
        core_arrival(mate)
        project(own_side, 3 * pair)

        core_arrival(omid)
        core_arrival(oend)
        project(far_side, 3 * pair)

        def rec_view(o, p):
            return rec_g.at[o, ds(p * strip, strip), :]

        pool_relays = [moved(pool_view(p), pq_s.at[i], pg_r.at[p], z(omid)) for i, p in enumerate(own_blocks)]

        def pool_relay(i):
            pool_sends[i].wait_recv()
            pool_relays[i].start()

        rec_sends = [moved(rec_view(side, p), rg_s.at[p], rg_r.at[side, p], z(omid)) for p in positions]
        for d in range(1, n_sp):
            o = lax.rem(s + d, n_sp)
            remote(spike, sbuf.at[o], sp_s.at[d - 1], sp_r.at[o], z(o)).wait_recv()
        tri_r = lax.broadcasted_iota(jnp.int32, (BLOCK, BLOCK), 0)
        tri_c = lax.broadcasted_iota(jnp.int32, (BLOCK, BLOCK), 1)
        causal = tri_r >= tri_c
        tri = causal.astype(BF16)
        tri = jnp.concatenate([tri, tri, tri], axis=1)
        heads = range(pair // width)

        def per_head(values):
            return jnp.concatenate([values(2 * side + h) for h in heads], axis=1)

        gate_low = jax.nn.sigmoid(-per_head(lambda h: low[h]))
        head_gain = [hgain[2 * side + h] for h in heads]

        def column(o, h):
            row = jnp.broadcast_to(sbuf[o, pl.ds(2 * side + h, 1)], (8, strip))
            return jnp.broadcast_to(jnp.transpose(row)[:, :1], (strip, width))

        state = [jnp.zeros((width, width), F32) for h in heads]
        for p in positions:
            projected = proj[p]
            spikes = jnp.concatenate([column(p, h) for h in heads], axis=1)
            q = projected[:, :pair].astype(F32)
            reader = q * jax.nn.sigmoid(q)
            key = gate_low * jax.nn.sigmoid(-projected[:, pair:2 * pair].astype(F32))
            logs = jnp.log1p(-key) + spikes
            high = logs.astype(BF16)
            rest = logs - high.astype(F32)
            middle = rest.astype(BF16)
            lowest = (rest - middle.astype(F32)).astype(BF16)
            for b in range(strip // BLOCK):
                here = slice(b * BLOCK, (b + 1) * BLOCK)
                terms = jnp.concatenate([high[here], middle[here], lowest[here]], axis=0)
                inner = jnp.dot(tri, terms, preferred_element_type=F32)
                closing = inner[BLOCK - 1:]
                read_scaled = (reader[here] * jnp.exp(inner)).astype(BF16)
                key_scaled = (key[here] * jnp.exp(-inner)).astype(BF16)
                key_tail = (key[here] * jnp.exp(closing - inner)).astype(BF16)
                kept = jnp.exp(closing)
                for h in heads:
                    at = slice(h * width, (h + 1) * width)
                    v = projected[here, 2 * pair + h * width:2 * pair + (h + 1) * width]
                    scores = lax.dot_general(read_scaled[:, at], key_scaled[:, at], NT, preferred_element_type=F32)
                    scores = jnp.where(causal, scores, 0.0).astype(BF16)
                    read = jnp.dot(scores, v, preferred_element_type=F32)
                    read = read + lax.dot_general(
                        read_scaled[:, at], state[h].astype(BF16), NT, preferred_element_type=F32
                    )
                    state[h] = kept[:, at] * state[h] + lax.dot_general(
                        v, key_tail[:, at], TN, preferred_element_type=F32
                    )
                    rec = read * lax.rsqrt(jnp.mean(read * read, axis=-1, keepdims=True) + EPSILON) * head_gain[h]
                    rec_g[side, p * strip + b * BLOCK:p * strip + (b + 1) * BLOCK, at] = rec.astype(BF16)
            rec_sends[p].start()
            if p > 0 and p < 3:
                pl.when(side == 0)(functools.partial(pool_relay, p - 1))
            if p == 2:
                for k in range(2):
                    wo_second(k, k)

        for i in (1, 0):
            pl.when(side == 1)(functools.partial(pool_relay, i))
        for k in range(2):
            finish(wo_loads[k])
        for k in range(2):
            wo_last(k, k)
        w_full = wo[...].reshape(2 * wo.shape[1], wo.shape[2])
        blocks = (0, 1, 3, 2)

        def across(i):
            return remote(part.at[i, 1 - t], dbuf.at[i], d_s.at[i], d_r.at[i], other)

        def deliver(i):
            return remote(summed.at[i], obuf.at[side], o_s.at[i], o_r.at[side], z(blocks[i]))

        def settle(i):
            across(i).wait_recv()
            both = (part[i, t].astype(F32) + dbuf[i].astype(F32)).astype(BF16)

            @pl.when(s == blocks[i])
            def _():
                obuf[side] = both

            @pl.when(s != blocks[i])
            def _():
                summed[i] = both
                deliver(i).start()

        for i, p in enumerate(blocks):
            pl.when(side != p // 2)(moved(pool_view(p), pq_s.at[i // 2], pg_r.at[p], z(omid)).wait_recv)
            moved(rec_view(1 - side, p), rg_s.at[i], rg_r.at[1 - side, p], z(omid)).wait_recv()
            here = pl.ds(p * strip, strip)
            mixed = jnp.concatenate([pool_g[here, :], rec_g[0, here, :], rec_g[1, here, :]], axis=1)
            acc = jnp.dot(mixed, w_full, preferred_element_type=F32).astype(BF16)
            for core in range(n_tp):
                part[i, core] = acc[core * rows:(core + 1) * rows]
            across(i).start()
            if i > 0:
                settle(i - 1)
        settle(n_sp - 1)
        common_drains()
        for copy in log + to_mate + to_far + relays + passes["mate"] + passes["omid"] + passes["oend"]:
            copy.wait_send()
        for copy in rec_sends + pool_relays + [to_end_mate]:
            copy.wait_send()
        moved(obuf.at[1 - side], o_s.at[0], o_r.at[1 - side], z(omid)).wait_recv()
        store()
        for i in range(n_sp):
            across(i).wait_send()
            pl.when(s != blocks[i])(deliver(i).wait_send)


def head_body(sizes, *args):
    (tokens, gain, w_pool, w_query, w_forget, w_value, maps, scale, low, spike, hgain, w_po, w_ro) = args
    n_sp, n_fs, n_tp = sizes
    tok = tokens[0]
    rows, features = tok.shape
    depth = w_pool.shape[0]
    width = w_pool.shape[1] // n_sp
    length = n_sp * n_tp * rows
    cols = w_po.shape[1]
    dma = pltpu.SemaphoreType.DMA
    whole = pl.BlockSpec(memory_space=pltpu.VMEM)
    here = pl.BlockSpec(memory_space=pl.ANY)
    result = pl.pallas_call(
        functools.partial(layer_kernel, n_fs, n_tp),
        out_shape=pltpu.VMEM((rows, n_sp * cols), BF16),
        in_specs=[here, whole, here, here, here, here, here, whole, whole, whole, whole, here, here],
        out_specs=whole,
        scratch_shapes=[
            pltpu.VMEM((rows, features), BF16),
            pltpu.VMEM((3, depth // n_fs, 6 * width), BF16),
            pltpu.VMEM((features, 6 * width), BF16),
            pltpu.VMEM((n_sp, n_tp, rows, features), BF16),
            pltpu.VMEM((n_sp,) + (spike.shape[2], spike.shape[1]), F32),
            pltpu.VMEM((n_sp, n_tp * rows, 6 * width), BF16),
            pltpu.VMEM((length, 4 * width), BF16),
            pltpu.VMEM((2, length, 2 * width), BF16),
            pltpu.VMEM((2, 2 ** (n_tp * maps.shape[0]), 4 * width), BF16),
            pltpu.VMEM((2, w_po.shape[0], 2 * cols), BF16),
            pltpu.VMEM(maps.shape, BF16),
            pltpu.VMEM((n_sp, n_tp, rows, 2 * cols), BF16),
            pltpu.VMEM((n_sp, rows, 2 * cols), BF16),
            pltpu.VMEM((n_sp, rows, 2 * cols), BF16),
            pltpu.VMEM((2, rows, 2 * cols), BF16),
            dma((20,)),
            dma((3,)), dma((n_sp,)),
            dma((4, 3)), dma((4, 3)),
            dma((3,)), dma((n_sp,)),
            dma((2, CHUNKS)), dma((CHUNKS,)), dma((n_sp, CHUNKS)),
            dma((n_sp, CHUNKS)), dma((n_sp, CHUNKS)),
            dma((2,)), dma((2,)),
            dma((4, 2)), dma((4, 2)),
            dma((2,)), dma((n_sp,)), dma((2,)),
            dma((1,)), dma((1,)),
            dma((n_sp,)), dma((2, n_sp)),
            dma((n_sp,)), dma((n_sp,)),
            dma((n_sp,)), dma((2,)),
            pltpu.SemaphoreType.REGULAR,
        ],
        compiler_params=pltpu.CompilerParams(
            collective_id=0, has_side_effects=True, vmem_limit_bytes=56 * 1024 * 1024
        ),
        name="layer",
    )(
        tok, gain[None], w_pool, w_query, w_forget, w_value, maps, scale[None],
        low.reshape(n_sp, 1, width), spike[0].T, hgain.reshape(n_sp, 1, width), w_po, w_ro,
    )
    return result[None]


def solution(mesh):
    placed = (
        P("fs", ("sp", "tp"), None),
        P(),
        P("sp", "tp"),
        P("sp", "tp"),
        P("sp", "tp"),
        P("sp", "tp"),
        P("tp", None, None),
        P("tp"),
        P("tp"),
        P("fs", "sp", "tp"),
        P("tp"),
        P("tp", "sp"),
        P("tp", "sp"),
    )
    sizes = (mesh.shape["sp"], mesh.shape["fs"], mesh.shape["tp"])

    def one(*args):
        maps, spike = args[6], args[9]
        width = args[2].shape[1] // sizes[0]
        fits = spike.shape[2] == sizes[0] and sizes == (4, 4, 2) and width % 128 == 0
        fits = fits and args[3].shape[1] == args[2].shape[1] and maps.shape[:2] == (2, 2 * width)
        return head_body(sizes, *args) if fits else body(*args)

    return jax.shard_map(
        one, mesh=mesh, in_specs=placed, out_specs=P("fs", ("sp", "tp"), None), check_vma=False
    )
```

```python
import functools

import jax
import jax.numpy as jnp
from jax import lax
from jax.experimental import pallas as pl
from jax.experimental.pallas import tpu as pltpu
from jax.sharding import PartitionSpec as P

BLOCK = 64


EPSILON = 1e-06
HIGHEST = lax.Precision.HIGHEST


def shifted(value, axis, steps):
    count = lax.axis_size(axis)
    first, last = (max(0, -steps), min(count, count - steps))
    return lax.ppermute(value, axis, [(source, source + steps) for source in range(first, last)])


def entering(shard, axis, join, neutral):
    place = lax.axis_index(axis)
    gathered = jax.tree.map(
        lambda a, kind: lax.all_gather(a.astype(kind), axis), shard, (jnp.bfloat16, jnp.bfloat16)
    )
    state = jax.tree.map(lambda a, e: jnp.zeros_like(a) + jnp.asarray(e, a.dtype), shard, neutral)

    def one(step, state):
        return join(
            state,
            jax.tree.map(
                lambda a, own: lax.dynamic_index_in_dim(a, step, 0, False).astype(own.dtype),
                gathered,
                shard,
            ),
        )

    return lax.fori_loop(0, place, one, state)


def rms_scale(values, gain):
    return values * lax.rsqrt(jnp.mean(values * values, axis=-1, keepdims=True) + EPSILON) * gain


def join_state(earlier, later):
    decay_one, state_one = earlier
    decay_two, state_two = later
    return (decay_one * decay_two, decay_two[..., None] * state_one + state_two)


def body(
    tokens,
    input_norm_gain,
    pooling_input_weight,
    query_weight,
    forget_weight,
    value_weight,
    pooling_group_maps,
    pooling_scale,
    lower_bound_logits,
    decay_spike,
    head_norm_gain,
    pooling_output_weight,
    recurrent_output_weight,
):
    gathered = lax.all_gather(tokens, "tp", axis=1, tiled=True)[0]
    length_total = gathered.shape[0]
    normed = rms_scale(gathered.astype(jnp.float32), input_norm_gain).astype(jnp.bfloat16)
    pool_width = pooling_input_weight.shape[1]
    rec_width = query_weight.shape[1]
    stacked = jnp.concatenate(
        [pooling_input_weight, query_weight, forget_weight, value_weight], axis=1
    )
    out_local = jnp.concatenate([pooling_output_weight, recurrent_output_weight], axis=0)
    groups_fs = lax.axis_size("fs")
    member = lax.axis_index("fs")
    slice_width = stacked.shape[1] // groups_fs
    own_slice = lax.dynamic_slice_in_dim(stacked, member * slice_width, slice_width, 1)
    column_part = lax.all_gather(own_slice, "sp", axis=0, tiled=True)
    full_input = lax.all_gather(column_part, "fs", axis=1, tiled=True)
    projected = jnp.dot(normed, full_input, preferred_element_type=jnp.float32)
    slice_height = out_local.shape[0] // groups_fs
    own_rows = lax.dynamic_slice_in_dim(out_local, member * slice_height, slice_height, 0)
    row_part = lax.all_gather(own_rows, "sp", axis=1, tiled=True)
    out_full = lax.all_gather(row_part, "fs", axis=0, tiled=True)
    rounded = lax.optimization_barrier(projected.astype(jnp.bfloat16))
    pool_input = rounded[:, :pool_width]
    query_matrix = rounded[:, pool_width : pool_width + rec_width].astype(jnp.float32)
    forget_gate_logit = rounded[:, pool_width + rec_width : pool_width + 2 * rec_width].astype(
        jnp.float32
    )
    value_projected = rounded[:, pool_width + 2 * rec_width :].astype(jnp.float32)
    groups_local = pooling_group_maps.shape[0]
    group_size = pooling_group_maps.shape[1]
    reach_rows = 2 ** (groups_local * lax.axis_size("tp"))
    previous = shifted(pool_input[length_total - reach_rows :], "sp", 1)
    extended = jnp.concatenate([previous, pool_input], axis=0).astype(jnp.float32)
    extended = extended.reshape(reach_rows + length_total, groups_local, group_size)
    group_ids = lax.axis_index("tp") * groups_local + jnp.arange(groups_local, dtype=jnp.int32)
    windows = jnp.left_shift(jnp.int32(2), group_ids)
    window_sum = jnp.zeros((length_total, groups_local, group_size), jnp.float32)
    for offset in range(reach_rows):
        inside = (offset < windows).astype(jnp.float32)
        window_sum = (
            window_sum
            + extended[reach_rows - offset : reach_rows - offset + length_total] * inside[:, None]
        )
    position_index = lax.axis_index("sp") * length_total + jnp.arange(length_total, dtype=jnp.int32)
    counts = jnp.minimum(position_index[:, None] + 1, windows[None, :]).astype(jnp.float32)
    pool_diff = (window_sum / counts[:, :, None] - extended[reach_rows:]).astype(jnp.bfloat16)
    pool_mapped = jnp.einsum(
        "tgc,gcd->tgd", pool_diff, pooling_group_maps, preferred_element_type=jnp.float32
    )
    pool_out = (pool_mapped.reshape(length_total, pool_width) * pooling_scale).astype(jnp.bfloat16)
    local_heads = decay_spike.shape[2]
    head_width = rec_width // local_heads
    blocks = length_total // BLOCK
    block_layout = (blocks, BLOCK, local_heads, head_width)
    reader = jax.nn.silu(query_matrix).reshape(block_layout)
    key_gate_value = jax.nn.sigmoid(-lower_bound_logits) * jax.nn.sigmoid(-forget_gate_logit)
    decay_logarithm = (
        jnp.log1p(-key_gate_value).reshape(length_total, local_heads, head_width)
        + decay_spike[0][:, :, None]
    ).reshape(block_layout)
    key_rows = key_gate_value.reshape(block_layout)
    value_rows = value_projected.reshape(block_layout)
    inner_log = jnp.cumsum(decay_logarithm, axis=1)
    read_scaled = reader * jnp.exp(inner_log)
    key_scaled = key_rows * jnp.exp(-inner_log)
    causal = (jnp.arange(BLOCK)[:, None] >= jnp.arange(BLOCK)[None, :]).astype(jnp.float32)
    scores = jnp.einsum("nthd,nshd->nhts", read_scaled, key_scaled, precision=HIGHEST) * causal
    within = jnp.einsum("nhts,nshe->nthe", scores, value_rows, precision=HIGHEST)
    closing = inner_log[:, -1]
    key_tail = key_rows * jnp.exp(closing[:, None] - inner_log)
    deltas = jnp.einsum("nshd,nshe->nhde", key_tail, value_rows, precision=HIGHEST)
    block_decay = jnp.exp(closing)

    def advance(carried, input_batch):
        decay_now, delta_now = input_batch
        return (decay_now[..., None] * carried + delta_now, carried)

    initial = jnp.zeros((local_heads, head_width, head_width), jnp.float32)
    device_state, entry_states = lax.scan(advance, initial, (block_decay, deltas))
    device_decay = jnp.exp(jnp.sum(closing, axis=0))
    scanned = entering(
        (device_decay, device_state),
        "sp",
        join_state,
        (jnp.ones_like(device_decay), jnp.zeros_like(device_state)),
    )
    prior_state = scanned[1]
    before = jnp.cumsum(closing, axis=0) - closing
    start_states = entry_states + jnp.exp(before)[..., None] * prior_state[None]
    read_out = within + jnp.einsum("nthd,nhde->nthe", read_scaled, start_states, precision=HIGHEST)
    read_out = read_out.reshape(length_total, local_heads, head_width)
    recurrent_output = (
        rms_scale(read_out, 1.0).reshape(length_total, rec_width) * head_norm_gain
    ).astype(jnp.bfloat16)
    mixed_rows = jnp.concatenate([pool_out, recurrent_output], axis=1)
    summed = lax.psum_scatter(
        jnp.dot(mixed_rows, out_full, preferred_element_type=jnp.float32).astype(jnp.bfloat16),
        "tp",
        scatter_dimension=0,
        tiled=True,
    )
    return summed[None]


F32 = jnp.float32
BF16 = jnp.bfloat16
NT = (((1,), (1,)), ((), ()))
TN = (((0,), (0,)), ((), ()))

CHUNKS = 4


def layer_kernel(
    n_fs, n_tp,
    tok, gain, w_pool, w_query, w_forget, w_value, maps, scale, low, spike, hgain, w_po, w_ro,
    out,
    tbuf, stage, wbuf, nbuf, sbuf, proj, pool_g, rec_g, halo, wo, map_v, part, dbuf, summed, obuf,
    ld, w_s, w_r, wt_s, wt_r, sp_s, sp_r, tf_s, tm_s, tz_r, td_s, td_r,
    wo_s, wo_r, ot_s, ot_r, pg_s, pg_r, pq_s, h_s, h_r, rg_s, rg_r, d_s, d_r, o_s, o_r, gate,
):
    s = lax.axis_index("sp")
    f = lax.axis_index("fs")
    t = lax.axis_index("tp")
    n_sp = 4
    rows = tok.shape[0]
    depth = w_pool.shape[0]
    width = w_pool.shape[1] // n_sp
    cols = w_po.shape[1]
    piece = depth // n_fs
    half = piece // 2
    strip = n_tp * rows
    pair = 2 * width
    reach_rows = halo.shape[1]

    side = s // 2
    end, mid, omid, oend = 3 * side, 1 + side, 2 - side, 3 - 3 * side
    mate = end + mid - s
    is_end, is_mid = s == end, s == mid
    peers = (mate, omid, oend)
    positions = range(n_sp)
    far_side, own_side = 2 - 2 * side, 2 * side

    def z(o):
        return {"sp": o, "fs": f, "tp": t}

    at_x = {"sp": s, "fs": f + 1 - 2 * lax.rem(f, 2), "tp": t}
    at_y = {"sp": s, "fs": f + 2 - 4 * (f // 2), "tp": t}
    other = {"sp": s, "fs": f, "tp": 1 - t}
    f_x, f_y, f_d = at_x["fs"], at_y["fs"], 3 - f

    def ds(start, size):
        return pl.ds(pl.multiple_of(start, size), size)

    def remote(src, dst, ssem, rsem, dev):
        return pltpu.make_async_remote_copy(
            src_ref=src, dst_ref=dst, send_sem=ssem, recv_sem=rsem,
            device_id=dev, device_id_type=pl.DeviceIdType.MESH,
        )

    def moved(view, ssem, rsem, dev):
        return remote(view, view, ssem, rsem, dev)

    def when(cond, action):
        if cond is None:
            action()
        else:
            pl.when(cond)(action)

    def load(src, dst, i, cond=None):
        copy = pltpu.make_async_copy(src, dst, ld.at[i])
        when(cond, copy.start)
        return copy, cond

    def finish(loaded):
        when(loaded[1], loaded[0].wait)

    barrier = pltpu.get_barrier_semaphore()
    partners = [z(o) for o in peers] + [at_x, at_y, other]
    for dev in partners:
        pl.semaphore_signal(barrier, inc=1, device_id=dev, device_id_type=pl.DeviceIdType.MESH)
    tok_load = load(tok, tbuf, 0)
    gates = (w_query, w_forget, w_value)
    stage_loads = []
    for j, dest in enumerate(peers):
        group_loads = []
        if j < 2:
            for m, w in enumerate(gates):
                group_loads.append(load(
                    w.at[ds(f * piece, piece), ds((dest // 2) * pair, pair)],
                    stage.at[j, :, pl.ds(m * pair, pair)], 1 + 4 * j + m, is_end if j == 0 else None,
                ))
        if j != 1:
            group_loads.append(load(
                w_pool.at[ds(f * piece, piece), :], stage.at[j, :, pl.ds(0, 2 * pair)],
                4 + 4 * j, is_mid if j == 0 else None,
            ))
        stage_loads.append(group_loads)
    own_rows = ds(s * depth, depth)
    own_loads = [
        load(w.at[:, ds(side * pair, pair)], wbuf.at[own_rows, pl.ds(m * pair, pair)], 13 + m, is_mid)
        for m, w in enumerate(gates)
    ]
    own_loads.append(load(w_pool, wbuf.at[own_rows, pl.ds(0, 2 * pair)], 16, is_end))
    map_load = load(maps, map_v, 17, is_end)
    wo_place = ds(lax.rem(s, 2) * cols, cols)
    wo_loads = [load(w, wo.at[k, :, wo_place], 18 + k, is_mid) for k, w in enumerate((w_po, w_ro))]

    pl.semaphore_wait(barrier, len(partners))

    def w_send(j, span):
        dst = wbuf.at[ds(s * depth + f * piece, piece), pl.ds(0, span)]
        return remote(stage.at[j, :, pl.ds(0, span)], dst, w_s.at[j], w_r.at[s], z(peers[j]))

    to_mid_mate, to_end_mate = w_send(0, 3 * pair), w_send(0, 2 * pair)
    to_omid, to_oend = w_send(1, 3 * pair), w_send(2, 2 * pair)
    for j in (1, 0, 2):
        for loaded in stage_loads[j]:
            finish(loaded)
    pl.when(is_mid)(to_omid.start)
    pl.when(is_mid)(to_oend.start)
    pl.when(is_mid)(to_end_mate.start)
    pl.when(is_end)(to_mid_mate.start)
    spike_sends = [remote(spike, sbuf.at[s], sp_s.at[j], sp_r.at[s], z(dest)) for j, dest in enumerate(peers)]
    for copy in spike_sends:
        copy.start()

    chunk = rows // CHUNKS

    def tok_view(o, core, c):
        return nbuf.at[o, core, pl.ds(c * chunk, chunk), :]

    def core_pass(o, c):
        return moved(tok_view(o, t, c), td_s.at[o, c], td_r.at[o, c], other)

    def core_arrival(o):
        for c in range(CHUNKS):
            moved(tok_view(o, 1 - t, c), td_s.at[o, c], td_r.at[o, c], other).wait_recv()

    finish(tok_load)
    x = tbuf[...].astype(F32)
    y = x * lax.rsqrt(jnp.mean(x * x, axis=-1, keepdims=True) + EPSILON) * gain[...]
    nbuf[s, t] = y.astype(BF16)
    to_mate = [moved(tok_view(s, t, c), tm_s.at[c], tz_r.at[s, c], z(mate)) for c in range(CHUNKS)]
    own_pass = [core_pass(s, c) for c in range(CHUNKS)]
    for copy in own_pass:
        copy.start()
    sbuf[s] = spike[...]

    def tree(view, ssem, rsem, log):
        def start(copy):
            copy.start()
            log.append(copy)

        def first(i, o):
            start(moved(view(o, f), ssem.at[0, i], rsem.at[0, i], at_x))
            start(moved(view(o, f), ssem.at[1, i], rsem.at[1, i], at_y))

        def second(i, o):
            moved(view(o, f_x), ssem.at[0, i], rsem.at[0, i], at_x).wait_recv()
            start(moved(view(o, f_x, 0), ssem.at[2, i], rsem.at[2, i], at_y))
            moved(view(o, f_y), ssem.at[1, i], rsem.at[1, i], at_y).wait_recv()
            start(moved(view(o, f_y, 1), ssem.at[3, i], rsem.at[3, i], at_x))

        def last(i, o):
            moved(view(o, f_d, 0), ssem.at[2, i], rsem.at[2, i], at_y).wait_recv()
            moved(view(o, f_d, 1), ssem.at[3, i], rsem.at[3, i], at_x).wait_recv()

        return first, second, last

    def w_tree(span, log):
        def view(o, giver, h=None):
            start, size = o * depth + giver * piece, piece
            if h is not None:
                start, size = start + h * half, half
            return wbuf.at[ds(start, size), pl.ds(0, span)]

        def arrival(j):
            moved(view(peers[j], f), w_s.at[j], w_r.at[peers[j]], z(peers[j])).wait_recv()

        first, second, last = tree(view, wt_s, wt_r, log)
        return (
            arrival,
            lambda j: first(j, peers[j]),
            lambda j: second(j, peers[j]),
            lambda j: last(j, peers[j]),
        )

    def project(base, span):
        x = nbuf[pl.ds(base, 2)].reshape(2 * strip, nbuf.shape[3])
        y = jnp.dot(x, wbuf[:, :span], preferred_element_type=F32)
        proj[pl.ds(base, 2), :, :span] = y.astype(BF16).reshape(2, strip, span)

    def pool_view(p):
        return pool_g.at[ds(p * strip, strip), :]

    own_blocks = (own_side, own_side + 1)
    pool_sends = [moved(pool_view(p), pg_s.at[i], pg_r.at[p], z(mid)) for i, p in enumerate(own_blocks)]
    tok_arrivals = {
        o: [moved(tok_view(p, t, c), tm_s.at[c], tz_r.at[p, c], z(p)) for c in range(CHUNKS)]
        for o, p in (("mate", mate), ("omid", omid), ("oend", oend))
    }

    def store():
        for h in range(2):
            out[:, 2 * h * cols:2 * (h + 1) * cols] = obuf[h]

    def common_drains():
        for copy in spike_sends + own_pass:
            copy.wait_send()

    @pl.when(is_end)
    def _():
        log = []
        arrival, first, second, last = w_tree(2 * pair, log)
        to_mid_mate.wait_send()
        to_omid.start()
        arrival(0)
        first(0)
        to_omid.wait_send()
        to_oend.start()
        second(0)
        to_oend.wait_send()

        @pl.when(t == 0)
        def _():
            pl.semaphore_signal(gate, inc=1, device_id=other, device_id_type=pl.DeviceIdType.MESH)

        @pl.when(t == 1)
        def _():
            pl.semaphore_wait(gate, 1)

        for copy in to_mate:
            copy.start()
        arrival(1)
        first(1)
        arrival(2)
        first(2)
        for copy in to_mate:
            copy.wait_send()
        wo_sends = [
            remote(
                w.at[ds(f * piece, piece), :], wo.at[k, ds(f * piece, piece), wo_place], wo_s.at[k], wo_r.at[k], z(mid)
            )
            for k, w in enumerate((w_po, w_ro))
        ]
        for copy in wo_sends:
            copy.start()
        second(1)
        second(2)
        passes = [core_pass(mate, c) for c in range(CHUNKS)]
        for c in range(CHUNKS):
            tok_arrivals["mate"][c].wait_recv()
            passes[c].start()
        for j in range(3):
            last(j)
        finish(own_loads[3])
        core_arrival(s)
        core_arrival(mate)
        project(own_side, 2 * pair)
        halo_copy = remote(halo.at[0], halo.at[1], h_s.at[0], h_r.at[0], z(oend))

        @pl.when(side == 0)
        def _():
            halo[0] = proj[1, strip - reach_rows:, :2 * pair]
            halo_copy.start()
            halo[1] = jnp.zeros((reach_rows, 2 * pair), BF16)

        finish(map_load)
        groups = maps.shape[0]
        group = t * groups + lax.broadcasted_iota(jnp.int32, (strip, 2 * pair), 1) // pair
        position = lax.broadcasted_iota(jnp.int32, (strip, 2 * pair), 0)
        scale_row = scale[...]

        def pool(i, before):
            x = jnp.concatenate([before, proj[own_side + i, :, :2 * pair]], axis=0).astype(F32)
            total = x
            for g in range(n_tp * groups):
                reach = 2 ** g
                total = total + jnp.concatenate([jnp.zeros((reach, 2 * pair), F32), total[:-reach]], axis=0)
                if g == 0:
                    window_sum = total[reach_rows:]
                    window = jnp.full((strip, 2 * pair), 2, jnp.int32)
                else:
                    window_sum = jnp.where(group == g, total[reach_rows:], window_sum)
                    window = jnp.where(group == g, 2 ** (g + 1), window)
            counts = jnp.minimum((own_side + i) * strip + position + 1, window).astype(F32)
            diff = (window_sum / counts - x[reach_rows:]).astype(BF16)
            mapped = jnp.concatenate(
                [
                    jnp.dot(diff[:, g * pair:(g + 1) * pair], map_v[g], preferred_element_type=F32)
                    for g in range(groups)
                ],
                axis=1,
            )
            pool_g[ds((own_side + i) * strip, strip), :] = (mapped * scale_row).astype(BF16)

        pool(1, proj[own_side, strip - reach_rows:, :2 * pair])

        @pl.when(side == 1)
        def _():
            pool_sends[1].start()
            halo_copy.wait_recv()

        pool(0, halo[1])
        pool_sends[0].start()
        pl.when(side == 0)(pool_sends[1].start)
        for o in range(1, n_sp):
            origin = lax.rem(s + o, n_sp)
            remote(spike, sbuf.at[origin], sp_s.at[o - 1], sp_r.at[origin], z(origin)).wait_recv()
        common_drains()
        for copy in log + passes + wo_sends + pool_sends:
            copy.wait_send()
        pl.when(side == 0)(halo_copy.wait_send)
        moved(obuf.at[1 - side], o_s.at[0], o_r.at[1 - side], z(omid)).wait_recv()
        moved(obuf.at[side], o_s.at[0], o_r.at[side], z(mid)).wait_recv()
        store()

    @pl.when(is_mid)
    def _():
        log = []
        arrival, first, second, last = w_tree(3 * pair, log)
        to_far = [moved(tok_view(s, t, c), tf_s.at[0, c], tz_r.at[s, c], z(omid)) for c in range(CHUNKS)]
        relays = [moved(tok_view(mate, t, c), tf_s.at[1, c], tz_r.at[mate, c], z(omid)) for c in range(CHUNKS)]
        passes = {
            "mate": [core_pass(mate, c) for c in range(CHUNKS)],
            "omid": [core_pass(omid, c) for c in range(CHUNKS)],
            "oend": [core_pass(oend, c) for c in range(CHUNKS)],
        }

        def relay(c):
            tok_arrivals["mate"][c].wait_recv()
            relays[c].start()
            passes["mate"][c].start()

        def receive(o, c):
            tok_arrivals[o][c].wait_recv()
            passes[o][c].start()

        for copy in to_mate:
            copy.start()
        arrival(0)
        first(0)
        arrival(1)
        first(1)
        to_omid.wait_send()
        to_oend.wait_send()

        @pl.when(t == 0)
        def _():
            pl.semaphore_signal(gate, inc=1, device_id=other, device_id_type=pl.DeviceIdType.MESH)
            for copy in to_far:
                copy.start()

        second(0)
        arrival(2)
        first(2)

        @pl.when(t == 1)
        def _():
            pl.semaphore_wait(gate, 1)
            for copy in to_far:
                copy.start()

        second(1)
        relay(0)
        relay(1)
        relay(2)
        relay(3)
        second(2)
        for c in range(CHUNKS):
            receive("omid", c)
        def wo_view(k, giver, h=None):
            start, size = giver * piece, piece
            if h is not None:
                start, size = start + h * half, half
            return wo.at[k, ds(start, size), ds(lax.rem(end, 2) * cols, cols)]

        wo_first, wo_second, wo_last = tree(wo_view, ot_s, ot_r, log)
        for k in range(2):
            moved(wo_view(k, f), wo_s.at[k], wo_r.at[k], z(end)).wait_recv()
            wo_first(k, k)
        for c in range(CHUNKS):
            receive("oend", c)
        for j in range(3):
            last(j)
        for loaded in own_loads[:3]:
            finish(loaded)

        def tokens_of(first_side):
            @pl.when(side == first_side)
            def _():
                core_arrival(s)
                core_arrival(mate)

            @pl.when(side != first_side)
            def _():
                core_arrival(omid)
                core_arrival(oend)

        tokens_of(0)
        project(0, 3 * pair)

        def rec_view(o, p):
            return rec_g.at[o, ds(p * strip, strip), :]

        pool_relays = [moved(pool_view(p), pq_s.at[i], pg_r.at[p], z(omid)) for i, p in enumerate(own_blocks)]

        def pool_relay(i):
            pool_sends[i].wait_recv()
            pool_relays[i].start()

        rec_sends = [moved(rec_view(side, p), rg_s.at[p], rg_r.at[side, p], z(omid)) for p in positions]
        for d in range(1, n_sp):
            o = lax.rem(s + d, n_sp)
            remote(spike, sbuf.at[o], sp_s.at[d - 1], sp_r.at[o], z(o)).wait_recv()
        tri_r = lax.broadcasted_iota(jnp.int32, (BLOCK, BLOCK), 0)
        tri_c = lax.broadcasted_iota(jnp.int32, (BLOCK, BLOCK), 1)
        causal = tri_r >= tri_c
        tri = causal.astype(BF16)
        tri = jnp.concatenate([tri, tri, tri], axis=1)
        heads = range(pair // width)

        def per_head(values):
            return jnp.concatenate([values(2 * side + h) for h in heads], axis=1)

        gate_low = jax.nn.sigmoid(-per_head(lambda h: low[h]))
        head_gain = [hgain[2 * side + h] for h in heads]

        def column(o, h):
            row = jnp.broadcast_to(sbuf[o, pl.ds(2 * side + h, 1)], (8, strip))
            return jnp.broadcast_to(jnp.transpose(row)[:, :1], (strip, width))

        state = [jnp.zeros((width, width), F32) for h in heads]
        for p in positions:
            if p == 2:
                tokens_of(1)
                project(2, 3 * pair)
            projected = proj[p]
            spikes = jnp.concatenate([column(p, h) for h in heads], axis=1)
            q = projected[:, :pair].astype(F32)
            reader = q * jax.nn.sigmoid(q)
            key = gate_low * jax.nn.sigmoid(-projected[:, pair:2 * pair].astype(F32))
            logs = jnp.log1p(-key) + spikes
            high = logs.astype(BF16)
            rest = logs - high.astype(F32)
            middle = rest.astype(BF16)
            lowest = (rest - middle.astype(F32)).astype(BF16)
            for b in range(strip // BLOCK):
                here = slice(b * BLOCK, (b + 1) * BLOCK)
                terms = jnp.concatenate([high[here], middle[here], lowest[here]], axis=0)
                inner = jnp.dot(tri, terms, preferred_element_type=F32)
                closing = inner[BLOCK - 1:]
                read_scaled = (reader[here] * jnp.exp(inner)).astype(BF16)
                key_scaled = (key[here] * jnp.exp(-inner)).astype(BF16)
                key_tail = (key[here] * jnp.exp(closing - inner)).astype(BF16)
                kept = jnp.exp(closing)
                for h in heads:
                    at = slice(h * width, (h + 1) * width)
                    v = projected[here, 2 * pair + h * width:2 * pair + (h + 1) * width]
                    scores = lax.dot_general(read_scaled[:, at], key_scaled[:, at], NT, preferred_element_type=F32)
                    scores = jnp.where(causal, scores, 0.0).astype(BF16)
                    read = jnp.dot(scores, v, preferred_element_type=F32)
                    read = read + lax.dot_general(
                        read_scaled[:, at], state[h].astype(BF16), NT, preferred_element_type=F32
                    )
                    state[h] = kept[:, at] * state[h] + lax.dot_general(
                        v, key_tail[:, at], TN, preferred_element_type=F32
                    )
                    rec = read * lax.rsqrt(jnp.mean(read * read, axis=-1, keepdims=True) + EPSILON) * head_gain[h]
                    rec_g[side, p * strip + b * BLOCK:p * strip + (b + 1) * BLOCK, at] = rec.astype(BF16)
            if p == 1:
                pl.when(side == 0)(rec_sends[p].start)
            else:
                rec_sends[p].start()
            if p > 0 and p < 3:
                wo_second(p - 1, p - 1)
            upper_one = jnp.logical_and(t == 1, side == 1)
            upper_zero = jnp.logical_and(t == 0, side == 1)
            if p == 0:
                pl.when(upper_one)(functools.partial(pool_relay, 1))
            if p == 1:
                pl.when(upper_zero)(functools.partial(pool_relay, 1))
            if p == 2:
                pl.when(upper_one)(functools.partial(pool_relay, 0))
            if p == 1 or p == 2:
                pl.when(side == 0)(functools.partial(pool_relay, p - 1))
        pl.when(jnp.logical_and(t == 0, side == 1))(functools.partial(pool_relay, 0))
        pl.when(side == 1)(rec_sends[1].start)
        for k in range(2):
            finish(wo_loads[k])
        for k in range(2):
            wo_last(k, k)
        w_full = wo[...].reshape(2 * wo.shape[1], wo.shape[2])
        blocks = (0 * side, 3 - 2 * side, 2 + side, 1 + side)
        crossed = (side == 1, None, side == 0)

        def across(i):
            return remote(part.at[i, 1 - t], dbuf.at[i], d_s.at[i], d_r.at[i], other)

        def deliver(i):
            return remote(summed.at[i], obuf.at[side], o_s.at[i], o_r.at[side], z(blocks[i]))

        def settle(i):
            across(i).wait_recv()
            both = (part[i, t].astype(F32) + dbuf[i].astype(F32)).astype(BF16)

            @pl.when(s == blocks[i])
            def _():
                obuf[side] = both

            @pl.when(s != blocks[i])
            def _():
                summed[i] = both
                deliver(i).start()

        for i, p in enumerate(blocks):
            if i < 3:
                when(crossed[i], moved(pool_view(p), pq_s.at[0], pg_r.at[p], z(omid)).wait_recv)
            moved(rec_view(1 - side, p), rg_s.at[i], rg_r.at[1 - side, p], z(omid)).wait_recv()
            here = ds(p * strip, strip)
            mixed = jnp.concatenate([pool_g[here, :], rec_g[0, here, :], rec_g[1, here, :]], axis=1)
            acc = jnp.dot(mixed, w_full, preferred_element_type=F32).astype(BF16)
            for core in range(n_tp):
                part[i, core] = acc[core * rows:(core + 1) * rows]
            across(i).start()
            if i > 0:
                settle(i - 1)
        settle(n_sp - 1)
        common_drains()
        for copy in log + to_mate + to_far + relays + passes["mate"] + passes["omid"] + passes["oend"]:
            copy.wait_send()
        for copy in rec_sends + pool_relays + [to_end_mate]:
            copy.wait_send()
        moved(obuf.at[1 - side], o_s.at[0], o_r.at[1 - side], z(omid)).wait_recv()
        store()
        for i in range(n_sp):
            across(i).wait_send()
            pl.when(s != blocks[i])(deliver(i).wait_send)


def head_body(sizes, *args):
    (tokens, gain, w_pool, w_query, w_forget, w_value, maps, scale, low, spike, hgain, w_po, w_ro) = args
    n_sp, n_fs, n_tp = sizes
    tok = tokens[0]
    rows, features = tok.shape
    depth = w_pool.shape[0]
    width = w_pool.shape[1] // n_sp
    length = n_sp * n_tp * rows
    cols = w_po.shape[1]
    dma = pltpu.SemaphoreType.DMA
    whole = pl.BlockSpec(memory_space=pltpu.VMEM)
    here = pl.BlockSpec(memory_space=pl.ANY)
    result = pl.pallas_call(
        functools.partial(layer_kernel, n_fs, n_tp),
        out_shape=pltpu.VMEM((rows, n_sp * cols), BF16),
        in_specs=[here, whole, here, here, here, here, here, whole, whole, whole, whole, here, here],
        out_specs=whole,
        scratch_shapes=[
            pltpu.VMEM((rows, features), BF16),
            pltpu.VMEM((3, depth // n_fs, 6 * width), BF16),
            pltpu.VMEM((features, 6 * width), BF16),
            pltpu.VMEM((n_sp, n_tp, rows, features), BF16),
            pltpu.VMEM((n_sp,) + (spike.shape[2], spike.shape[1]), F32),
            pltpu.VMEM((n_sp, n_tp * rows, 6 * width), BF16),
            pltpu.VMEM((length, 4 * width), BF16),
            pltpu.VMEM((2, length, 2 * width), BF16),
            pltpu.VMEM((2, 2 ** (n_tp * maps.shape[0]), 4 * width), BF16),
            pltpu.VMEM((2, w_po.shape[0], 2 * cols), BF16),
            pltpu.VMEM(maps.shape, BF16),
            pltpu.VMEM((n_sp, n_tp, rows, 2 * cols), BF16),
            pltpu.VMEM((n_sp, rows, 2 * cols), BF16),
            pltpu.VMEM((n_sp, rows, 2 * cols), BF16),
            pltpu.VMEM((2, rows, 2 * cols), BF16),
            dma((20,)),
            dma((3,)), dma((n_sp,)),
            dma((4, 3)), dma((4, 3)),
            dma((3,)), dma((n_sp,)),
            dma((2, CHUNKS)), dma((CHUNKS,)), dma((n_sp, CHUNKS)),
            dma((n_sp, CHUNKS)), dma((n_sp, CHUNKS)),
            dma((2,)), dma((2,)),
            dma((4, 2)), dma((4, 2)),
            dma((2,)), dma((n_sp,)), dma((2,)),
            dma((1,)), dma((1,)),
            dma((n_sp,)), dma((2, n_sp)),
            dma((n_sp,)), dma((n_sp,)),
            dma((n_sp,)), dma((2,)),
            pltpu.SemaphoreType.REGULAR,
        ],
        compiler_params=pltpu.CompilerParams(
            collective_id=0, has_side_effects=True, vmem_limit_bytes=56 * 1024 * 1024
        ),
        name="layer",
    )(
        tok, gain[None], w_pool, w_query, w_forget, w_value, maps, scale[None],
        low.reshape(n_sp, 1, width), spike[0].T, hgain.reshape(n_sp, 1, width), w_po, w_ro,
    )
    return result[None]


def solution(mesh):
    placed = (
        P("fs", ("sp", "tp"), None),
        P(),
        P("sp", "tp"),
        P("sp", "tp"),
        P("sp", "tp"),
        P("sp", "tp"),
        P("tp", None, None),
        P("tp"),
        P("tp"),
        P("fs", "sp", "tp"),
        P("tp"),
        P("tp", "sp"),
        P("tp", "sp"),
    )
    sizes = (mesh.shape["sp"], mesh.shape["fs"], mesh.shape["tp"])

    def one(*args):
        maps, spike = args[6], args[9]
        width = args[2].shape[1] // sizes[0]
        fits = spike.shape[2] == sizes[0] and sizes == (4, 4, 2) and width % 128 == 0
        fits = fits and args[3].shape[1] == args[2].shape[1] and maps.shape[:2] == (2, 2 * width)
        return head_body(sizes, *args) if fits else body(*args)

    return jax.shard_map(
        one, mesh=mesh, in_specs=placed, out_specs=P("fs", ("sp", "tp"), None), check_vma=False
    )
```

```python
import functools

import jax
import jax.numpy as jnp
from jax import lax
from jax.experimental import pallas as pl
from jax.experimental.pallas import tpu as pltpu
from jax.sharding import PartitionSpec as P

BLOCK = 64


EPSILON = 1e-06
HIGHEST = lax.Precision.HIGHEST


def shifted(value, axis, steps):
    count = lax.axis_size(axis)
    first, last = (max(0, -steps), min(count, count - steps))
    return lax.ppermute(value, axis, [(source, source + steps) for source in range(first, last)])


def entering(shard, axis, join, neutral):
    place = lax.axis_index(axis)
    gathered = jax.tree.map(
        lambda a, kind: lax.all_gather(a.astype(kind), axis), shard, (jnp.bfloat16, jnp.bfloat16)
    )
    state = jax.tree.map(lambda a, e: jnp.zeros_like(a) + jnp.asarray(e, a.dtype), shard, neutral)

    def one(step, state):
        return join(
            state,
            jax.tree.map(
                lambda a, own: lax.dynamic_index_in_dim(a, step, 0, False).astype(own.dtype),
                gathered,
                shard,
            ),
        )

    return lax.fori_loop(0, place, one, state)


def rms_scale(values, gain):
    return values * lax.rsqrt(jnp.mean(values * values, axis=-1, keepdims=True) + EPSILON) * gain


def join_state(earlier, later):
    decay_one, state_one = earlier
    decay_two, state_two = later
    return (decay_one * decay_two, decay_two[..., None] * state_one + state_two)


def body(
    tokens,
    input_norm_gain,
    pooling_input_weight,
    query_weight,
    forget_weight,
    value_weight,
    pooling_group_maps,
    pooling_scale,
    lower_bound_logits,
    decay_spike,
    head_norm_gain,
    pooling_output_weight,
    recurrent_output_weight,
):
    gathered = lax.all_gather(tokens, "tp", axis=1, tiled=True)[0]
    length_total = gathered.shape[0]
    normed = rms_scale(gathered.astype(jnp.float32), input_norm_gain).astype(jnp.bfloat16)
    pool_width = pooling_input_weight.shape[1]
    rec_width = query_weight.shape[1]
    stacked = jnp.concatenate(
        [pooling_input_weight, query_weight, forget_weight, value_weight], axis=1
    )
    out_local = jnp.concatenate([pooling_output_weight, recurrent_output_weight], axis=0)
    groups_fs = lax.axis_size("fs")
    member = lax.axis_index("fs")
    slice_width = stacked.shape[1] // groups_fs
    own_slice = lax.dynamic_slice_in_dim(stacked, member * slice_width, slice_width, 1)
    column_part = lax.all_gather(own_slice, "sp", axis=0, tiled=True)
    full_input = lax.all_gather(column_part, "fs", axis=1, tiled=True)
    projected = jnp.dot(normed, full_input, preferred_element_type=jnp.float32)
    slice_height = out_local.shape[0] // groups_fs
    own_rows = lax.dynamic_slice_in_dim(out_local, member * slice_height, slice_height, 0)
    row_part = lax.all_gather(own_rows, "sp", axis=1, tiled=True)
    out_full = lax.all_gather(row_part, "fs", axis=0, tiled=True)
    rounded = lax.optimization_barrier(projected.astype(jnp.bfloat16))
    pool_input = rounded[:, :pool_width]
    query_matrix = rounded[:, pool_width : pool_width + rec_width].astype(jnp.float32)
    forget_gate_logit = rounded[:, pool_width + rec_width : pool_width + 2 * rec_width].astype(
        jnp.float32
    )
    value_projected = rounded[:, pool_width + 2 * rec_width :].astype(jnp.float32)
    groups_local = pooling_group_maps.shape[0]
    group_size = pooling_group_maps.shape[1]
    reach_rows = 2 ** (groups_local * lax.axis_size("tp"))
    previous = shifted(pool_input[length_total - reach_rows :], "sp", 1)
    extended = jnp.concatenate([previous, pool_input], axis=0).astype(jnp.float32)
    extended = extended.reshape(reach_rows + length_total, groups_local, group_size)
    group_ids = lax.axis_index("tp") * groups_local + jnp.arange(groups_local, dtype=jnp.int32)
    windows = jnp.left_shift(jnp.int32(2), group_ids)
    window_sum = jnp.zeros((length_total, groups_local, group_size), jnp.float32)
    for offset in range(reach_rows):
        inside = (offset < windows).astype(jnp.float32)
        window_sum = (
            window_sum
            + extended[reach_rows - offset : reach_rows - offset + length_total] * inside[:, None]
        )
    position_index = lax.axis_index("sp") * length_total + jnp.arange(length_total, dtype=jnp.int32)
    counts = jnp.minimum(position_index[:, None] + 1, windows[None, :]).astype(jnp.float32)
    pool_diff = (window_sum / counts[:, :, None] - extended[reach_rows:]).astype(jnp.bfloat16)
    pool_mapped = jnp.einsum(
        "tgc,gcd->tgd", pool_diff, pooling_group_maps, preferred_element_type=jnp.float32
    )
    pool_out = (pool_mapped.reshape(length_total, pool_width) * pooling_scale).astype(jnp.bfloat16)
    local_heads = decay_spike.shape[2]
    head_width = rec_width // local_heads
    blocks = length_total // BLOCK
    block_layout = (blocks, BLOCK, local_heads, head_width)
    reader = jax.nn.silu(query_matrix).reshape(block_layout)
    key_gate_value = jax.nn.sigmoid(-lower_bound_logits) * jax.nn.sigmoid(-forget_gate_logit)
    decay_logarithm = (
        jnp.log1p(-key_gate_value).reshape(length_total, local_heads, head_width)
        + decay_spike[0][:, :, None]
    ).reshape(block_layout)
    key_rows = key_gate_value.reshape(block_layout)
    value_rows = value_projected.reshape(block_layout)
    inner_log = jnp.cumsum(decay_logarithm, axis=1)
    read_scaled = reader * jnp.exp(inner_log)
    key_scaled = key_rows * jnp.exp(-inner_log)
    causal = (jnp.arange(BLOCK)[:, None] >= jnp.arange(BLOCK)[None, :]).astype(jnp.float32)
    scores = jnp.einsum("nthd,nshd->nhts", read_scaled, key_scaled, precision=HIGHEST) * causal
    within = jnp.einsum("nhts,nshe->nthe", scores, value_rows, precision=HIGHEST)
    closing = inner_log[:, -1]
    key_tail = key_rows * jnp.exp(closing[:, None] - inner_log)
    deltas = jnp.einsum("nshd,nshe->nhde", key_tail, value_rows, precision=HIGHEST)
    block_decay = jnp.exp(closing)

    def advance(carried, input_batch):
        decay_now, delta_now = input_batch
        return (decay_now[..., None] * carried + delta_now, carried)

    initial = jnp.zeros((local_heads, head_width, head_width), jnp.float32)
    device_state, entry_states = lax.scan(advance, initial, (block_decay, deltas))
    device_decay = jnp.exp(jnp.sum(closing, axis=0))
    scanned = entering(
        (device_decay, device_state),
        "sp",
        join_state,
        (jnp.ones_like(device_decay), jnp.zeros_like(device_state)),
    )
    prior_state = scanned[1]
    before = jnp.cumsum(closing, axis=0) - closing
    start_states = entry_states + jnp.exp(before)[..., None] * prior_state[None]
    read_out = within + jnp.einsum("nthd,nhde->nthe", read_scaled, start_states, precision=HIGHEST)
    read_out = read_out.reshape(length_total, local_heads, head_width)
    recurrent_output = (
        rms_scale(read_out, 1.0).reshape(length_total, rec_width) * head_norm_gain
    ).astype(jnp.bfloat16)
    mixed_rows = jnp.concatenate([pool_out, recurrent_output], axis=1)
    summed = lax.psum_scatter(
        jnp.dot(mixed_rows, out_full, preferred_element_type=jnp.float32).astype(jnp.bfloat16),
        "tp",
        scatter_dimension=0,
        tiled=True,
    )
    return summed[None]


F32 = jnp.float32
BF16 = jnp.bfloat16
NT = (((1,), (1,)), ((), ()))
TN = (((0,), (0,)), ((), ()))

CHUNKS = 2


def layer_kernel(
    n_fs, n_tp,
    tok, gain, w_pool, w_query, w_forget, w_value, maps, scale, low, spike, hgain, w_po, w_ro,
    out,
    tbuf, stage, wbuf, nbuf, sbuf, proj, pool_g, rec_g, halo, wo, map_v, part, dbuf, summed, obuf,
    ld, w_s, w_r, wt_s, wt_r, sp_s, sp_r, tf_s, tm_s, tz_r, td_s, td_r,
    wo_s, wo_r, ot_s, ot_r, pg_s, pg_r, pq_s, h_s, h_r, rg_s, rg_r, d_s, d_r, o_s, o_r, gate,
):
    s = lax.axis_index("sp")
    f = lax.axis_index("fs")
    t = lax.axis_index("tp")
    n_sp = 4
    rows = tok.shape[0]
    depth = w_pool.shape[0]
    width = w_pool.shape[1] // n_sp
    cols = w_po.shape[1]
    piece = depth // n_fs
    half = piece // 2
    strip = n_tp * rows
    pair = 2 * width
    reach_rows = halo.shape[1]

    side = s // 2
    end, mid, omid, oend = 3 * side, 1 + side, 2 - side, 3 - 3 * side
    mate = end + mid - s
    is_end, is_mid = s == end, s == mid
    peers = (mate, omid, oend)
    positions = range(n_sp)
    far_side, own_side = 2 - 2 * side, 2 * side

    def z(o):
        return {"sp": o, "fs": f, "tp": t}

    at_x = {"sp": s, "fs": f + 1 - 2 * lax.rem(f, 2), "tp": t}
    at_y = {"sp": s, "fs": f + 2 - 4 * (f // 2), "tp": t}
    other = {"sp": s, "fs": f, "tp": 1 - t}
    f_x, f_y, f_d = at_x["fs"], at_y["fs"], 3 - f

    def ds(start, size):
        return pl.ds(pl.multiple_of(start, size), size)

    def remote(src, dst, ssem, rsem, dev):
        return pltpu.make_async_remote_copy(
            src_ref=src, dst_ref=dst, send_sem=ssem, recv_sem=rsem,
            device_id=dev, device_id_type=pl.DeviceIdType.MESH,
        )

    def moved(view, ssem, rsem, dev):
        return remote(view, view, ssem, rsem, dev)

    def when(cond, action):
        if cond is None:
            action()
        else:
            pl.when(cond)(action)

    def load(src, dst, i, cond=None):
        copy = pltpu.make_async_copy(src, dst, ld.at[i])
        when(cond, copy.start)
        return copy, cond

    def finish(loaded):
        when(loaded[1], loaded[0].wait)

    barrier = pltpu.get_barrier_semaphore()
    partners = [z(o) for o in peers] + [at_x, at_y, other]
    for dev in partners:
        pl.semaphore_signal(barrier, inc=1, device_id=dev, device_id_type=pl.DeviceIdType.MESH)
    tok_load = load(tok, tbuf, 0)
    gates = (w_query, w_forget, w_value)
    stage_loads = []
    for j, dest in enumerate(peers):
        group_loads = []
        if j < 2:
            for m, w in enumerate(gates):
                group_loads.append(load(
                    w.at[ds(f * piece, piece), ds((dest // 2) * pair, pair)],
                    stage.at[j, :, pl.ds(m * pair, pair)], 1 + 4 * j + m, is_end if j == 0 else None,
                ))
        if j != 1:
            group_loads.append(load(
                w_pool.at[ds(f * piece, piece), :], stage.at[j, :, pl.ds(0, 2 * pair)],
                4 + 4 * j, is_mid if j == 0 else None,
            ))
        stage_loads.append(group_loads)
    own_rows = ds(s * depth, depth)
    own_loads = [
        load(w.at[:, ds(side * pair, pair)], wbuf.at[own_rows, pl.ds(m * pair, pair)], 13 + m, is_mid)
        for m, w in enumerate(gates)
    ]
    own_loads.append(load(w_pool, wbuf.at[own_rows, pl.ds(0, 2 * pair)], 16, is_end))
    map_load = load(maps, map_v, 17, is_end)
    wo_place = ds(lax.rem(s, 2) * cols, cols)
    wo_loads = [load(w, wo.at[k, :, wo_place], 18 + k, is_mid) for k, w in enumerate((w_po, w_ro))]

    pl.semaphore_wait(barrier, len(partners))

    def w_send(j, span):
        dst = wbuf.at[ds(s * depth + f * piece, piece), pl.ds(0, span)]
        return remote(stage.at[j, :, pl.ds(0, span)], dst, w_s.at[j], w_r.at[s], z(peers[j]))

    to_mid_mate, to_end_mate = w_send(0, 3 * pair), w_send(0, 2 * pair)
    to_omid, to_oend = w_send(1, 3 * pair), w_send(2, 2 * pair)
    for j in (1, 0, 2):
        for loaded in stage_loads[j]:
            finish(loaded)
    pl.when(is_mid)(to_omid.start)
    pl.when(is_mid)(to_oend.start)
    pl.when(is_mid)(to_end_mate.start)
    pl.when(is_end)(to_mid_mate.start)
    spike_sends = [remote(spike, sbuf.at[s], sp_s.at[j], sp_r.at[s], z(dest)) for j, dest in enumerate(peers)]
    for copy in spike_sends:
        copy.start()

    chunk = rows // CHUNKS

    def tok_view(o, core, c):
        return nbuf.at[o, core, pl.ds(c * chunk, chunk), :]

    def core_pass(o, c):
        return moved(tok_view(o, t, c), td_s.at[o, c], td_r.at[o, c], other)

    def core_arrival(o):
        for c in range(CHUNKS):
            moved(tok_view(o, 1 - t, c), td_s.at[o, c], td_r.at[o, c], other).wait_recv()

    finish(tok_load)
    x = tbuf[...].astype(F32)
    y = x * lax.rsqrt(jnp.mean(x * x, axis=-1, keepdims=True) + EPSILON) * gain[...]
    nbuf[s, t] = y.astype(BF16)
    to_mate = [moved(tok_view(s, t, c), tm_s.at[c], tz_r.at[s, c], z(mate)) for c in range(CHUNKS)]
    own_pass = [core_pass(s, c) for c in range(CHUNKS)]
    for copy in own_pass:
        copy.start()
    sbuf[s] = spike[...]

    def tree(view, ssem, rsem, log):
        def start(copy):
            copy.start()
            log.append(copy)

        def first(i, o):
            start(moved(view(o, f), ssem.at[0, i], rsem.at[0, i], at_x))
            start(moved(view(o, f), ssem.at[1, i], rsem.at[1, i], at_y))

        def second(i, o):
            moved(view(o, f_x), ssem.at[0, i], rsem.at[0, i], at_x).wait_recv()
            start(moved(view(o, f_x, 0), ssem.at[2, i], rsem.at[2, i], at_y))
            moved(view(o, f_y), ssem.at[1, i], rsem.at[1, i], at_y).wait_recv()
            start(moved(view(o, f_y, 1), ssem.at[3, i], rsem.at[3, i], at_x))

        def last(i, o):
            moved(view(o, f_d, 0), ssem.at[2, i], rsem.at[2, i], at_y).wait_recv()
            moved(view(o, f_d, 1), ssem.at[3, i], rsem.at[3, i], at_x).wait_recv()

        return first, second, last

    def w_tree(span, log):
        def view(o, giver, h=None):
            start, size = o * depth + giver * piece, piece
            if h is not None:
                start, size = start + h * half, half
            return wbuf.at[ds(start, size), pl.ds(0, span)]

        def arrival(j):
            moved(view(peers[j], f), w_s.at[j], w_r.at[peers[j]], z(peers[j])).wait_recv()

        first, second, last = tree(view, wt_s, wt_r, log)
        return (
            arrival,
            lambda j: first(j, peers[j]),
            lambda j: second(j, peers[j]),
            lambda j: last(j, peers[j]),
        )

    def project(base, span):
        x = nbuf[pl.ds(base, 2)].reshape(2 * strip, nbuf.shape[3])
        y = jnp.dot(x, wbuf[:, :span], preferred_element_type=F32)
        proj[pl.ds(base, 2), :, :span] = y.astype(BF16).reshape(2, strip, span)

    def pool_view(p):
        return pool_g.at[ds(p * strip, strip), :]

    own_blocks = (own_side, own_side + 1)
    pool_sends = [moved(pool_view(p), pg_s.at[i], pg_r.at[p], z(mid)) for i, p in enumerate(own_blocks)]
    tok_arrivals = {
        o: [moved(tok_view(p, t, c), tm_s.at[c], tz_r.at[p, c], z(p)) for c in range(CHUNKS)]
        for o, p in (("mate", mate), ("omid", omid), ("oend", oend))
    }

    def store():
        for h in range(2):
            out[:, 2 * h * cols:2 * (h + 1) * cols] = obuf[h]

    def common_drains():
        for copy in spike_sends + own_pass:
            copy.wait_send()

    @pl.when(is_end)
    def _():
        log = []
        arrival, first, second, last = w_tree(2 * pair, log)
        to_mid_mate.wait_send()
        to_omid.start()
        arrival(0)
        first(0)
        to_omid.wait_send()
        to_oend.start()
        for copy in to_mate:
            copy.start()
        second(0)
        arrival(1)
        first(1)
        arrival(2)
        first(2)
        for copy in to_mate:
            copy.wait_send()
        wo_sends = [
            remote(
                w.at[ds(f * piece, piece), :], wo.at[k, ds(f * piece, piece), wo_place], wo_s.at[k], wo_r.at[k], z(mid)
            )
            for k, w in enumerate((w_po, w_ro))
        ]
        for copy in wo_sends:
            copy.start()
        second(1)
        second(2)
        passes = [core_pass(mate, c) for c in range(CHUNKS)]
        for c in range(CHUNKS):
            tok_arrivals["mate"][c].wait_recv()
            passes[c].start()
        for j in range(3):
            last(j)
        finish(own_loads[3])
        core_arrival(s)
        core_arrival(mate)
        project(own_side, 2 * pair)
        halo_copy = remote(halo.at[0], halo.at[1], h_s.at[0], h_r.at[0], z(oend))

        @pl.when(side == 0)
        def _():
            halo[0] = proj[1, strip - reach_rows:, :2 * pair]
            halo_copy.start()
            halo[1] = jnp.zeros((reach_rows, 2 * pair), BF16)

        finish(map_load)
        groups = maps.shape[0]
        group = t * groups + lax.broadcasted_iota(jnp.int32, (strip, 2 * pair), 1) // pair
        position = lax.broadcasted_iota(jnp.int32, (strip, 2 * pair), 0)
        scale_row = scale[...]

        def pool(i, before):
            x = jnp.concatenate([before, proj[own_side + i, :, :2 * pair]], axis=0).astype(F32)
            total = x
            for g in range(n_tp * groups):
                reach = 2 ** g
                total = total + jnp.concatenate([jnp.zeros((reach, 2 * pair), F32), total[:-reach]], axis=0)
                if g == 0:
                    window_sum = total[reach_rows:]
                    window = jnp.full((strip, 2 * pair), 2, jnp.int32)
                else:
                    window_sum = jnp.where(group == g, total[reach_rows:], window_sum)
                    window = jnp.where(group == g, 2 ** (g + 1), window)
            counts = jnp.minimum((own_side + i) * strip + position + 1, window).astype(F32)
            diff = (window_sum / counts - x[reach_rows:]).astype(BF16)
            mapped = jnp.concatenate(
                [
                    jnp.dot(diff[:, g * pair:(g + 1) * pair], map_v[g], preferred_element_type=F32)
                    for g in range(groups)
                ],
                axis=1,
            )
            pool_g[ds((own_side + i) * strip, strip), :] = (mapped * scale_row).astype(BF16)

        pool(1, proj[own_side, strip - reach_rows:, :2 * pair])

        @pl.when(side == 1)
        def _():
            pool_sends[1].start()
            halo_copy.wait_recv()

        pool(0, halo[1])
        pool_sends[0].start()
        pl.when(side == 0)(pool_sends[1].start)
        for o in range(1, n_sp):
            origin = lax.rem(s + o, n_sp)
            remote(spike, sbuf.at[origin], sp_s.at[o - 1], sp_r.at[origin], z(origin)).wait_recv()
        common_drains()
        for copy in log + passes + wo_sends + pool_sends + [to_oend]:
            copy.wait_send()
        pl.when(side == 0)(halo_copy.wait_send)
        moved(obuf.at[1 - side], o_s.at[0], o_r.at[1 - side], z(omid)).wait_recv()
        moved(obuf.at[side], o_s.at[0], o_r.at[side], z(mid)).wait_recv()
        store()

    @pl.when(is_mid)
    def _():
        log = []
        arrival, first, second, last = w_tree(3 * pair, log)
        to_far = [moved(tok_view(s, t, c), tf_s.at[0, c], tz_r.at[s, c], z(omid)) for c in range(CHUNKS)]
        relays = [moved(tok_view(mate, t, c), tf_s.at[1, c], tz_r.at[mate, c], z(omid)) for c in range(CHUNKS)]
        passes = {
            "mate": [core_pass(mate, c) for c in range(CHUNKS)],
            "omid": [core_pass(omid, c) for c in range(CHUNKS)],
            "oend": [core_pass(oend, c) for c in range(CHUNKS)],
        }

        def relay(c):
            tok_arrivals["mate"][c].wait_recv()
            relays[c].start()
            passes["mate"][c].start()

        def receive(o, c):
            tok_arrivals[o][c].wait_recv()
            passes[o][c].start()

        for copy in to_mate:
            copy.start()
        arrival(0)
        first(0)
        arrival(1)
        first(1)
        to_omid.wait_send()

        @pl.when(t == 0)
        def _():
            pl.semaphore_signal(gate, inc=1, device_id=other, device_id_type=pl.DeviceIdType.MESH)
            for copy in to_far:
                copy.start()

        second(0)
        arrival(2)
        first(2)

        @pl.when(t == 1)
        def _():
            pl.semaphore_wait(gate, 1)
            for copy in to_far:
                copy.start()

        second(1)
        relay(0)
        relay(1)
        second(2)
        for c in range(CHUNKS):
            receive("omid", c)
        def wo_view(k, giver, h=None):
            start, size = giver * piece, piece
            if h is not None:
                start, size = start + h * half, half
            return wo.at[k, ds(start, size), ds(lax.rem(end, 2) * cols, cols)]

        wo_first, wo_second, wo_last = tree(wo_view, ot_s, ot_r, log)
        for k in range(2):
            moved(wo_view(k, f), wo_s.at[k], wo_r.at[k], z(end)).wait_recv()
            wo_first(k, k)
        for c in range(CHUNKS):
            receive("oend", c)
        for j in range(3):
            last(j)
        for loaded in own_loads[:3]:
            finish(loaded)

        def tokens_of(first_side):
            @pl.when(side == first_side)
            def _():
                core_arrival(s)
                core_arrival(mate)

            @pl.when(side != first_side)
            def _():
                core_arrival(omid)
                core_arrival(oend)

        tokens_of(0)
        project(0, 3 * pair)

        def rec_view(o, p):
            return rec_g.at[o, ds(p * strip, strip), :]

        pool_relays = [moved(pool_view(p), pq_s.at[i], pg_r.at[p], z(omid)) for i, p in enumerate(own_blocks)]

        def pool_relay(i):
            pool_sends[i].wait_recv()
            pool_relays[i].start()

        rec_sends = [moved(rec_view(side, p), rg_s.at[p], rg_r.at[side, p], z(omid)) for p in positions]
        for d in range(1, n_sp):
            o = lax.rem(s + d, n_sp)
            remote(spike, sbuf.at[o], sp_s.at[d - 1], sp_r.at[o], z(o)).wait_recv()
        tri_r = lax.broadcasted_iota(jnp.int32, (BLOCK, BLOCK), 0)
        tri_c = lax.broadcasted_iota(jnp.int32, (BLOCK, BLOCK), 1)
        causal = tri_r >= tri_c
        tri = causal.astype(BF16)
        tri = jnp.concatenate([tri, tri, tri], axis=1)
        heads = range(pair // width)

        def per_head(values):
            return jnp.concatenate([values(2 * side + h) for h in heads], axis=1)

        gate_low = jax.nn.sigmoid(-per_head(lambda h: low[h]))
        head_gain = [hgain[2 * side + h] for h in heads]

        def column(o, h):
            row = jnp.broadcast_to(sbuf[o, pl.ds(2 * side + h, 1)], (8, strip))
            return jnp.broadcast_to(jnp.transpose(row)[:, :1], (strip, width))

        state = [jnp.zeros((width, width), F32) for h in heads]
        for p in positions:
            if p == 2:
                tokens_of(1)
                project(2, 3 * pair)
            projected = proj[p]
            spikes = jnp.concatenate([column(p, h) for h in heads], axis=1)
            q = projected[:, :pair].astype(F32)
            reader = q * jax.nn.sigmoid(q)
            key = gate_low * jax.nn.sigmoid(-projected[:, pair:2 * pair].astype(F32))
            logs = jnp.log1p(-key) + spikes
            high = logs.astype(BF16)
            rest = logs - high.astype(F32)
            middle = rest.astype(BF16)
            lowest = (rest - middle.astype(F32)).astype(BF16)
            for b in range(strip // BLOCK):
                here = slice(b * BLOCK, (b + 1) * BLOCK)
                terms = jnp.concatenate([high[here], middle[here], lowest[here]], axis=0)
                inner = jnp.dot(tri, terms, preferred_element_type=F32)
                closing = inner[BLOCK - 1:]
                read_scaled = (reader[here] * jnp.exp(inner)).astype(BF16)
                key_scaled = (key[here] * jnp.exp(-inner)).astype(BF16)
                key_tail = (key[here] * jnp.exp(closing - inner)).astype(BF16)
                kept = jnp.exp(closing)
                for h in heads:
                    at = slice(h * width, (h + 1) * width)
                    v = projected[here, 2 * pair + h * width:2 * pair + (h + 1) * width]
                    scores = lax.dot_general(read_scaled[:, at], key_scaled[:, at], NT, preferred_element_type=F32)
                    scores = jnp.where(causal, scores, 0.0).astype(BF16)
                    read = jnp.dot(scores, v, preferred_element_type=F32)
                    read = read + lax.dot_general(
                        read_scaled[:, at], state[h].astype(BF16), NT, preferred_element_type=F32
                    )
                    state[h] = kept[:, at] * state[h] + lax.dot_general(
                        v, key_tail[:, at], TN, preferred_element_type=F32
                    )
                    rec = read * lax.rsqrt(jnp.mean(read * read, axis=-1, keepdims=True) + EPSILON) * head_gain[h]
                    rec_g[side, p * strip + b * BLOCK:p * strip + (b + 1) * BLOCK, at] = rec.astype(BF16)
            if p == 1:
                pl.when(side == 0)(rec_sends[p].start)
            else:
                rec_sends[p].start()
            if p > 0 and p < 3:
                wo_second(p - 1, p - 1)
            upper_one = jnp.logical_and(t == 1, side == 1)
            upper_zero = jnp.logical_and(t == 0, side == 1)
            if p == 0:
                pl.when(upper_one)(functools.partial(pool_relay, 1))
            if p == 1:
                pl.when(upper_zero)(functools.partial(pool_relay, 1))
            if p == 2:
                pl.when(upper_one)(functools.partial(pool_relay, 0))
            if p == 1 or p == 2:
                pl.when(side == 0)(functools.partial(pool_relay, p - 1))
        pl.when(jnp.logical_and(t == 0, side == 1))(functools.partial(pool_relay, 0))
        pl.when(side == 1)(rec_sends[1].start)
        for k in range(2):
            finish(wo_loads[k])
        for k in range(2):
            wo_last(k, k)
        w_full = wo[...].reshape(2 * wo.shape[1], wo.shape[2])
        blocks = (0 * side, 3 - 2 * side, 2 + side, 1 + side)
        crossed = (side == 1, None, side == 0)

        def across(i):
            return remote(part.at[i, 1 - t], dbuf.at[i], d_s.at[i], d_r.at[i], other)

        def deliver(i):
            return remote(summed.at[i], obuf.at[side], o_s.at[i], o_r.at[side], z(blocks[i]))

        def settle(i):
            across(i).wait_recv()
            both = (part[i, t].astype(F32) + dbuf[i].astype(F32)).astype(BF16)

            @pl.when(s == blocks[i])
            def _():
                obuf[side] = both

            @pl.when(s != blocks[i])
            def _():
                summed[i] = both
                deliver(i).start()

        for i, p in enumerate(blocks):
            if i < 3:
                when(crossed[i], moved(pool_view(p), pq_s.at[0], pg_r.at[p], z(omid)).wait_recv)
            moved(rec_view(1 - side, p), rg_s.at[i], rg_r.at[1 - side, p], z(omid)).wait_recv()
            here = ds(p * strip, strip)
            mixed = jnp.concatenate([pool_g[here, :], rec_g[0, here, :], rec_g[1, here, :]], axis=1)
            acc = jnp.dot(mixed, w_full, preferred_element_type=F32).astype(BF16)
            for core in range(n_tp):
                part[i, core] = acc[core * rows:(core + 1) * rows]
            across(i).start()
            settle(i)
        common_drains()
        for copy in log + to_mate + to_far + relays + passes["mate"] + passes["omid"] + passes["oend"]:
            copy.wait_send()
        for copy in rec_sends + pool_relays + [to_end_mate, to_oend]:
            copy.wait_send()
        moved(obuf.at[1 - side], o_s.at[0], o_r.at[1 - side], z(omid)).wait_recv()
        store()
        for i in range(n_sp):
            across(i).wait_send()
            pl.when(s != blocks[i])(deliver(i).wait_send)


def head_body(sizes, *args):
    (tokens, gain, w_pool, w_query, w_forget, w_value, maps, scale, low, spike, hgain, w_po, w_ro) = args
    n_sp, n_fs, n_tp = sizes
    tok = tokens[0]
    rows, features = tok.shape
    depth = w_pool.shape[0]
    width = w_pool.shape[1] // n_sp
    length = n_sp * n_tp * rows
    cols = w_po.shape[1]
    dma = pltpu.SemaphoreType.DMA
    whole = pl.BlockSpec(memory_space=pltpu.VMEM)
    here = pl.BlockSpec(memory_space=pl.ANY)
    result = pl.pallas_call(
        functools.partial(layer_kernel, n_fs, n_tp),
        out_shape=pltpu.VMEM((rows, n_sp * cols), BF16),
        in_specs=[here, whole, here, here, here, here, here, whole, whole, whole, whole, here, here],
        out_specs=whole,
        scratch_shapes=[
            pltpu.VMEM((rows, features), BF16),
            pltpu.VMEM((3, depth // n_fs, 6 * width), BF16),
            pltpu.VMEM((features, 6 * width), BF16),
            pltpu.VMEM((n_sp, n_tp, rows, features), BF16),
            pltpu.VMEM((n_sp,) + (spike.shape[2], spike.shape[1]), F32),
            pltpu.VMEM((n_sp, n_tp * rows, 6 * width), BF16),
            pltpu.VMEM((length, 4 * width), BF16),
            pltpu.VMEM((2, length, 2 * width), BF16),
            pltpu.VMEM((2, 2 ** (n_tp * maps.shape[0]), 4 * width), BF16),
            pltpu.VMEM((2, w_po.shape[0], 2 * cols), BF16),
            pltpu.VMEM(maps.shape, BF16),
            pltpu.VMEM((n_sp, n_tp, rows, 2 * cols), BF16),
            pltpu.VMEM((n_sp, rows, 2 * cols), BF16),
            pltpu.VMEM((n_sp, rows, 2 * cols), BF16),
            pltpu.VMEM((2, rows, 2 * cols), BF16),
            dma((20,)),
            dma((3,)), dma((n_sp,)),
            dma((4, 3)), dma((4, 3)),
            dma((3,)), dma((n_sp,)),
            dma((2, CHUNKS)), dma((CHUNKS,)), dma((n_sp, CHUNKS)),
            dma((n_sp, CHUNKS)), dma((n_sp, CHUNKS)),
            dma((2,)), dma((2,)),
            dma((4, 2)), dma((4, 2)),
            dma((2,)), dma((n_sp,)), dma((2,)),
            dma((1,)), dma((1,)),
            dma((n_sp,)), dma((2, n_sp)),
            dma((n_sp,)), dma((n_sp,)),
            dma((n_sp,)), dma((2,)),
            pltpu.SemaphoreType.REGULAR,
        ],
        compiler_params=pltpu.CompilerParams(
            collective_id=0, has_side_effects=True, vmem_limit_bytes=56 * 1024 * 1024
        ),
        name="layer",
    )(
        tok, gain[None], w_pool, w_query, w_forget, w_value, maps, scale[None],
        low.reshape(n_sp, 1, width), spike[0].T, hgain.reshape(n_sp, 1, width), w_po, w_ro,
    )
    return result[None]


def solution(mesh):
    placed = (
        P("fs", ("sp", "tp"), None),
        P(),
        P("sp", "tp"),
        P("sp", "tp"),
        P("sp", "tp"),
        P("sp", "tp"),
        P("tp", None, None),
        P("tp"),
        P("tp"),
        P("fs", "sp", "tp"),
        P("tp"),
        P("tp", "sp"),
        P("tp", "sp"),
    )
    sizes = (mesh.shape["sp"], mesh.shape["fs"], mesh.shape["tp"])

    def one(*args):
        maps, spike = args[6], args[9]
        width = args[2].shape[1] // sizes[0]
        fits = spike.shape[2] == sizes[0] and sizes == (4, 4, 2) and width % 128 == 0
        fits = fits and args[3].shape[1] == args[2].shape[1] and maps.shape[:2] == (2, 2 * width)
        return head_body(sizes, *args) if fits else body(*args)

    return jax.shard_map(
        one, mesh=mesh, in_specs=placed, out_specs=P("fs", ("sp", "tp"), None), check_vma=False
    )
```

```python
import functools

import jax
import jax.numpy as jnp
from jax import lax
from jax.experimental import pallas as pl
from jax.experimental.pallas import tpu as pltpu
from jax.sharding import PartitionSpec as P

BLOCK = 64


EPSILON = 1e-06
HIGHEST = lax.Precision.HIGHEST


def shifted(value, axis, steps):
    count = lax.axis_size(axis)
    first, last = (max(0, -steps), min(count, count - steps))
    return lax.ppermute(value, axis, [(source, source + steps) for source in range(first, last)])


def entering(shard, axis, join, neutral):
    place = lax.axis_index(axis)
    gathered = jax.tree.map(
        lambda a, kind: lax.all_gather(a.astype(kind), axis), shard, (jnp.bfloat16, jnp.bfloat16)
    )
    state = jax.tree.map(lambda a, e: jnp.zeros_like(a) + jnp.asarray(e, a.dtype), shard, neutral)

    def one(step, state):
        return join(
            state,
            jax.tree.map(
                lambda a, own: lax.dynamic_index_in_dim(a, step, 0, False).astype(own.dtype),
                gathered,
                shard,
            ),
        )

    return lax.fori_loop(0, place, one, state)


def rms_scale(values, gain):
    return values * lax.rsqrt(jnp.mean(values * values, axis=-1, keepdims=True) + EPSILON) * gain


def join_state(earlier, later):
    decay_one, state_one = earlier
    decay_two, state_two = later
    return (decay_one * decay_two, decay_two[..., None] * state_one + state_two)


def body(
    tokens,
    input_norm_gain,
    pooling_input_weight,
    query_weight,
    forget_weight,
    value_weight,
    pooling_group_maps,
    pooling_scale,
    lower_bound_logits,
    decay_spike,
    head_norm_gain,
    pooling_output_weight,
    recurrent_output_weight,
):
    gathered = lax.all_gather(tokens, "tp", axis=1, tiled=True)[0]
    length_total = gathered.shape[0]
    normed = rms_scale(gathered.astype(jnp.float32), input_norm_gain).astype(jnp.bfloat16)
    pool_width = pooling_input_weight.shape[1]
    rec_width = query_weight.shape[1]
    stacked = jnp.concatenate(
        [pooling_input_weight, query_weight, forget_weight, value_weight], axis=1
    )
    out_local = jnp.concatenate([pooling_output_weight, recurrent_output_weight], axis=0)
    groups_fs = lax.axis_size("fs")
    member = lax.axis_index("fs")
    slice_width = stacked.shape[1] // groups_fs
    own_slice = lax.dynamic_slice_in_dim(stacked, member * slice_width, slice_width, 1)
    column_part = lax.all_gather(own_slice, "sp", axis=0, tiled=True)
    full_input = lax.all_gather(column_part, "fs", axis=1, tiled=True)
    projected = jnp.dot(normed, full_input, preferred_element_type=jnp.float32)
    slice_height = out_local.shape[0] // groups_fs
    own_rows = lax.dynamic_slice_in_dim(out_local, member * slice_height, slice_height, 0)
    row_part = lax.all_gather(own_rows, "sp", axis=1, tiled=True)
    out_full = lax.all_gather(row_part, "fs", axis=0, tiled=True)
    rounded = lax.optimization_barrier(projected.astype(jnp.bfloat16))
    pool_input = rounded[:, :pool_width]
    query_matrix = rounded[:, pool_width : pool_width + rec_width].astype(jnp.float32)
    forget_gate_logit = rounded[:, pool_width + rec_width : pool_width + 2 * rec_width].astype(
        jnp.float32
    )
    value_projected = rounded[:, pool_width + 2 * rec_width :].astype(jnp.float32)
    groups_local = pooling_group_maps.shape[0]
    group_size = pooling_group_maps.shape[1]
    reach_rows = 2 ** (groups_local * lax.axis_size("tp"))
    previous = shifted(pool_input[length_total - reach_rows :], "sp", 1)
    extended = jnp.concatenate([previous, pool_input], axis=0).astype(jnp.float32)
    extended = extended.reshape(reach_rows + length_total, groups_local, group_size)
    group_ids = lax.axis_index("tp") * groups_local + jnp.arange(groups_local, dtype=jnp.int32)
    windows = jnp.left_shift(jnp.int32(2), group_ids)
    window_sum = jnp.zeros((length_total, groups_local, group_size), jnp.float32)
    for offset in range(reach_rows):
        inside = (offset < windows).astype(jnp.float32)
        window_sum = (
            window_sum
            + extended[reach_rows - offset : reach_rows - offset + length_total] * inside[:, None]
        )
    position_index = lax.axis_index("sp") * length_total + jnp.arange(length_total, dtype=jnp.int32)
    counts = jnp.minimum(position_index[:, None] + 1, windows[None, :]).astype(jnp.float32)
    pool_diff = (window_sum / counts[:, :, None] - extended[reach_rows:]).astype(jnp.bfloat16)
    pool_mapped = jnp.einsum(
        "tgc,gcd->tgd", pool_diff, pooling_group_maps, preferred_element_type=jnp.float32
    )
    pool_out = (pool_mapped.reshape(length_total, pool_width) * pooling_scale).astype(jnp.bfloat16)
    local_heads = decay_spike.shape[2]
    head_width = rec_width // local_heads
    blocks = length_total // BLOCK
    block_layout = (blocks, BLOCK, local_heads, head_width)
    reader = jax.nn.silu(query_matrix).reshape(block_layout)
    key_gate_value = jax.nn.sigmoid(-lower_bound_logits) * jax.nn.sigmoid(-forget_gate_logit)
    decay_logarithm = (
        jnp.log1p(-key_gate_value).reshape(length_total, local_heads, head_width)
        + decay_spike[0][:, :, None]
    ).reshape(block_layout)
    key_rows = key_gate_value.reshape(block_layout)
    value_rows = value_projected.reshape(block_layout)
    inner_log = jnp.cumsum(decay_logarithm, axis=1)
    read_scaled = reader * jnp.exp(inner_log)
    key_scaled = key_rows * jnp.exp(-inner_log)
    causal = (jnp.arange(BLOCK)[:, None] >= jnp.arange(BLOCK)[None, :]).astype(jnp.float32)
    scores = jnp.einsum("nthd,nshd->nhts", read_scaled, key_scaled, precision=HIGHEST) * causal
    within = jnp.einsum("nhts,nshe->nthe", scores, value_rows, precision=HIGHEST)
    closing = inner_log[:, -1]
    key_tail = key_rows * jnp.exp(closing[:, None] - inner_log)
    deltas = jnp.einsum("nshd,nshe->nhde", key_tail, value_rows, precision=HIGHEST)
    block_decay = jnp.exp(closing)

    def advance(carried, input_batch):
        decay_now, delta_now = input_batch
        return (decay_now[..., None] * carried + delta_now, carried)

    initial = jnp.zeros((local_heads, head_width, head_width), jnp.float32)
    device_state, entry_states = lax.scan(advance, initial, (block_decay, deltas))
    device_decay = jnp.exp(jnp.sum(closing, axis=0))
    scanned = entering(
        (device_decay, device_state),
        "sp",
        join_state,
        (jnp.ones_like(device_decay), jnp.zeros_like(device_state)),
    )
    prior_state = scanned[1]
    before = jnp.cumsum(closing, axis=0) - closing
    start_states = entry_states + jnp.exp(before)[..., None] * prior_state[None]
    read_out = within + jnp.einsum("nthd,nhde->nthe", read_scaled, start_states, precision=HIGHEST)
    read_out = read_out.reshape(length_total, local_heads, head_width)
    recurrent_output = (
        rms_scale(read_out, 1.0).reshape(length_total, rec_width) * head_norm_gain
    ).astype(jnp.bfloat16)
    mixed_rows = jnp.concatenate([pool_out, recurrent_output], axis=1)
    summed = lax.psum_scatter(
        jnp.dot(mixed_rows, out_full, preferred_element_type=jnp.float32).astype(jnp.bfloat16),
        "tp",
        scatter_dimension=0,
        tiled=True,
    )
    return summed[None]


F32 = jnp.float32
BF16 = jnp.bfloat16
NT = (((1,), (1,)), ((), ()))
TN = (((0,), (0,)), ((), ()))

CHUNKS = 2


def layer_kernel(
    n_fs, n_tp,
    tok, gain, w_pool, w_query, w_forget, w_value, maps, scale, low, spike, hgain, w_po, w_ro,
    out,
    tbuf, stage, wbuf, nbuf, sbuf, proj, pool_g, rec_g, halo, wo, map_v, part, dbuf, summed, obuf,
    ld, w_s, w_r, wt_s, wt_r, sp_s, sp_r, tf_s, tm_s, tz_r, td_s, td_r,
    wo_s, wo_r, ot_s, ot_r, pg_s, pg_r, pq_s, h_s, h_r, rg_s, rg_r, d_s, d_r, o_s, o_r, gate,
):
    s = lax.axis_index("sp")
    f = lax.axis_index("fs")
    t = lax.axis_index("tp")
    n_sp = 4
    rows = tok.shape[0]
    depth = w_pool.shape[0]
    width = w_pool.shape[1] // n_sp
    cols = w_po.shape[1]
    piece = depth // n_fs
    half = piece // 2
    strip = n_tp * rows
    pair = 2 * width
    reach_rows = halo.shape[1]

    side = s // 2
    end, mid, omid, oend = 3 * side, 1 + side, 2 - side, 3 - 3 * side
    mate = end + mid - s
    is_end, is_mid = s == end, s == mid
    peers = (mate, omid, oend)
    positions = range(n_sp)
    far_side, own_side = 2 - 2 * side, 2 * side

    def z(o):
        return {"sp": o, "fs": f, "tp": t}

    at_x = {"sp": s, "fs": f + 1 - 2 * lax.rem(f, 2), "tp": t}
    at_y = {"sp": s, "fs": f + 2 - 4 * (f // 2), "tp": t}
    other = {"sp": s, "fs": f, "tp": 1 - t}
    f_x, f_y, f_d = at_x["fs"], at_y["fs"], 3 - f

    def ds(start, size):
        return pl.ds(pl.multiple_of(start, size), size)

    def remote(src, dst, ssem, rsem, dev):
        return pltpu.make_async_remote_copy(
            src_ref=src, dst_ref=dst, send_sem=ssem, recv_sem=rsem,
            device_id=dev, device_id_type=pl.DeviceIdType.MESH,
        )

    def moved(view, ssem, rsem, dev):
        return remote(view, view, ssem, rsem, dev)

    def when(cond, action):
        if cond is None:
            action()
        else:
            pl.when(cond)(action)

    def load(src, dst, i, cond=None):
        copy = pltpu.make_async_copy(src, dst, ld.at[i])
        when(cond, copy.start)
        return copy, cond

    def finish(loaded):
        when(loaded[1], loaded[0].wait)

    barrier = pltpu.get_barrier_semaphore()
    partners = [z(o) for o in peers] + [at_x, at_y, other]
    for dev in partners:
        pl.semaphore_signal(barrier, inc=1, device_id=dev, device_id_type=pl.DeviceIdType.MESH)
    tok_load = load(tok, tbuf, 0)
    gates = (w_query, w_forget, w_value)
    stage_loads = []
    for j, dest in enumerate(peers):
        group_loads = []
        if j < 2:
            for m, w in enumerate(gates):
                group_loads.append(load(
                    w.at[ds(f * piece, piece), ds((dest // 2) * pair, pair)],
                    stage.at[j, :, pl.ds(m * pair, pair)], 1 + 4 * j + m, is_end if j == 0 else None,
                ))
        if j != 1:
            group_loads.append(load(
                w_pool.at[ds(f * piece, piece), :], stage.at[j, :, pl.ds(0, 2 * pair)],
                4 + 4 * j, is_mid if j == 0 else None,
            ))
        stage_loads.append(group_loads)
    own_rows = ds(s * depth, depth)
    own_loads = [
        load(w.at[:, ds(side * pair, pair)], wbuf.at[own_rows, pl.ds(m * pair, pair)], 13 + m, is_mid)
        for m, w in enumerate(gates)
    ]
    own_loads.append(load(w_pool, wbuf.at[own_rows, pl.ds(0, 2 * pair)], 16, is_end))
    map_load = load(maps, map_v, 17, is_end)
    wo_place = ds(lax.rem(s, 2) * cols, cols)
    wo_loads = [load(w, wo.at[k, :, wo_place], 18 + k, is_mid) for k, w in enumerate((w_po, w_ro))]

    pl.semaphore_wait(barrier, len(partners))

    def w_send(j, span):
        dst = wbuf.at[ds(s * depth + f * piece, piece), pl.ds(0, span)]
        return remote(stage.at[j, :, pl.ds(0, span)], dst, w_s.at[j], w_r.at[s], z(peers[j]))

    to_mid_mate, to_end_mate = w_send(0, 3 * pair), w_send(0, 2 * pair)
    to_omid, to_oend = w_send(1, 3 * pair), w_send(2, 2 * pair)
    for j in (1, 0, 2):
        for loaded in stage_loads[j]:
            finish(loaded)
    pl.when(is_mid)(to_omid.start)
    pl.when(is_mid)(to_oend.start)
    pl.when(is_mid)(to_end_mate.start)
    pl.when(is_end)(to_mid_mate.start)
    spike_sends = [remote(spike, sbuf.at[s], sp_s.at[j], sp_r.at[s], z(dest)) for j, dest in enumerate(peers)]
    for copy in spike_sends:
        copy.start()

    chunk = rows // CHUNKS

    def tok_view(o, core, c):
        return nbuf.at[o, core, pl.ds(c * chunk, chunk), :]

    def core_pass(o, c):
        return moved(tok_view(o, t, c), td_s.at[o, c], td_r.at[o, c], other)

    def core_arrival(o):
        for c in range(CHUNKS):
            moved(tok_view(o, 1 - t, c), td_s.at[o, c], td_r.at[o, c], other).wait_recv()

    finish(tok_load)
    x = tbuf[...].astype(F32)
    y = x * lax.rsqrt(jnp.mean(x * x, axis=-1, keepdims=True) + EPSILON) * gain[...]
    nbuf[s, t] = y.astype(BF16)
    to_mate = [moved(tok_view(s, t, c), tm_s.at[c], tz_r.at[s, c], z(mate)) for c in range(CHUNKS)]
    own_pass = [core_pass(s, c) for c in range(CHUNKS)]
    for copy in own_pass:
        copy.start()
    sbuf[s] = spike[...]

    def tree(view, ssem, rsem, log):
        def start(copy):
            copy.start()
            log.append(copy)

        def first(i, o):
            start(moved(view(o, f), ssem.at[0, i], rsem.at[0, i], at_x))
            start(moved(view(o, f), ssem.at[1, i], rsem.at[1, i], at_y))

        def second(i, o):
            moved(view(o, f_x), ssem.at[0, i], rsem.at[0, i], at_x).wait_recv()
            start(moved(view(o, f_x, 0), ssem.at[2, i], rsem.at[2, i], at_y))
            moved(view(o, f_y), ssem.at[1, i], rsem.at[1, i], at_y).wait_recv()
            start(moved(view(o, f_y, 1), ssem.at[3, i], rsem.at[3, i], at_x))

        def last(i, o):
            moved(view(o, f_d, 0), ssem.at[2, i], rsem.at[2, i], at_y).wait_recv()
            moved(view(o, f_d, 1), ssem.at[3, i], rsem.at[3, i], at_x).wait_recv()

        return first, second, last

    def w_tree(span, log):
        def view(o, giver, h=None):
            start, size = o * depth + giver * piece, piece
            if h is not None:
                start, size = start + h * half, half
            return wbuf.at[ds(start, size), pl.ds(0, span)]

        def arrival(j):
            moved(view(peers[j], f), w_s.at[j], w_r.at[peers[j]], z(peers[j])).wait_recv()

        first, second, last = tree(view, wt_s, wt_r, log)
        return (
            arrival,
            lambda j: first(j, peers[j]),
            lambda j: second(j, peers[j]),
            lambda j: last(j, peers[j]),
        )

    def project(base, span):
        x = nbuf[pl.ds(base, 2)].reshape(2 * strip, nbuf.shape[3])
        y = jnp.dot(x, wbuf[:, :span], preferred_element_type=F32)
        proj[pl.ds(base, 2), :, :span] = y.astype(BF16).reshape(2, strip, span)

    def pool_view(p):
        return pool_g.at[ds(p * strip, strip), :]

    own_blocks = (own_side, own_side + 1)
    pool_sends = [moved(pool_view(p), pg_s.at[i], pg_r.at[p], z(mid)) for i, p in enumerate(own_blocks)]
    tok_arrivals = {
        o: [moved(tok_view(p, t, c), tm_s.at[c], tz_r.at[p, c], z(p)) for c in range(CHUNKS)]
        for o, p in (("mate", mate), ("omid", omid), ("oend", oend))
    }

    def store(h):
        out[:, ds(2 * h * cols, 2 * cols)] = obuf[h]

    def common_drains():
        for copy in spike_sends + own_pass:
            copy.wait_send()

    @pl.when(is_end)
    def _():
        log = []
        arrival, first, second, last = w_tree(2 * pair, log)
        to_mid_mate.wait_send()
        to_omid.start()
        arrival(0)
        first(0)
        to_omid.wait_send()
        to_oend.start()
        for copy in to_mate:
            copy.start()
        second(0)
        arrival(1)
        first(1)
        arrival(2)
        first(2)
        for copy in to_mate:
            copy.wait_send()
        wo_sends = [
            remote(
                w.at[ds(f * piece, piece), :], wo.at[k, ds(f * piece, piece), wo_place], wo_s.at[k], wo_r.at[k], z(mid)
            )
            for k, w in enumerate((w_po, w_ro))
        ]
        for copy in wo_sends:
            copy.start()
        second(1)
        second(2)
        passes = [core_pass(mate, c) for c in range(CHUNKS)]
        for c in range(CHUNKS):
            tok_arrivals["mate"][c].wait_recv()
            passes[c].start()
        for j in range(3):
            last(j)
        finish(own_loads[3])
        core_arrival(s)
        core_arrival(mate)
        project(own_side, 2 * pair)
        halo_copy = remote(halo.at[0], halo.at[1], h_s.at[0], h_r.at[0], z(oend))

        @pl.when(side == 0)
        def _():
            halo[0] = proj[1, strip - reach_rows:, :2 * pair]
            halo_copy.start()
            halo[1] = jnp.zeros((reach_rows, 2 * pair), BF16)

        finish(map_load)
        groups = maps.shape[0]
        group = t * groups + lax.broadcasted_iota(jnp.int32, (strip, 2 * pair), 1) // pair
        position = lax.broadcasted_iota(jnp.int32, (strip, 2 * pair), 0)
        scale_row = scale[...]

        def pool(i, before):
            x = jnp.concatenate([before, proj[own_side + i, :, :2 * pair]], axis=0).astype(F32)
            total = x
            for g in range(n_tp * groups):
                reach = 2 ** g
                total = total + jnp.concatenate([jnp.zeros((reach, 2 * pair), F32), total[:-reach]], axis=0)
                if g == 0:
                    window_sum = total[reach_rows:]
                    window = jnp.full((strip, 2 * pair), 2, jnp.int32)
                else:
                    window_sum = jnp.where(group == g, total[reach_rows:], window_sum)
                    window = jnp.where(group == g, 2 ** (g + 1), window)
            counts = jnp.minimum((own_side + i) * strip + position + 1, window).astype(F32)
            diff = (window_sum / counts - x[reach_rows:]).astype(BF16)
            mapped = jnp.concatenate(
                [
                    jnp.dot(diff[:, g * pair:(g + 1) * pair], map_v[g], preferred_element_type=F32)
                    for g in range(groups)
                ],
                axis=1,
            )
            pool_g[ds((own_side + i) * strip, strip), :] = (mapped * scale_row).astype(BF16)

        pool(1, proj[own_side, strip - reach_rows:, :2 * pair])

        @pl.when(side == 1)
        def _():
            pool_sends[1].start()
            halo_copy.wait_recv()

        pool(0, halo[1])
        pool_sends[0].start()
        pl.when(side == 0)(pool_sends[1].start)
        for o in range(1, n_sp):
            origin = lax.rem(s + o, n_sp)
            remote(spike, sbuf.at[origin], sp_s.at[o - 1], sp_r.at[origin], z(origin)).wait_recv()
        common_drains()
        for copy in log + passes + wo_sends + pool_sends + [to_oend]:
            copy.wait_send()
        pl.when(side == 0)(halo_copy.wait_send)
        moved(obuf.at[1 - side], o_s.at[0], o_r.at[1 - side], z(omid)).wait_recv()
        store(1 - side)
        moved(obuf.at[side], o_s.at[0], o_r.at[side], z(mid)).wait_recv()
        store(side)

    @pl.when(is_mid)
    def _():
        log = []
        arrival, first, second, last = w_tree(3 * pair, log)
        to_far = [moved(tok_view(s, t, c), tf_s.at[0, c], tz_r.at[s, c], z(omid)) for c in range(CHUNKS)]
        relays = [moved(tok_view(mate, t, c), tf_s.at[1, c], tz_r.at[mate, c], z(omid)) for c in range(CHUNKS)]
        passes = {
            "mate": [core_pass(mate, c) for c in range(CHUNKS)],
            "omid": [core_pass(omid, c) for c in range(CHUNKS)],
            "oend": [core_pass(oend, c) for c in range(CHUNKS)],
        }

        def relay(c):
            tok_arrivals["mate"][c].wait_recv()
            relays[c].start()
            passes["mate"][c].start()

        def receive(o, c):
            tok_arrivals[o][c].wait_recv()
            passes[o][c].start()

        for copy in to_mate:
            copy.start()
        arrival(0)
        first(0)
        arrival(1)
        first(1)
        to_omid.wait_send()

        @pl.when(t == 0)
        def _():
            pl.semaphore_signal(gate, inc=1, device_id=other, device_id_type=pl.DeviceIdType.MESH)
            for copy in to_far:
                copy.start()

        second(0)
        arrival(2)
        first(2)

        @pl.when(t == 1)
        def _():
            pl.semaphore_wait(gate, 1)
            for copy in to_far:
                copy.start()

        second(1)
        relay(0)
        relay(1)
        second(2)
        for c in range(CHUNKS):
            receive("omid", c)
        def wo_view(k, giver, h=None):
            start, size = giver * piece, piece
            if h is not None:
                start, size = start + h * half, half
            return wo.at[k, ds(start, size), ds(lax.rem(end, 2) * cols, cols)]

        wo_first, wo_second, wo_last = tree(wo_view, ot_s, ot_r, log)
        for k in range(2):
            moved(wo_view(k, f), wo_s.at[k], wo_r.at[k], z(end)).wait_recv()
            wo_first(k, k)
        for c in range(CHUNKS):
            receive("oend", c)
        for j in range(3):
            last(j)
        for loaded in own_loads[:3]:
            finish(loaded)

        def tokens_of(first_side):
            @pl.when(side == first_side)
            def _():
                core_arrival(s)
                core_arrival(mate)

            @pl.when(side != first_side)
            def _():
                core_arrival(omid)
                core_arrival(oend)

        tokens_of(0)
        project(0, 3 * pair)

        def rec_view(o, p):
            return rec_g.at[o, ds(p * strip, strip), :]

        pool_relays = [moved(pool_view(p), pq_s.at[i], pg_r.at[p], z(omid)) for i, p in enumerate(own_blocks)]

        def pool_relay(i):
            pool_sends[i].wait_recv()
            pool_relays[i].start()

        rec_sends = [moved(rec_view(side, p), rg_s.at[p], rg_r.at[side, p], z(omid)) for p in positions]
        for d in range(1, n_sp):
            o = lax.rem(s + d, n_sp)
            remote(spike, sbuf.at[o], sp_s.at[d - 1], sp_r.at[o], z(o)).wait_recv()
        tri_r = lax.broadcasted_iota(jnp.int32, (BLOCK, BLOCK), 0)
        tri_c = lax.broadcasted_iota(jnp.int32, (BLOCK, BLOCK), 1)
        causal = tri_r >= tri_c
        tri = causal.astype(BF16)
        tri = jnp.concatenate([tri, tri, tri], axis=1)
        heads = range(pair // width)

        def per_head(values):
            return jnp.concatenate([values(2 * side + h) for h in heads], axis=1)

        gate_low = jax.nn.sigmoid(-per_head(lambda h: low[h]))
        head_gain = [hgain[2 * side + h] for h in heads]

        def column(o, h):
            row = jnp.broadcast_to(sbuf[o, pl.ds(2 * side + h, 1)], (8, strip))
            return jnp.broadcast_to(jnp.transpose(row)[:, :1], (strip, width))

        state = [jnp.zeros((width, width), F32) for h in heads]
        for p in positions:
            if p == 2:
                tokens_of(1)
                project(2, 3 * pair)
            projected = proj[p]
            spikes = jnp.concatenate([column(p, h) for h in heads], axis=1)
            q = projected[:, :pair].astype(F32)
            reader = q * jax.nn.sigmoid(q)
            key = gate_low * jax.nn.sigmoid(-projected[:, pair:2 * pair].astype(F32))
            logs = jnp.log1p(-key) + spikes
            high = logs.astype(BF16)
            rest = logs - high.astype(F32)
            middle = rest.astype(BF16)
            lowest = (rest - middle.astype(F32)).astype(BF16)
            for b in range(strip // BLOCK):
                here = slice(b * BLOCK, (b + 1) * BLOCK)
                terms = jnp.concatenate([high[here], middle[here], lowest[here]], axis=0)
                inner = jnp.dot(tri, terms, preferred_element_type=F32)
                closing = inner[BLOCK - 1:]
                read_scaled = (reader[here] * jnp.exp(inner)).astype(BF16)
                key_scaled = (key[here] * jnp.exp(-inner)).astype(BF16)
                key_tail = (key[here] * jnp.exp(closing - inner)).astype(BF16)
                kept = jnp.exp(closing)
                for h in heads:
                    at = slice(h * width, (h + 1) * width)
                    v = projected[here, 2 * pair + h * width:2 * pair + (h + 1) * width]
                    scores = lax.dot_general(read_scaled[:, at], key_scaled[:, at], NT, preferred_element_type=F32)
                    scores = jnp.where(causal, scores, 0.0).astype(BF16)
                    read = jnp.dot(scores, v, preferred_element_type=F32)
                    read = read + lax.dot_general(
                        read_scaled[:, at], state[h].astype(BF16), NT, preferred_element_type=F32
                    )
                    state[h] = kept[:, at] * state[h] + lax.dot_general(
                        v, key_tail[:, at], TN, preferred_element_type=F32
                    )
                    rec = read * lax.rsqrt(jnp.mean(read * read, axis=-1, keepdims=True) + EPSILON) * head_gain[h]
                    rec_g[side, p * strip + b * BLOCK:p * strip + (b + 1) * BLOCK, at] = rec.astype(BF16)
            if p == 1:
                pl.when(side == 0)(rec_sends[p].start)
            else:
                rec_sends[p].start()
            if p > 0 and p < 3:
                wo_second(p - 1, p - 1)
            upper_one = jnp.logical_and(t == 1, side == 1)
            upper_zero = jnp.logical_and(t == 0, side == 1)
            if p == 0:
                pl.when(upper_one)(functools.partial(pool_relay, 1))
            if p == 1:
                pl.when(upper_zero)(functools.partial(pool_relay, 1))
            if p == 2:
                pl.when(upper_one)(functools.partial(pool_relay, 0))
            if p == 1 or p == 2:
                pl.when(side == 0)(functools.partial(pool_relay, p - 1))
        pl.when(jnp.logical_and(t == 0, side == 1))(functools.partial(pool_relay, 0))
        pl.when(side == 1)(rec_sends[1].start)
        for k in range(2):
            finish(wo_loads[k])
        for k in range(2):
            wo_last(k, k)
        w_full = wo[...].reshape(2 * wo.shape[1], wo.shape[2])
        blocks = (0 * side, 3 - 2 * side, 2 + side, 1 + side)
        crossed = (side == 1, None, side == 0)

        def across(i):
            return remote(part.at[i, 1 - t], dbuf.at[i], d_s.at[i], d_r.at[i], other)

        def deliver(i):
            return remote(summed.at[i], obuf.at[side], o_s.at[i], o_r.at[side], z(blocks[i]))

        def settle(i):
            across(i).wait_recv()
            both = (part[i, t].astype(F32) + dbuf[i].astype(F32)).astype(BF16)

            @pl.when(s == blocks[i])
            def _():
                obuf[side] = both

            @pl.when(s != blocks[i])
            def _():
                summed[i] = both
                deliver(i).start()

        for i, p in enumerate(blocks):
            if i < 3:
                when(crossed[i], moved(pool_view(p), pq_s.at[0], pg_r.at[p], z(omid)).wait_recv)
            moved(rec_view(1 - side, p), rg_s.at[i], rg_r.at[1 - side, p], z(omid)).wait_recv()
            here = ds(p * strip, strip)
            mixed = jnp.concatenate([pool_g[here, :], rec_g[0, here, :], rec_g[1, here, :]], axis=1)
            acc = jnp.dot(mixed, w_full, preferred_element_type=F32).astype(BF16)
            for core in range(n_tp):
                part[i, core] = acc[core * rows:(core + 1) * rows]
            across(i).start()
            settle(i)
        common_drains()
        for copy in log + to_mate + to_far + relays + passes["mate"] + passes["omid"] + passes["oend"]:
            copy.wait_send()
        for copy in rec_sends + pool_relays + [to_end_mate, to_oend]:
            copy.wait_send()
        store(side)
        moved(obuf.at[1 - side], o_s.at[0], o_r.at[1 - side], z(omid)).wait_recv()
        store(1 - side)
        for i in range(n_sp):
            across(i).wait_send()
            pl.when(s != blocks[i])(deliver(i).wait_send)


def head_body(sizes, *args):
    (tokens, gain, w_pool, w_query, w_forget, w_value, maps, scale, low, spike, hgain, w_po, w_ro) = args
    n_sp, n_fs, n_tp = sizes
    tok = tokens[0]
    rows, features = tok.shape
    depth = w_pool.shape[0]
    width = w_pool.shape[1] // n_sp
    length = n_sp * n_tp * rows
    cols = w_po.shape[1]
    dma = pltpu.SemaphoreType.DMA
    whole = pl.BlockSpec(memory_space=pltpu.VMEM)
    here = pl.BlockSpec(memory_space=pl.ANY)
    result = pl.pallas_call(
        functools.partial(layer_kernel, n_fs, n_tp),
        out_shape=pltpu.VMEM((rows, n_sp * cols), BF16),
        in_specs=[here, whole, here, here, here, here, here, whole, whole, whole, whole, here, here],
        out_specs=whole,
        scratch_shapes=[
            pltpu.VMEM((rows, features), BF16),
            pltpu.VMEM((3, depth // n_fs, 6 * width), BF16),
            pltpu.VMEM((features, 6 * width), BF16),
            pltpu.VMEM((n_sp, n_tp, rows, features), BF16),
            pltpu.VMEM((n_sp,) + (spike.shape[2], spike.shape[1]), F32),
            pltpu.VMEM((n_sp, n_tp * rows, 6 * width), BF16),
            pltpu.VMEM((length, 4 * width), BF16),
            pltpu.VMEM((2, length, 2 * width), BF16),
            pltpu.VMEM((2, 2 ** (n_tp * maps.shape[0]), 4 * width), BF16),
            pltpu.VMEM((2, w_po.shape[0], 2 * cols), BF16),
            pltpu.VMEM(maps.shape, BF16),
            pltpu.VMEM((n_sp, n_tp, rows, 2 * cols), BF16),
            pltpu.VMEM((n_sp, rows, 2 * cols), BF16),
            pltpu.VMEM((n_sp, rows, 2 * cols), BF16),
            pltpu.VMEM((2, rows, 2 * cols), BF16),
            dma((20,)),
            dma((3,)), dma((n_sp,)),
            dma((4, 3)), dma((4, 3)),
            dma((3,)), dma((n_sp,)),
            dma((2, CHUNKS)), dma((CHUNKS,)), dma((n_sp, CHUNKS)),
            dma((n_sp, CHUNKS)), dma((n_sp, CHUNKS)),
            dma((2,)), dma((2,)),
            dma((4, 2)), dma((4, 2)),
            dma((2,)), dma((n_sp,)), dma((2,)),
            dma((1,)), dma((1,)),
            dma((n_sp,)), dma((2, n_sp)),
            dma((n_sp,)), dma((n_sp,)),
            dma((n_sp,)), dma((2,)),
            pltpu.SemaphoreType.REGULAR,
        ],
        compiler_params=pltpu.CompilerParams(
            collective_id=0, has_side_effects=True, vmem_limit_bytes=56 * 1024 * 1024
        ),
        name="layer",
    )(
        tok, gain[None], w_pool, w_query, w_forget, w_value, maps, scale[None],
        low.reshape(n_sp, 1, width), spike[0].T, hgain.reshape(n_sp, 1, width), w_po, w_ro,
    )
    return result[None]


def solution(mesh):
    placed = (
        P("fs", ("sp", "tp"), None),
        P(),
        P("sp", "tp"),
        P("sp", "tp"),
        P("sp", "tp"),
        P("sp", "tp"),
        P("tp", None, None),
        P("tp"),
        P("tp"),
        P("fs", "sp", "tp"),
        P("tp"),
        P("tp", "sp"),
        P("tp", "sp"),
    )
    sizes = (mesh.shape["sp"], mesh.shape["fs"], mesh.shape["tp"])

    def one(*args):
        maps, spike = args[6], args[9]
        width = args[2].shape[1] // sizes[0]
        fits = spike.shape[2] == sizes[0] and sizes == (4, 4, 2) and width % 128 == 0
        fits = fits and args[3].shape[1] == args[2].shape[1] and maps.shape[:2] == (2, 2 * width)
        return head_body(sizes, *args) if fits else body(*args)

    return jax.shard_map(
        one, mesh=mesh, in_specs=placed, out_specs=P("fs", ("sp", "tp"), None), check_vma=False
    )
```
